32 devices in a mesh: sp: 4 (over z), fs: 4 (over y, x), tp: 2 (over core).
Axes of the slice: x: 2, y: 2, z: 4, core: 2. Of those that a mesh axis runs over, the one named last changes fastest.
Arguments:
- tokens: bfloat16 [4096, 2048], P(('fs', 'sp', 'tp')), parts along dimension 0, may hold values from -6 to 6
- norm_gain: float32 [2048], replicated, may hold values from 0.1 to 1.9
- recurrent_input: bfloat16 [2048, 1024], P(None, 'tp'), may hold values from -0.125 to 0.125
- recurrent_gate: bfloat16 [2048, 1024], P(None, 'tp'), may hold values from -0.125 to 0.125
- attention_gate: bfloat16 [2048, 1024], P(None, 'tp'), may hold values from -0.125 to 0.125
- query_proj: bfloat16 [2048, 1536], P(None, 'tp'), may hold values from -0.125 to 0.125
- latent_down: bfloat16 [2048, 512], P(None, 'tp'), may hold values from -0.125 to 0.125
- rope_key_down: bfloat16 [2048, 64], replicated, may hold values from -0.125 to 0.125
- conv_kernel: float32 [4, 1024], P(None, 'tp'), may hold values from -3 to 3
- recurrence_gate_blocks: bfloat16 [16, 64, 64], P('tp'), may hold values from -0.75 to 0.75
- input_gate_blocks: bfloat16 [16, 64, 64], P('tp'), may hold values from -0.75 to 0.75
- decay_rate: float32 [1024], P('tp'), as said below
- decay_shift: float32 [4096], P(('fs', 'sp')), parts along dimension 0, may hold values from -2 to 0, as said below
- initial_state: float32 [4096], P(('fs', 'tp')), parts along dimension 0, may hold values from -6 to 6
- latent_gain: float32 [512], replicated, may hold values from 0.1 to 1.9
- latent_up: bfloat16 [512, 2048], P(None, 'tp'), may hold values from -0.25 to 0.25
- query_gain: float32 [192], replicated, may hold values from 0.4 to 250, as said below
- recurrent_output: bfloat16 [1024, 2048], P('tp'), may hold values from -0.25 to 0.25
- attention_output: bfloat16 [1024, 2048], P('tp'), may hold values from -0.25 to 0.25
Outputs:
- mixed_output: bfloat16 [4096, 2048], P(('fs', 'sp', 'tp')), parts along dimension 0
The draws below stay inside these ranges and needn't reach their ends.
There are 4 independent parts, one for each index of `fs`. The reference program is written for one: setup_inputs(seed, part) draws one part's arguments, and reference() takes and returns one part's arrays. A program takes and returns all parts, laid end to end along the dimension named above; an argument that names none is the same for every part. Nothing has to cross between parts.
Inputs may be any that keep to these rules, and one draw needn't show every extreme that they name: `decay_rate`: positive. `decay_shift`: negative. `query_gain`: positive.
All inputs are finite; a program needn't handle non-finite values.
Results may differ from the reference program's by a relative error of at most 0.03.
The reference program's roundings to bfloat16 on the way count: a program that leaves them out, or rounds other values in their place, can miss the bound.
Values may be sent and summed in bfloat16 or wider, within the bound.
A program may use at most 128 MiB of HBM per device.

```python
import math
import jax
import jax.numpy as jnp
from jax import lax

D = 2048
DR = 1024
BLK = 64
BLOCKS = 16
CONV = 4
H = 8
NOPE = 128
ROPE = 64
VH = 128
LAT = 512
DA = 1024
TOK_DEV = 256
SEQUENCE_LENGTH = 1024
N_TP = 2


def draw_decay_rate(key, part):
    pick_key, slow_key, fast_key = jax.random.split(key, 3)
    slow_share = 0.5
    slow_mask = jax.random.bernoulli(pick_key, slow_share, (DR,))
    slow_rate = jnp.exp(jax.random.uniform(slow_key, (DR,), jnp.float32, jnp.log(0.05), jnp.log(1.0))) / (8.0 * SEQUENCE_LENGTH)
    fast_rate = jnp.exp(jax.random.uniform(fast_key, (DR,), jnp.float32, jnp.log(0.004), jnp.log(0.012)))
    return jnp.where(slow_mask, slow_rate, fast_rate)


def draw_decay_shift(key, part):
    level_key, place_key, depth_key = jax.random.split(key, 3)
    block_count = SEQUENCE_LENGTH // TOK_DEV
    levels = jnp.exp(jax.random.uniform(level_key, (block_count,), jnp.float32, jnp.log(0.05), jnp.log(0.5))) / SEQUENCE_LENGTH
    baseline_offset = -jnp.repeat(levels, TOK_DEV)
    slot_indices = jax.random.randint(place_key, (2,), 0, SEQUENCE_LENGTH)
    layer_depths = jnp.log(jax.random.uniform(depth_key, (2,), jnp.float32, 0.5, 0.8))
    spike_flags = jnp.arange(SEQUENCE_LENGTH)[:, None] == slot_indices[None, :]
    return baseline_offset + jnp.sum(jnp.where(spike_flags, layer_depths[None, :], 0.0), axis=1)


def draw_query_gain(key, part):
    gain_key = jax.random.fold_in(key, 0)
    gain_values = jax.random.uniform(gain_key, (NOPE + ROPE,), jnp.float32, 0.4, 1.6)
    return gain_values


def level_of(rng, extent, cuts, least, high):
    level = 1.0
    for axis_at, parts in cuts:
        heights = jax.random.uniform(jax.random.fold_in(jax.random.fold_in(rng, 6), axis_at), (parts,), jnp.float32, least / len(cuts), high / len(cuts))
        level = level * jnp.repeat(jnp.exp(heights), extent[axis_at] // parts).reshape((-1,) + (1,) * (len(extent) - 1 - axis_at))
    return level


def scatter_about(key, extent, scale, bound, cuts=(), kind=jnp.bfloat16):
    array = scale * jax.random.normal(key, extent, jnp.float32)
    if cuts:
        array = array * level_of(key, extent, cuts, -0.22, 0.18)
    return jnp.clip(array, -bound, bound).astype(kind)


def setup_inputs(seed: int = 0, part: int = 0) -> dict:
    splits = jax.random.split(jax.random.key(seed), 20)
    part_keys = jax.random.split(jax.random.fold_in(splits[19], part), 20)
    return {
        "tokens": scatter_about(part_keys[0], (SEQUENCE_LENGTH, D), 1.0, 6.0, ((0, 8),)),
        "norm_gain": jnp.clip(1.0 + 0.18 * jax.random.normal(splits[1], (D,), jnp.float32), 0.1, 1.9),
        "recurrent_input": scatter_about(splits[2], (D, DR), D ** -0.5, 0.125, ((1, 2),)),
        "recurrent_gate": scatter_about(splits[3], (D, DR), D ** -0.5, 0.125, ((1, 2),)),
        "attention_gate": scatter_about(splits[4], (D, DA), D ** -0.5, 0.125, ((1, 2),)),
        "query_proj": scatter_about(splits[5], (D, H * (NOPE + ROPE)), D ** -0.5, 0.125, ((1, 2),)),
        "latent_down": scatter_about(splits[6], (D, LAT), D ** -0.5, 0.125, ((1, 2),)),
        "rope_key_down": scatter_about(splits[7], (D, ROPE), D ** -0.5, 0.125),
        "conv_kernel": scatter_about(splits[8], (CONV, DR), 0.5, 3.0, ((1, 2),), jnp.float32),
        "recurrence_gate_blocks": scatter_about(splits[9], (BLOCKS, BLK, BLK), BLK ** -0.5, 0.75, ((0, 2),)),
        "input_gate_blocks": scatter_about(splits[10], (BLOCKS, BLK, BLK), BLK ** -0.5, 0.75, ((0, 2),)),
        "decay_rate": draw_decay_rate(jax.random.fold_in(splits[19], 71), part),
        "decay_shift": draw_decay_shift(jax.random.fold_in(jax.random.fold_in(splits[19], part), 71), part),
        "initial_state": scatter_about(part_keys[13], (DR,), 1.0, 6.0, ((0, 2),), jnp.float32),
        "latent_gain": jnp.clip(1.0 + 0.18 * jax.random.normal(splits[14], (LAT,), jnp.float32), 0.1, 1.9),
        "latent_up": scatter_about(splits[15], (LAT, H * (NOPE + VH)), LAT ** -0.5, 0.25, ((1, 2),)),
        "query_gain": draw_query_gain(jax.random.fold_in(splits[19], 71), part),
        "recurrent_output": scatter_about(splits[17], (DR, D), ((DR + DA) // 4) ** -0.5, 0.25, ((0, 2),)),
        "attention_output": scatter_about(splits[18], (DA, D), ((DR + DA) // 4) ** -0.5, 0.25, ((0, 2),)),
    }


EPS = 1e-06
RECURRENT_SCALE = 8.0
THETA = 10000.0

def rotate_half(values, token_positions):
    half_width = values.shape[-1] // 2
    inv_freq = 1.0 / THETA ** (jnp.arange(0, 2 * half_width, 2, dtype=jnp.float32) / (2 * half_width))
    angles = token_positions.astype(jnp.float32)[:, None] * inv_freq[None, :]
    cosine = jnp.cos(angles)
    sine_part = jnp.sin(angles)
    if values.ndim == 3:
        cosine = cosine[:, None, :]
        sine_part = sine_part[:, None, :]
    first_half = values[..., :half_width]
    second_half = values[..., half_width:]
    return jnp.concatenate([first_half * cosine - second_half * sine_part, first_half * sine_part + second_half * cosine], axis=-1)

def rms_scaled(values, gain_vec):
    return values * lax.rsqrt(lax.optimization_barrier(jnp.mean(values * values, axis=-1, keepdims=True)) + EPS) * gain_vec

def rounded(values):
    return lax.optimization_barrier(values.astype(jnp.bfloat16)).astype(jnp.float32)

def linear_step(earlier, later_part):
    return (earlier[0] * later_part[0], later_part[0] * earlier[1] + later_part[1])

def reference(tokens, norm_gain, recurrent_input, recurrent_gate, attention_gate, query_proj, latent_down, rope_key_down, conv_kernel, recurrence_gate_blocks, input_gate_blocks, decay_rate, decay_shift, initial_state, latent_gain, latent_up, query_gain, recurrent_output, attention_output):
    normed = rms_scaled(tokens.astype(jnp.float32), norm_gain).astype(jnp.bfloat16)

    def project(weight):
        return jnp.dot(normed, weight, preferred_element_type=jnp.float32).astype(jnp.bfloat16)
    recur_signal = project(recurrent_input)
    recur_gate_pre = project(recurrent_gate)
    attention_pre = project(attention_gate)
    query_raw = project(query_proj)
    latent_raw = project(latent_down)
    rope_raw = project(rope_key_down)
    token_positions = jnp.arange(SEQUENCE_LENGTH, dtype=jnp.int32)
    padded = jnp.concatenate([jnp.zeros((CONV - 1, DR), jnp.bfloat16), recur_signal], axis=0).astype(jnp.float32)
    conv_sum = conv_kernel[0] * padded[0:SEQUENCE_LENGTH]
    for tap_index in range(1, CONV):
        conv_sum = conv_sum + conv_kernel[tap_index] * padded[tap_index:tap_index + SEQUENCE_LENGTH]
    conv_back = rounded(conv_sum)
    grouped = conv_back.reshape(SEQUENCE_LENGTH, BLOCKS, BLK)
    recur_rate = jax.nn.sigmoid(jnp.einsum('tbi,bij->tbj', grouped, recurrence_gate_blocks.astype(jnp.float32)).reshape(SEQUENCE_LENGTH, DR))
    input_rate = jax.nn.sigmoid(jnp.einsum('tbi,bij->tbj', grouped, input_gate_blocks.astype(jnp.float32)).reshape(SEQUENCE_LENGTH, DR))
    log_decay = -RECURRENT_SCALE * recur_rate * decay_rate + decay_shift[:, None]
    decay = jnp.exp(log_decay)
    driven = jnp.sqrt(-jnp.expm1(2.0 * log_decay)) * input_rate * conv_back
    driven = driven.at[0].add(decay[0] * initial_state)
    decay_prod, states = lax.associative_scan(linear_step, (decay, driven), axis=0)
    recur_out = (states * jax.nn.silu(recur_gate_pre.astype(jnp.float32))).astype(jnp.bfloat16)
    query_rows = rms_scaled(query_raw.astype(jnp.float32).reshape(SEQUENCE_LENGTH, H, NOPE + ROPE), query_gain)
    query_rows = jnp.concatenate([query_rows[..., :NOPE], rotate_half(query_rows[..., NOPE:], token_positions)], axis=-1).astype(jnp.bfloat16)
    latent = rms_scaled(latent_raw.astype(jnp.float32), latent_gain).astype(jnp.bfloat16)
    key_values = jnp.dot(latent, latent_up, preferred_element_type=jnp.float32).astype(jnp.bfloat16).reshape(SEQUENCE_LENGTH, H, NOPE + VH)
    key_nope = key_values[..., :NOPE].astype(jnp.float32)
    values_all = key_values[..., NOPE:].astype(jnp.float32)
    key_rope = rotate_half(rope_raw.astype(jnp.float32), token_positions).astype(jnp.bfloat16).astype(jnp.float32)
    query_block = math.gcd(SEQUENCE_LENGTH, 512)
    score_scale = (NOPE + ROPE) ** (-0.5)

    def attend(block_index):
        begin_row = (block_index * query_block).astype(jnp.int32)
        query_part = lax.dynamic_slice_in_dim(query_rows, begin_row, query_block, 0).astype(jnp.float32)
        scores = jnp.einsum('thd,khd->htk', query_part[..., :NOPE], key_nope)
        scores = scores + jnp.einsum('thr,kr->htk', query_part[..., NOPE:], key_rope)
        scores = scores * score_scale
        query_pos = begin_row + jnp.arange(query_block, dtype=jnp.int32)
        allowed = token_positions[None, None, :] <= query_pos[None, :, None]
        scores = jnp.where(allowed, scores, -jnp.inf)
        row_max = lax.optimization_barrier(jnp.max(scores, axis=-1, keepdims=True))
        weights = jnp.exp(scores - row_max)
        denominator = lax.optimization_barrier(jnp.sum(weights, axis=-1))
        weighted = jnp.einsum('htk,khd->thd', rounded(weights), values_all)
        return weighted / jnp.transpose(denominator)[:, :, None]
    attended = lax.map(attend, jnp.arange(SEQUENCE_LENGTH // query_block, dtype=jnp.int32)).reshape(SEQUENCE_LENGTH, DA)
    attention_out = (attended * jax.nn.silu(attention_pre.astype(jnp.float32))).astype(jnp.bfloat16)
    recur_group = DR // N_TP
    attend_group = DA // N_TP

    def add_group(group_index, running):
        index_value = group_index.astype(jnp.int32)
        recur_part = lax.dynamic_slice_in_dim(recur_out, index_value * recur_group, recur_group, 1)
        recur_rows = lax.dynamic_slice_in_dim(recurrent_output, index_value * recur_group, recur_group, 0)
        attend_part = lax.dynamic_slice_in_dim(attention_out, index_value * attend_group, attend_group, 1)
        attend_rows = lax.dynamic_slice_in_dim(attention_output, index_value * attend_group, attend_group, 0)
        partial_sum = jnp.dot(recur_part, recur_rows, preferred_element_type=jnp.float32) + jnp.dot(attend_part, attend_rows, preferred_element_type=jnp.float32)
        return running + rounded(partial_sum)
    total = lax.fori_loop(0, N_TP, add_group, jnp.zeros((SEQUENCE_LENGTH, D), jnp.float32))
    return total.astype(jnp.bfloat16)
```

```python
import functools

import jax
import jax.numpy as jnp
import numpy as np
from jax import lax
from jax.experimental import pallas as pl
from jax.experimental.pallas import tpu as pltpu
from jax.sharding import PartitionSpec as P

EPS = 1e-06
RECURRENT_SCALE = 8.0
THETA = 10000.0
F32 = jnp.float32
BF16 = jnp.bfloat16
LANES = 128


def expm1_neg(y):
    small = y * (1.0 + y * (0.5 + y * (1.0 / 6 + y * (1.0 / 24 + y * (1.0 / 120 + y / 720)))))
    return jnp.where(y > -0.35, small, jnp.exp(y) - 1.0)


def block_diagonal(scratch, blocks_ref, first):
    size = blocks_ref.shape[1]
    scratch[...] = jnp.zeros_like(scratch)
    for k in range(scratch.shape[0] // size):
        scratch[k * size : (k + 1) * size, k * size : (k + 1) * size] = blocks_ref[first + k]
    return scratch[...]


def scan_rows(decay, state):
    rows = decay.shape[0]
    row = lax.broadcasted_iota(jnp.int32, decay.shape, 0)
    step = 1
    while step < rows:
        inside = row >= step
        before_decay = jnp.where(inside, pltpu.roll(decay, step, 0), 1.0)
        before_state = jnp.where(inside, pltpu.roll(state, step, 0), 0.0)
        state = state + decay * before_state
        decay = decay * before_decay
        step *= 2
    return decay, state


def rms_scaled(values, gain_vec):
    return values * lax.rsqrt(jnp.mean(values * values, axis=-1, keepdims=True) + EPS) * gain_vec


LOG2E = 1.4426950408889634


def rotary_tables(positions, width):
    inv_freq = (1.0 / THETA ** (np.arange(0, width, 2, dtype=np.float32) / width)).astype(np.float32)
    angles = np.arange(positions, dtype=np.float32)[:, None] * inv_freq[None, :]
    cosine = np.cos(angles.astype(np.float64)).astype(np.float32)
    sine = np.sin(angles.astype(np.float64)).astype(np.float32)
    return cosine, sine


def column_step(width):
    return 256 if width % 256 == 0 else width


def remote(src, dst, send, recv, **where):
    return pltpu.make_async_remote_copy(
        src_ref=src, dst_ref=dst, send_sem=send, recv_sem=recv,
        device_id=where, device_id_type=pl.DeviceIdType.MESH,
    )


def scope(name):
    return jax.named_scope(name)


def layer_kernel(
    sp_count, tp_count,
    h_tokens, h_lat, h_norm, h_rope, h_ktab, h_in, h_query, h_qgain, h_qtab, h_conv, h_rec, h_inp,
    h_rate, h_shift, h_gate, h_att, h_lgain, h_up, h_init, h_rout, h_aout,
    out,
    tokens, w_lat, norm_gain, w_rope, key_table, w_in, w_query, query_gain, query_table,
    conv_kernel, rec_blocks, inp_blocks, decay_rate, decay_shift, w_gate, w_att, latent_gain,
    w_up, initial_state, w_rout, w_aout,
    tok_all, normed, lat_all, sig, gate, attp, turned_q, queries, rim_in, ext, diag_a, diag_b,
    prod, state, car_out, car_in, rout, racc, xlat, row_max, row_sum, acc, aout,
    part, own_part, part_in,
    w_sem, tok_s, tok_r, z_s, z_r, fwd_s, fwd_r, l_s, l_r, rim_s, rim_r, c_s, c_r, p_s, p_r, ready,
):
    sp = lax.axis_index("sp")
    tp = lax.axis_index("tp")
    share, model = tokens.shape
    rows = normed.shape[0]
    taps, width = conv_kernel.shape
    head_dim = query_gain.shape[1]
    rope = w_rope.shape[0]
    half = rope // 2
    nope = head_dim - rope
    heads = w_query.shape[1] // head_dim
    lat = w_lat.shape[1]
    value = w_att.shape[1] // heads
    packed = lat // rope
    tall = share // packed
    early = share + tall
    pieces = tok_s.shape[1]
    piece = share // pieces

    h_refs = (
        h_tokens, h_lat, h_norm, h_rope, h_ktab.at[sp * tp_count + tp], h_in, h_query, h_qgain,
        h_qtab.at[sp], h_conv, h_rec, h_inp, h_rate, h_shift, h_gate, h_att, h_lgain, h_up,
        h_init, h_rout, h_aout,
    )
    w_refs = (
        tokens, w_lat, norm_gain, w_rope, key_table, w_in, w_query, query_gain, query_table,
        conv_kernel, rec_blocks, inp_blocks, decay_rate, decay_shift, w_gate, w_att, latent_gain,
        w_up, initial_state, w_rout, w_aout,
    )
    loads = [
        pltpu.make_async_copy(a, b, w_sem.at[k]) for k, (a, b) in enumerate(zip(h_refs, w_refs))
    ]

    def peer(d):
        return lax.rem(tp + d, tp_count)

    def source(d):
        return lax.rem(tp - d + tp_count, tp_count)

    def greet(sem, **where):
        pl.semaphore_signal(sem, inc=1, device_id=where, device_id_type=pl.DeviceIdType.MESH)

    barrier = pltpu.get_barrier_semaphore()
    with scope("a_loads"):
        for d in range(1, tp_count):
            greet(barrier, tp=peer(d))
        for e in range(1, sp_count):
            pl.when(sp + e < sp_count)(lambda e=e: greet(barrier, sp=sp + e))
        for load in loads:
            load.start()
    (
        l_tok, l_lat, l_norm, l_rope, l_ktab, l_in, l_query, l_qgain, l_qtab, l_conv, l_rec, l_inp,
        l_rate, l_shift, l_gate, l_att, l_lgain, l_up, l_init, l_rout, l_aout,
    ) = loads

    def token_copy(d, k):
        part_rows = pl.ds(k * piece, piece)
        return remote(
            h_tokens.at[part_rows], tok_all.at[d - 1, part_rows],
            tok_s.at[d - 1, k], tok_r.at[d - 1, k], tp=peer(d),
        )

    with scope("b_barrier"):
        pl.semaphore_wait(barrier, tp_count - 1 + sp)
        for k in range(pieces):
            for d in range(1, tp_count):
                token_copy(d, k).start()
        for e in range(1, sp_count):
            pl.when(sp >= e)(lambda e=e: greet(ready.at[e - 1], sp=sp - e))

    def share_rows(place):
        return pl.ds(pl.multiple_of(place * share, share), share)

    def put_normed(block, place, k):
        first = pl.multiple_of(place * share + k * piece, piece)
        normed[pl.ds(first, piece)] = rms_scaled(block.astype(F32), norm_gain[...]).astype(BF16)

    def project(weight, into, here=slice(None)):
        step = column_step(weight.shape[1])
        for c in range(weight.shape[1] // step):
            cols = slice(c * step, (c + 1) * step)
            into[here, cols] = jnp.dot(
                normed[here], weight[:, cols], preferred_element_type=F32
            ).astype(BF16)

    own = lat_all.at[sp, tp]
    with scope("c_norm_own"):
        l_tok.wait()
        l_norm.wait()
        for k in range(pieces):
            put_normed(tokens[k * piece : (k + 1) * piece], tp, k)
    with scope("d_lat_a"):
        l_lat.wait()
        mine = normed[share_rows(tp)]
        own[:share] = jnp.dot(mine, w_lat[...], preferred_element_type=F32).astype(BF16)
        l_rope.wait()
        l_ktab.wait()
        raw = lax.dot_general(
            mine, w_rope[...], (((1,), (1,)), ((), ())), preferred_element_type=F32
        ).astype(BF16).astype(F32)
        swapped = jnp.concatenate([raw[:, half:], raw[:, :half]], axis=1)
        keyed = (raw * key_table[:, :rope] + swapped * key_table[:, rope:]).astype(BF16)
        for k in range(packed):
            own[share:early, k * rope : (k + 1) * rope] = keyed[k * tall : (k + 1) * tall]
    with scope("e_in_own"):
        l_in.wait()
        project(w_in, sig, share_rows(tp))

    def along(k):
        block = lat_all.at[sp, tp, (pl.ds(0, early), pl.ds(early, rows - share))[k]]
        return remote(block, block, z_s.at[k], z_r.at[k], sp=sp + 1)

    def landed(k):
        block = lat_all.at[sp - 1, tp, (pl.ds(0, early), pl.ds(early, rows - share))[k]]
        return remote(block, block, z_s.at[k], z_r.at[k], sp=sp - 1)

    def direct(e):
        block = lat_all.at[sp, tp]
        return remote(block, block, fwd_s.at[e - 2], fwd_r.at[e - 2], sp=sp + e)

    def forward():
        block = lat_all.at[sp - 1, tp]
        return remote(block, block, fwd_s.at[0], fwd_r.at[0], sp=sp + 1)

    def arrived(e):
        block = lat_all.at[sp - e, tp]
        return remote(block, block, fwd_s.at[e - 2], fwd_r.at[e - 2], sp=sp - 1)

    def across(e, d):
        block = lat_all.at[sp - e, tp]
        return remote(block, block, l_s.at[e, d - 1], l_r.at[e, d - 1], tp=peer(d))

    def crossed(e, d):
        block = lat_all.at[sp - e, source(d)]
        return remote(block, block, l_s.at[e, d - 1], l_r.at[e, d - 1], tp=source(d))

    def cross(e):
        for d in range(1, tp_count):
            across(e, d).start()

    def wait_crossed(e):
        for d in range(1, tp_count):
            crossed(e, d).wait_recv()

    has_next = sp + 1 < sp_count
    with scope("f_send_a"):

        @pl.when(has_next)
        def _():
            pl.semaphore_wait(ready.at[0], 1)
            along(0).start()

    with scope("g_norm_peer"):
        for k in range(pieces):
            for d in range(1, tp_count):
                token_copy(d, k).wait_recv()
                put_normed(tok_all[d - 1, k * piece : (k + 1) * piece], source(d), k)
    with scope("h_in_peer"):
        for d in range(1, tp_count):
            project(w_in, sig, share_rows(source(d)))

    def rim_copy():
        return remote(sig.at[pl.ds(rows - 16, 16)], rim_in, rim_s, rim_r, sp=sp + 1)

    def rim_landed():
        return remote(sig.at[pl.ds(rows - 16, 16)], rim_in, rim_s, rim_r, sp=sp - 1)

    with scope("i_lat_b"):
        pl.when(has_next)(lambda: rim_copy().start())
        for d in range(1, tp_count):
            own[early + (d - 1) * share : early + d * share] = jnp.dot(
                normed[share_rows(source(d))], w_lat[...], preferred_element_type=F32
            ).astype(BF16)
        pl.when(has_next)(lambda: along(1).start())
        cross(0)

    with scope("j_query"):
        l_query.wait()
        step = column_step(w_query.shape[1])
        for c in range(w_query.shape[1] // step):
            cols = slice(c * step, (c + 1) * step)
            raw = jnp.dot(normed[...], w_query[:, cols], preferred_element_type=F32).astype(BF16)
            turned_q[cols] = raw.T
    with scope("k_rotate"):
        l_qgain.wait()
        l_qtab.wait()
        spare = -head_dim % LANES
        gain = query_gain[...]
        if spare:
            gain = jnp.concatenate([gain, jnp.zeros((1, spare), F32)], axis=1)
        gain = jnp.broadcast_to(gain, (LANES, head_dim + spare)).T[:head_dim]
        gain = jnp.concatenate([gain] * (rows // LANES), axis=1)
        cosine = query_table[:half]
        sine = query_table[half:]
        for h in range(heads):
            head = turned_q[h * head_dim : (h + 1) * head_dim].astype(F32)
            square = jnp.sum(head * head, axis=0, keepdims=True)
            head = head * lax.rsqrt(square / head_dim + EPS) * gain
            first, second = head[nope : nope + half], head[nope + half :]
            queries[h, :nope] = head[:nope].astype(BF16)
            queries[h, nope : nope + half] = (first * cosine - second * sine).astype(BF16)
            queries[h, nope + half :] = (first * sine + second * cosine).astype(BF16)

    with scope("l_direct"):
        for e in range(2, sp_count):

            @pl.when(sp + e < sp_count)
            def _(e=e):
                pl.semaphore_wait(ready.at[e - 1], 1)
                if e > 2:
                    direct(e).start()

    with scope("m_rim"):

        @pl.when(sp == 0)
        def _():
            rim_in[...] = jnp.zeros_like(rim_in)

        pl.when(sp > 0)(lambda: rim_landed().wait_recv())
    with scope("n_scan"):
        for load in (l_conv, l_rec, l_inp, l_rate, l_shift):
            load.wait()
        ext[0:8] = rim_in[8:16].astype(F32)
        ext[8 : 8 + rows] = sig[...].astype(F32)
        size = rec_blocks.shape[1]
        car_out[...] = jnp.zeros_like(car_out)
        shift = jnp.broadcast_to(decay_shift[...], (LANES, rows)).T
        for c in range(width // LANES):
            cols = slice(c * LANES, (c + 1) * LANES)
            conv = conv_kernel[0:1, cols] * ext[9 - taps : 9 - taps + rows, cols]
            for j in range(1, taps):
                first = 9 - taps + j
                conv = conv + conv_kernel[j : j + 1, cols] * ext[first : first + rows, cols]
            conv = conv.astype(BF16)
            per = LANES // size
            rec = jax.nn.sigmoid(
                jnp.dot(conv, block_diagonal(diag_a, rec_blocks, c * per), preferred_element_type=F32)
            )
            inp = jax.nn.sigmoid(
                jnp.dot(conv, block_diagonal(diag_b, inp_blocks, c * per), preferred_element_type=F32)
            )
            log_decay = -RECURRENT_SCALE * rec * decay_rate[0:1, cols] + shift
            driven = jnp.sqrt(-expm1_neg(2.0 * log_decay)) * inp * conv.astype(F32)
            one, two = scan_rows(jnp.exp(log_decay), driven)
            prod[:, cols] = one
            state[:, cols] = two
            car_out[0:1, cols] = one[rows - 1 :]
            car_out[1:2, cols] = two[rows - 1 :]

    def carry_copy(e):
        return remote(car_out, car_in.at[e - 1], c_s.at[e - 1], c_r.at[e - 1], sp=sp + e)

    def carry_landed(e):
        return remote(car_out, car_in.at[e - 1], c_s.at[e - 1], c_r.at[e - 1], sp=sp - e)

    with scope("o_carry"):
        for e in range(1, sp_count):
            pl.when(sp + e < sp_count)(lambda e=e: carry_copy(e).start())
    with scope("p_relay1"):
        if sp_count > 1:

            @pl.when(sp >= 1)
            def _():
                landed(0).wait_recv()
                landed(1).wait_recv()
                if sp_count > 2:
                    pl.when(has_next)(lambda: forward().start())
                cross(1)

    with scope("q_gates"):
        l_gate.wait()
        project(w_gate, gate)
        l_att.wait()
        project(w_att, attp)

    factor = head_dim ** (-0.5) * LOG2E

    def attend(e, diagonal):
        place = sp - e
        blocks = []
        for n in range(tp_count):
            order = [(n - r) % tp_count for r in range(tp_count)]
            first = [0 if j == 0 else early + (j - 1) * share for j in order]
            blocks.append(
                jnp.concatenate([lat_all[place, n, f : f + share] for f in first], axis=0).astype(F32)
            )
        square = sum(jnp.sum(x * x, axis=-1, keepdims=True) for x in blocks)
        inverse = lax.rsqrt(square / (lat * tp_count) + EPS)
        for n, x in enumerate(blocks):
            cols = slice(n * lat, (n + 1) * lat)
            xlat[:, cols] = (x * inverse * latent_gain[0:1, cols]).astype(BF16)
        turned = jnp.concatenate(
            [
                lat_all[place, n, share:early, k * rope : (k + 1) * rope]
                for n in range(tp_count)
                for k in range(packed)
            ],
            axis=0,
        )
        for h in range(heads):
            base = h * (nope + value)
            kv = jnp.dot(
                xlat[...], w_up[:, base : base + nope + value], preferred_element_type=F32
            ).astype(BF16)
            keys = jnp.concatenate([kv[:, :nope], turned], axis=1)
            scores = jnp.dot(keys, queries[h], preferred_element_type=F32) * factor
            if diagonal:
                seen = lax.broadcasted_iota(jnp.int32, scores.shape, 0)
                scores = jnp.where(
                    seen <= lax.broadcasted_iota(jnp.int32, scores.shape, 1), scores, -jnp.inf
                )
            top = jnp.max(scores, axis=0, keepdims=True)
            if not diagonal:
                before = row_max[h, 0:1]
                top = jnp.maximum(top, before)
                fade = jnp.exp2(before - top)
            weights = jnp.exp2(scores - top)
            mass = jnp.sum(weights, axis=0, keepdims=True)
            term = jnp.dot(
                kv[:, nope:].T, weights.astype(BF16), preferred_element_type=F32
            )
            if not diagonal:
                mass = mass + row_sum[h, 0:1] * fade
                term = term + acc[h] * fade
            row_max[h, 0:1] = top
            row_sum[h, 0:1] = mass
            acc[h] = term

    with scope("r_att0"):
        l_lgain.wait()
        l_up.wait()
        wait_crossed(0)
        attend(0, True)
    with scope("s_att1"):
        if sp_count > 1:

            @pl.when(sp >= 1)
            def _():
                wait_crossed(1)
                attend(1, False)

    with scope("t_relay3"):
        if sp_count > 3:

            @pl.when(sp >= 3)
            def _():
                arrived(3).wait_recv()
                cross(3)

    with scope("u_carrywait"):
        for e in range(1, sp_count):

            @pl.when(sp >= e)
            def _(e=e):
                carry_landed(e).wait_recv()

            @pl.when(sp < e)
            def _(e=e):
                car_in[e - 1, 0:1] = jnp.ones((1, width), F32)
                car_in[e - 1, 1:2] = jnp.zeros((1, width), F32)

    with scope("v_rout"):
        l_init.wait()
        incoming = initial_state[...]
        for e in range(sp_count - 1, 0, -1):
            incoming = car_in[e - 1, 0:1] * incoming + car_in[e - 1, 1:2]
        for c in range(width // LANES):
            cols = slice(c * LANES, (c + 1) * LANES)
            full = state[:, cols] + prod[:, cols] * incoming[:, cols]
            rout[:, cols] = (full * jax.nn.silu(gate[:, cols].astype(F32))).astype(BF16)
        l_rout.wait()
        step = column_step(model)
        for c in range(model // step):
            cols = slice(c * step, (c + 1) * step)
            racc[:, cols] = jnp.dot(rout[...], w_rout[:, cols], preferred_element_type=F32)
    with scope("w_att3"):
        if sp_count > 3:

            @pl.when(sp >= 3)
            def _():
                wait_crossed(3)
                attend(3, False)

        if sp_count > 4:

            def later(e, carry):
                block = lat_all.at[sp - e, tp]
                remote(block, block, fwd_s.at[e - 2], fwd_r.at[e - 2], sp=sp - 1).wait_recv()
                cross(e)
                wait_crossed(e)
                attend(e, False)
                return carry

            lax.fori_loop(4, sp + 1, later, 0)
    with scope("x_relay2"):
        if sp_count > 2:

            @pl.when(sp >= 2)
            def _():
                arrived(2).wait_recv()
                cross(2)
                wait_crossed(2)

    with scope("y_att2"):
        if sp_count > 2:
            pl.when(sp >= 2)(lambda: attend(2, False))
    with scope("z_aout"):
        for h in range(heads):
            cols = slice(h * value, (h + 1) * value)
            attended = (acc[h] * (1.0 / row_sum[h, 0:1])).T
            aout[:, cols] = (attended * jax.nn.silu(attp[:, cols].astype(F32))).astype(BF16)

    chunks, step = part.shape[1], part.shape[3]

    def part_copy(d, c):
        return remote(
            part.at[d - 1, c], part_in.at[d - 1, c], p_s.at[d - 1, c], p_r.at[d - 1, c], tp=peer(d)
        )

    def partial(place, c):
        cols = slice(c * step, (c + 1) * step)
        here = share_rows(place)
        both = racc[here, cols] + jnp.dot(aout[here], w_aout[:, cols], preferred_element_type=F32)
        return both.astype(BF16)

    with scope("z_outmm"):
        l_aout.wait()
        for c in range(chunks):
            for d in range(1, tp_count):
                part[d - 1, c] = partial(peer(d), c)
                part_copy(d, c).start()
        for c in range(chunks):
            own_part[c] = partial(tp, c)
    with scope("z_sum"):
        for c in range(chunks):
            summed = own_part[c].astype(F32)
            for d in range(1, tp_count):
                part_copy(d, c).wait_recv()
                summed = summed + part_in[d - 1, c].astype(F32)
            out[:, c * step : (c + 1) * step] = summed.astype(BF16)

    with scope("z_waits"):
        for d in range(1, tp_count):
            for k in range(pieces):
                token_copy(d, k).wait_send()
            for c in range(chunks):
                part_copy(d, c).wait_send()
            across(0, d).wait_send()

        @pl.when(has_next)
        def _():
            rim_copy().wait_send()
            along(0).wait_send()
            along(1).wait_send()

        for e in range(1, sp_count):

            @pl.when(sp + e < sp_count)
            def _(e=e):
                carry_copy(e).wait_send()
                if e > 2:
                    direct(e).wait_send()

            @pl.when(sp >= e)
            def _(e=e):
                for d in range(1, tp_count):
                    across(e, d).wait_send()

        if sp_count > 2:
            pl.when((sp >= 1) & has_next)(lambda: forward().wait_send())


def body(
    tokens, norm_gain, recurrent_input, recurrent_gate, attention_gate, query_proj, latent_down,
    rope_key_down, conv_kernel, recurrence_gate_blocks, input_gate_blocks, decay_rate, decay_shift,
    initial_state, latent_gain, latent_up, query_gain, recurrent_output, attention_output,
):
    tp_count = lax.axis_size("tp")
    sp_count = lax.axis_size("sp")
    share, model = tokens.shape
    rows = share * tp_count
    width = recurrent_input.shape[1]
    taken = attention_gate.shape[1]
    head_dim = query_gain.shape[0]
    heads = query_proj.shape[1] // head_dim
    value = taken // heads
    lat = latent_down.shape[1]
    rope = rope_key_down.shape[1]
    cosine, sine = rotary_tables(sp_count * rows, rope)
    key_table = np.concatenate([cosine, cosine, -sine, sine], 1).reshape(-1, share, 2 * rope)
    query_table = np.concatenate([cosine, sine], 1).reshape(sp_count, rows, rope).transpose(0, 2, 1)
    hbm = [
        tokens, latent_down, norm_gain[None], rope_key_down.T, jnp.asarray(key_table),
        recurrent_input, query_proj, query_gain[None], jnp.asarray(query_table), conv_kernel,
        recurrence_gate_blocks, input_gate_blocks, decay_rate[None], decay_shift[None],
        recurrent_gate, attention_gate, latent_gain[None], latent_up, initial_state[None],
        recurrent_output, attention_output,
    ]
    held = [a.shape for a in hbm]
    held[4] = key_table.shape[1:]
    held[8] = query_table.shape[1:]
    vmem = pltpu.VMEM
    dma = pltpu.SemaphoreType.DMA
    others = max(tp_count - 1, 1)
    hops = max(sp_count - 1, 1)
    pieces = 4 if share % 64 == 0 else 1
    chunks = 4 if model % (4 * LANES) == 0 else 1
    return pl.pallas_call(
        functools.partial(layer_kernel, sp_count, tp_count),
        out_shape=pltpu.VMEM((share, model), BF16),
        in_specs=[pl.BlockSpec(memory_space=pl.ANY)] * len(hbm),
        out_specs=pl.BlockSpec(memory_space=pltpu.VMEM),
        scratch_shapes=[vmem(s, a.dtype) for s, a in zip(held, hbm)]
        + [
            vmem((others, share, model), BF16),
            vmem((rows, model), BF16),
            vmem((sp_count, tp_count, rows + share * rope // lat, lat), BF16),
            vmem((rows, width), BF16),
            vmem((rows, width), BF16),
            vmem((rows, taken), BF16),
            vmem((query_proj.shape[1], rows), BF16),
            vmem((heads, head_dim, rows), BF16),
            vmem((16, width), BF16),
            vmem((rows + 8, width), F32),
            vmem((LANES, LANES), BF16),
            vmem((LANES, LANES), BF16),
            vmem((rows, width), F32),
            vmem((rows, width), F32),
            vmem((8, width), F32),
            vmem((hops, 8, width), F32),
            vmem((rows, width), BF16),
            vmem((rows, model), F32),
            vmem((rows, lat * tp_count), BF16),
            vmem((heads, 8, rows), F32),
            vmem((heads, 8, rows), F32),
            vmem((heads, value, rows), F32),
            vmem((rows, taken), BF16),
            vmem((others, chunks, share, model // chunks), BF16),
            vmem((chunks, share, model // chunks), BF16),
            vmem((others, chunks, share, model // chunks), BF16),
            dma((len(hbm),)),
            dma((others, pieces)), dma((others, pieces)),
            dma((2,)), dma((2,)),
            dma((hops,)), dma((hops,)),
            dma((sp_count, others)), dma((sp_count, others)),
            dma, dma,
            dma((hops,)), dma((hops,)),
            dma((others, chunks)), dma((others, chunks)),
            pltpu.SemaphoreType.REGULAR((hops,)),
        ],
        compiler_params=pltpu.CompilerParams(
            collective_id=0, has_side_effects=True, vmem_limit_bytes=61400 * 1024
        ),
    )(*hbm)


def solution(mesh):
    return jax.shard_map(
        body,
        mesh=mesh,
        in_specs=(
            P(("fs", "sp", "tp"), None),
            P(),
            P(None, "tp"),
            P(None, "tp"),
            P(None, "tp"),
            P(None, "tp"),
            P(None, "tp"),
            P(),
            P(None, "tp"),
            P("tp", None, None),
            P("tp", None, None),
            P("tp"),
            P(("fs", "sp")),
            P(("fs", "tp")),
            P(),
            P(None, "tp"),
            P(),
            P("tp", None),
            P("tp", None),
        ),
        out_specs=P(("fs", "sp", "tp"), None),
        check_vma=False,
    )
```

```python
import functools

import jax
import jax.numpy as jnp
import numpy as np
from jax import lax
from jax.experimental import pallas as pl
from jax.experimental.pallas import tpu as pltpu
from jax.sharding import PartitionSpec as P

EPS = 1e-06
RECURRENT_SCALE = 8.0
THETA = 10000.0
F32 = jnp.float32
BF16 = jnp.bfloat16
LANES = 128


def expm1_neg(y, root):
    small = y * (1.0 + y * (0.5 + y * (1.0 / 6 + y * (1.0 / 24 + y / 120))))
    return jnp.where(y > -0.1, small, root * root - 1.0)


def block_diagonal(scratch, blocks_ref, first):
    size = blocks_ref.shape[1]
    scratch[...] = jnp.zeros_like(scratch)
    for k in range(scratch.shape[0] // size):
        scratch[k * size : (k + 1) * size, k * size : (k + 1) * size] = blocks_ref[first + k]
    return scratch[...]


def scan_rows(decay, state):
    rows = decay.shape[0]
    row = lax.broadcasted_iota(jnp.int32, decay.shape, 0)
    step = 1
    while step < rows:
        inside = row >= step
        before_decay = jnp.where(inside, pltpu.roll(decay, step, 0), 1.0)
        before_state = jnp.where(inside, pltpu.roll(state, step, 0), 0.0)
        state = state + decay * before_state
        decay = decay * before_decay
        step *= 2
    return decay, state


def rms_scaled(values, gain_vec):
    return values * lax.rsqrt(jnp.mean(values * values, axis=-1, keepdims=True) + EPS) * gain_vec


LOG2E = 1.4426950408889634


def rotary_tables(positions, width):
    inv_freq = (1.0 / THETA ** (np.arange(0, width, 2, dtype=np.float32) / width)).astype(np.float32)
    angles = np.arange(positions, dtype=np.float32)[:, None] * inv_freq[None, :]
    cosine = np.cos(angles.astype(np.float64)).astype(np.float32)
    sine = np.sin(angles.astype(np.float64)).astype(np.float32)
    return cosine, sine


def column_step(width):
    return 256 if width % 256 == 0 else width


def remote(src, dst, send, recv, **where):
    return pltpu.make_async_remote_copy(
        src_ref=src, dst_ref=dst, send_sem=send, recv_sem=recv,
        device_id=where, device_id_type=pl.DeviceIdType.MESH,
    )


def scope(name):
    return jax.named_scope(name)


def layer_kernel(
    sp_count, tp_count,
    h_tokens, h_lat, h_norm, h_rope, h_ktab, h_in, h_query, h_qgain, h_qtab, h_conv, h_rec, h_inp,
    h_rate, h_shift, h_gate, h_att, h_lgain, h_up, h_init, h_rout, h_aout,
    out,
    tokens, w_lat, norm_gain, w_rope, key_table, w_in, w_query, query_gain, query_table,
    conv_kernel, rec_blocks, inp_blocks, decay_rate, decay_shift, w_gate, w_att, latent_gain,
    w_up, initial_state, w_rout, w_aout,
    tok_all, normed, lat_all, sig, gate, attp, turned_q, queries, rim_out, rim_in, ext, diag_a, diag_b,
    mixer, unmixer, shift, silu_gate, mixed_rout,
    prod, state, segments, car_out, car_in, rout, racc, xlat, rope_keys, kv, held, row_max, row_sum,
    acc, aout, part, own_part, part_in,
    w_sem, tok_sem, tok_s, tok_r, z_s, z_r, y_s, y_r, fwd_s, fwd_r, l_s, l_r, rim_s, rim_r, c_s, c_r,
    p_s, p_r, ready,
):
    sp = lax.axis_index("sp")
    tp = lax.axis_index("tp")
    share, model = tokens.shape
    rows = normed.shape[0]
    taps, width = conv_kernel.shape
    head_dim = query_gain.shape[1]
    rope = w_rope.shape[0]
    half = rope // 2
    nope = head_dim - rope
    heads = w_query.shape[1] // head_dim
    lat = w_lat.shape[1]
    value = w_att.shape[1] // heads
    packed = lat // rope
    tall = share // packed
    pieces = tok_s.shape[1]
    piece = share // pieces
    long = rows // 8

    h_refs = (
        h_tokens, h_lat, h_norm, h_rope, h_ktab.at[sp * tp_count + tp], h_in, h_query, h_qgain,
        h_qtab.at[sp], h_conv, h_rec, h_inp, h_rate, h_shift, h_gate, h_att, h_lgain, h_up,
        h_init, h_rout, h_aout,
    )
    w_refs = (
        tokens, w_lat, norm_gain, w_rope, key_table, w_in, w_query, query_gain, query_table,
        conv_kernel, rec_blocks, inp_blocks, decay_rate, decay_shift, w_gate, w_att, latent_gain,
        w_up, initial_state, w_rout, w_aout,
    )
    loads = [
        pltpu.make_async_copy(a, b, w_sem.at[k]) for k, (a, b) in enumerate(zip(h_refs, w_refs)) if k
    ]
    token_loads = [
        pltpu.make_async_copy(
            h_tokens.at[pl.ds(k * piece, piece)], tokens.at[pl.ds(k * piece, piece)], tok_sem.at[k]
        )
        for k in range(pieces)
    ]

    def peer(d):
        return lax.rem(tp + d, tp_count)

    def source(d):
        return lax.rem(tp - d + tp_count, tp_count)

    def greet(sem, **where):
        pl.semaphore_signal(sem, inc=1, device_id=where, device_id_type=pl.DeviceIdType.MESH)

    barrier = pltpu.get_barrier_semaphore()
    with scope("a_loads"):
        for d in range(1, tp_count):
            greet(barrier, tp=peer(d))
        for e in range(1, sp_count):
            pl.when(sp + e < sp_count)(lambda e=e: greet(barrier, sp=sp + e))
        for load in [loads[1], *token_loads, loads[0]]:
            load.start()
    (
        l_lat, l_norm, l_rope, l_ktab, l_in, l_query, l_qgain, l_qtab, l_conv, l_rec, l_inp,
        l_rate, l_shift, l_gate, l_att, l_lgain, l_up, l_init, l_rout, l_aout,
    ) = loads

    def token_copy(d, k):
        part_rows = pl.ds(k * piece, piece)
        return remote(
            h_tokens.at[part_rows], tok_all.at[d - 1, part_rows],
            tok_s.at[d - 1, k], tok_r.at[d - 1, k], tp=peer(d),
        )

    with scope("b_barrier"):
        pl.semaphore_wait(barrier, tp_count - 1 + sp)
        for k in range(pieces):
            for d in range(1, tp_count):
                token_copy(d, k).start()
        for e in range(1, sp_count):
            pl.when(sp >= e)(lambda e=e: greet(ready.at[e - 1], sp=sp - e))
        for load in (loads[2], loads[3], loads[4], loads[5]):
            load.start()

    def share_rows(place):
        return pl.ds(pl.multiple_of(place * share, share), share)

    def put_normed(block, place):
        normed[share_rows(place)] = rms_scaled(block.astype(F32), norm_gain[...]).astype(BF16)

    def put_latent(first, place):
        own[first : first + share] = jnp.dot(
            normed[share_rows(place)], w_lat[...], preferred_element_type=F32
        ).astype(BF16)

    def project(weight, into, here=slice(None)):
        step = column_step(weight.shape[1])
        for c in range(weight.shape[1] // step):
            cols = slice(c * step, (c + 1) * step)
            into[here, cols] = jnp.dot(
                normed[here], weight[:, cols], preferred_element_type=F32
            ).astype(BF16)

    own = lat_all.at[sp, tp]
    with scope("c_norm_own"):
        l_norm.wait()
        for k in range(pieces):
            token_loads[k].wait()
        put_normed(tokens[...], tp)
    with scope("d_lat_a"):
        l_lat.wait()
        put_latent(0, tp)

    def along(k):
        block = lat_all.at[sp, tp, (pl.ds(0, share), pl.ds(share, rows + tall - share))[k]]
        return remote(block, block, z_s.at[k], z_r.at[k], sp=sp + 1)

    def landed(k):
        block = lat_all.at[sp - 1, tp, (pl.ds(0, share), pl.ds(share, rows + tall - share))[k]]
        return remote(block, block, z_s.at[k], z_r.at[k], sp=sp - 1)

    def direct(e):
        block = lat_all.at[sp, tp]
        return remote(block, block, fwd_s.at[e - 2], fwd_r.at[e - 2], sp=sp + e)

    def forward(k):
        block = lat_all.at[sp - 1, tp, (pl.ds(0, share), pl.ds(share, rows + tall - share))[k]]
        return remote(block, block, y_s.at[k], y_r.at[k], sp=sp + 1)

    def forwarded(k):
        block = lat_all.at[sp - 2, tp, (pl.ds(0, share), pl.ds(share, rows + tall - share))[k]]
        return remote(block, block, y_s.at[k], y_r.at[k], sp=sp - 1)

    def arrived(e):
        block = lat_all.at[sp - e, tp]
        return remote(block, block, fwd_s.at[e - 2], fwd_r.at[e - 2], sp=sp - 1)

    def across(e, d):
        block = lat_all.at[sp - e, tp]
        return remote(block, block, l_s.at[e, d - 1], l_r.at[e, d - 1], tp=peer(d))

    def crossed(e, d):
        block = lat_all.at[sp - e, source(d)]
        return remote(block, block, l_s.at[e, d - 1], l_r.at[e, d - 1], tp=source(d))

    def cross(e):
        for d in range(1, tp_count):
            across(e, d).start()

    def wait_crossed(e):
        for d in range(1, tp_count):
            crossed(e, d).wait_recv()

    has_next = sp + 1 < sp_count
    with scope("f_send_a"):

        @pl.when(has_next)
        def _():
            pl.semaphore_wait(ready.at[0], 1)
            along(0).start()

    with scope("e_mixers"):
        row = lax.broadcasted_iota(jnp.int32, (rows, rows), 0)
        column = lax.broadcasted_iota(jnp.int32, (rows, rows), 1)
        mixer[...] = jnp.where(column == (row & 7) * long + (row >> 3), 1.0, 0.0).astype(BF16)
        unmixer[...] = jnp.where(row == (column & 7) * long + (column >> 3), 1.0, 0.0).astype(BF16)
    with scope("e_rope"):
        l_rope.wait()
        l_ktab.wait()
        raw = lax.dot_general(
            normed[share_rows(tp)], w_rope[...], (((1,), (1,)), ((), ())),
            preferred_element_type=F32,
        ).astype(BF16).astype(F32)
        swapped = jnp.concatenate([raw[:, half:], raw[:, :half]], axis=1)
        keyed = (raw * key_table[:, :rope] + swapped * key_table[:, rope:]).astype(BF16)
        for k in range(packed):
            own[share : share + tall, k * rope : (k + 1) * rope] = keyed[k * tall : (k + 1) * tall]
    with scope("e_in_own"):
        for load in loads[6:8]:
            load.start()
        l_in.wait()
        project(w_in, sig, share_rows(tp))
    with scope("g_norm_peer"):
        for k in range(pieces):
            for d in range(1, tp_count):
                token_copy(d, k).wait_recv()
        for d in range(1, tp_count):
            put_normed(tok_all[d - 1], source(d))
    def rim_copy():
        return remote(rim_out, rim_in, rim_s, rim_r, sp=sp + 1)

    def rim_landed():
        return remote(rim_out, rim_in, rim_s, rim_r, sp=sp - 1)

    with scope("h_in_peer"):
        for load in loads[8:]:
            load.start()
        for d in range(1, tp_count):
            project(w_in, sig, share_rows(source(d)))
        tail = sig[rows - 16 :].astype(F32)[12:]
        tail = [tail[:, c * LANES : (c + 1) * LANES] for c in range(width // LANES)]
        if len(tail) * 4 < rim_out.shape[0]:
            tail.append(jnp.zeros((rim_out.shape[0] - len(tail) * 4, LANES), F32))
        rim_out[...] = jnp.concatenate(tail, axis=0).astype(BF16)
        pl.when(has_next)(lambda: rim_copy().start())
    with scope("i_lat_b"):
        for d in range(1, tp_count):
            put_latent(d * share + tall, source(d))
        pl.when(has_next)(lambda: along(1).start())
        cross(0)
    with scope("j_query"):
        l_query.wait()
        step = column_step(w_query.shape[1])
        for c in range(w_query.shape[1] // step):
            cols = slice(c * step, (c + 1) * step)
            raw = jnp.dot(normed[...], w_query[:, cols], preferred_element_type=F32).astype(BF16)
            turned_q[cols] = raw.T
    with scope("k_rotate"):
        l_qgain.wait()
        l_qtab.wait()
        spare = -head_dim % LANES
        gain = query_gain[...]
        if spare:
            gain = jnp.concatenate([gain, jnp.zeros((1, spare), F32)], axis=1)
        gain = jnp.broadcast_to(gain, (LANES, head_dim + spare)).T[:head_dim]
        gain = jnp.concatenate([gain] * (rows // LANES), axis=1)
        cosine = query_table[:half]
        sine = query_table[half:]
        for h in range(heads):
            head = turned_q[h * head_dim : (h + 1) * head_dim].astype(F32)
            square = jnp.sum(head * head, axis=0, keepdims=True)
            head = head * lax.rsqrt(square / head_dim + EPS) * gain
            first, second = head[nope : nope + half], head[nope + half :]
            queries[h, :nope] = head[:nope].astype(BF16)
            queries[h, nope : nope + half] = (first * cosine - second * sine).astype(BF16)
            queries[h, nope + half :] = (first * sine + second * cosine).astype(BF16)

    with scope("l_direct"):
        for e in range(2, sp_count):

            @pl.when(sp + e < sp_count)
            def _(e=e):
                pl.semaphore_wait(ready.at[e - 1], 1)
                if e > 2:
                    direct(e).start()

    with scope("m_rim"):

        @pl.when(sp == 0)
        def _():
            rim_in[...] = jnp.zeros_like(rim_in)

        pl.when(sp > 0)(lambda: rim_landed().wait_recv())
    with scope("n_scan"):
        for load in (l_conv, l_rec, l_inp, l_rate, l_shift):
            load.wait()
        size = rec_blocks.shape[1]
        car_out[...] = jnp.zeros_like(car_out)
        lead = 8 * (taps - 1)
        ext[lead : lead + rows] = jnp.dot(mixer[...], sig[...], preferred_element_type=F32)
        top_row = lax.broadcasted_iota(jnp.int32, (8, width), 0) == 0
        rim = rim_in[...].astype(F32)
        rim = jnp.concatenate(
            [rim[4 * c : 4 * c + 4] for c in range(width // LANES)], axis=1
        )
        for k in range(1, taps):
            last = ext[lead + rows - 8 * k : lead + rows - 8 * k + 8]
            ext[lead - 8 * k : lead - 8 * k + 8] = jnp.where(
                top_row, rim[4 - k : 5 - k], pltpu.roll(last, 1, 0)
            )
        table = jnp.concatenate(
            [decay_shift[:, k * long : (k + 1) * long] for k in range(8)], axis=0
        )
        for i in range(long):
            shift[8 * i : 8 * i + 8] = jnp.broadcast_to(table[:, i : i + 1], (8, LANES))
        groups = width // LANES
        for c in range(groups):
            cols = slice(c * LANES, (c + 1) * LANES)
            conv = conv_kernel[0:1, cols] * ext[0:rows, cols]
            for j in range(1, taps):
                conv = conv + conv_kernel[j : j + 1, cols] * ext[8 * j : 8 * j + rows, cols]
            conv = conv.astype(BF16)
            per = LANES // size
            rec = jax.nn.sigmoid(
                jnp.dot(conv, block_diagonal(diag_a, rec_blocks, c * per), preferred_element_type=F32)
            )
            inp = jax.nn.sigmoid(
                jnp.dot(conv, block_diagonal(diag_b, inp_blocks, c * per), preferred_element_type=F32)
            )
            log_decay = -RECURRENT_SCALE * rec * decay_rate[0:1, cols] + shift[...]
            decay = jnp.exp(log_decay)
            prod[c] = decay
            state[c] = jnp.sqrt(-expm1_neg(2.0 * log_decay, decay)) * inp * conv.astype(F32)
        ones = [prod[c, 0:8] for c in range(groups)]
        twos = [state[c, 0:8] for c in range(groups)]
        for i in range(1, long):
            here = slice(8 * i, 8 * i + 8)
            for c in range(groups):
                decay = prod[c, here]
                twos[c] = decay * twos[c] + state[c, here]
                ones[c] = decay * ones[c]
                prod[c, here] = ones[c]
                state[c, here] = twos[c]
        first_row = lax.broadcasted_iota(jnp.int32, (8, LANES), 0) == 0
        for c in range(groups):
            cols = slice(c * LANES, (c + 1) * LANES)
            one, two = scan_rows(ones[c], twos[c])
            segments[0:8, cols] = jnp.where(first_row, 1.0, pltpu.roll(one, 1, 0))
            segments[8:16, cols] = jnp.where(first_row, 0.0, pltpu.roll(two, 1, 0))
            car_out[2 * c : 2 * c + 1] = one[7:8]
            car_out[2 * c + 1 : 2 * c + 2] = two[7:8]

    def carry_copy(e):
        return remote(car_out, car_in.at[e - 1], c_s.at[e - 1], c_r.at[e - 1], sp=sp + e)

    def carry_landed(e):
        return remote(car_out, car_in.at[e - 1], c_s.at[e - 1], c_r.at[e - 1], sp=sp - e)

    with scope("o_carry"):
        for e in range(1, sp_count):
            pl.when(sp + e < sp_count)(lambda e=e: carry_copy(e).start())
    def relay1(k):
        if sp_count > 1:

            @pl.when(sp >= 1)
            def _():
                landed(k).wait_recv()
                if sp_count > 2:
                    pl.when(has_next)(lambda: forward(k).start())
                if k:
                    cross(1)

    with scope("p_relay1a"):
        relay1(0)

    with scope("q_gates"):
        l_gate.wait()
        project(w_gate, gate)
        l_att.wait()
        project(w_att, attp)
        silu_gate[...] = jax.nn.silu(
            jnp.dot(mixer[...], gate[...], preferred_element_type=F32)
        )

    factor = head_dim ** (-0.5) * LOG2E

    def prepare(e):
        place = sp - e
        blocks = []
        for n in range(tp_count):
            order = [(n - r) % tp_count for r in range(tp_count)]
            first = [0 if j == 0 else tall + j * share for j in order]
            blocks.append(
                jnp.concatenate([lat_all[place, n, f : f + share] for f in first], axis=0).astype(F32)
            )
        square = sum(jnp.sum(x * x, axis=-1, keepdims=True) for x in blocks)
        inverse = lax.rsqrt(square / (lat * tp_count) + EPS)
        for n, x in enumerate(blocks):
            cols = slice(n * lat, (n + 1) * lat)
            xlat[:, cols] = (x * inverse * latent_gain[0:1, cols]).astype(BF16)
        rope_keys[...] = jnp.concatenate(
            [
                lat_all[place, n, share : share + tall, k * rope : (k + 1) * rope]
                for n in range(tp_count)
                for k in range(packed)
            ],
            axis=0,
        )
        step = column_step(w_up.shape[1])
        for c in range(w_up.shape[1] // step):
            cols = slice(c * step, (c + 1) * step)
            kv[:, cols] = jnp.dot(xlat[...], w_up[:, cols], preferred_element_type=F32).astype(BF16)

    def heads_over(diagonal, lanes=slice(None), count=None):
        count = rows if count is None else count

        def score(h):
            base = h * (nope + value)
            keys = jnp.concatenate([kv[:, base : base + nope], rope_keys[...]], axis=1)
            scores = jnp.dot(keys, queries[h, :, lanes], preferred_element_type=F32) * factor
            if diagonal:
                seen = lax.broadcasted_iota(jnp.int32, scores.shape, 0)
                scores = jnp.where(
                    seen <= lax.broadcasted_iota(jnp.int32, scores.shape, 1), scores, -jnp.inf
                )
            held[h, :, :count] = scores
            return jnp.max(scores, axis=0, keepdims=True)

        def mix(h, top):
            base = h * (nope + value) + nope
            if not diagonal:
                before = row_max[h, 0:1, lanes]
                top = jnp.maximum(top, before)
                fade = jnp.exp2(before - top)
            weights = jnp.exp2(held[h, :, :count] - top)
            mass = jnp.sum(weights, axis=0, keepdims=True)
            term = jnp.dot(
                kv[:, base : base + value].T, weights.astype(BF16), preferred_element_type=F32
            )
            if not diagonal:
                mass = mass + row_sum[h, 0:1, lanes] * fade
                term = term + acc[h, :, lanes] * fade
            row_max[h, 0:1, lanes] = top
            row_sum[h, 0:1, lanes] = mass
            acc[h, :, lanes] = term

        tops = score(0)
        for h in range(heads):
            now = tops
            if h + 1 < heads:
                tops = score(h + 1)
            mix(h, now)

    def attend(e, diagonal):
        prepare(e)
        heads_over(diagonal)

    with scope("r_att0"):
        l_lgain.wait()
        l_up.wait()
        wait_crossed(0)
        prepare(0)
    with scope("p_relay1b"):
        relay1(1)
    with scope("r_att0_heads"):
        heads_over(True)
    with scope("t_relay3"):
        if sp_count > 3:

            @pl.when(sp >= 3)
            def _():
                arrived(3).wait_recv()
                cross(3)

    with scope("s_att1"):
        if sp_count > 1:

            @pl.when(sp >= 1)
            def _():
                wait_crossed(1)
                attend(1, False)

    with scope("w_att3"):
        if sp_count > 3:

            @pl.when(sp >= 3)
            def _():
                wait_crossed(3)
                attend(3, False)

        if sp_count > 4:

            def later(e, carry):
                block = lat_all.at[sp - e, tp]
                remote(block, block, fwd_s.at[e - 2], fwd_r.at[e - 2], sp=sp - 1).wait_recv()
                cross(e)
                wait_crossed(e)
                attend(e, False)
                return carry

            lax.fori_loop(4, sp + 1, later, 0)
    with scope("x_relay2"):
        if sp_count > 2:

            @pl.when(sp >= 2)
            def _():
                forwarded(0).wait_recv()
                forwarded(1).wait_recv()
                cross(2)

    with scope("u_carrywait"):
        for e in range(1, sp_count):

            @pl.when(sp >= e)
            def _(e=e):
                carry_landed(e).wait_recv()

            @pl.when(sp < e)
            def _(e=e):
                row = lax.broadcasted_iota(jnp.int32, car_out.shape, 0)
                car_in[e - 1] = jnp.where((row & 1) == 0, 1.0, 0.0)

    with scope("v_rout"):
        l_init.wait()
        for c in range(width // LANES):
            cols = slice(c * LANES, (c + 1) * LANES)
            incoming = initial_state[:, cols]
            for e in range(sp_count - 1, 0, -1):
                incoming = (
                    car_in[e - 1, 2 * c : 2 * c + 1] * incoming
                    + car_in[e - 1, 2 * c + 1 : 2 * c + 2]
                )
            enter = segments[0:8, cols] * incoming + segments[8:16, cols]
            full = state[c] + prod[c] * jnp.concatenate([enter] * long, axis=0)
            mixed_rout[:, cols] = (full * silu_gate[:, cols]).astype(BF16)
        rout[...] = jnp.dot(
            unmixer[...], mixed_rout[...], preferred_element_type=F32
        ).astype(BF16)
        l_rout.wait()
        step = column_step(model)
        for c in range(model // step):
            cols = slice(c * step, (c + 1) * step)
            racc[:, cols] = jnp.dot(rout[...], w_rout[:, cols], preferred_element_type=F32)
    chunks, step = part_in.shape[1], part_in.shape[3]
    split = share % LANES == 0

    def part_copy(d, c):
        return remote(
            part.at[d - 1, c], part_in.at[d - 1, c], p_s.at[d - 1, c], p_r.at[d - 1, c], tp=peer(d)
        )

    def partial(place, c):
        cols = slice(c * step, (c + 1) * step)
        here = share_rows(place)
        both = racc[here, cols] + jnp.dot(aout[here], w_aout[:, cols], preferred_element_type=F32)
        return both.astype(BF16)

    def finish(here):
        for h in range(heads):
            cols = slice(h * value, (h + 1) * value)
            attended = (acc[h, :, here] * (1.0 / row_sum[h, 0:1, here])).T
            aout[here, cols] = (attended * jax.nn.silu(attp[here, cols].astype(F32))).astype(BF16)

    def last(place):
        if sp_count > 2:
            pl.when(sp >= 2)(lambda: heads_over(False, share_rows(place), share))
        finish(share_rows(place))

    with scope("y_att2"):
        if sp_count > 2:

            @pl.when(sp >= 2)
            def _():
                wait_crossed(2)
                prepare(2)
                if not split:
                    heads_over(False)

        if not split:
            finish(slice(None))
    with scope("z_peer"):
        l_aout.wait()
        for d in range(1, tp_count):
            if split:
                last(peer(d))
            for c in range(chunks):
                part[d - 1, c] = partial(peer(d), c)
                part_copy(d, c).start()
    with scope("z_own"):
        if split:
            last(tp)
        for c in range(chunks):
            own_part[c] = partial(tp, c)
    with scope("z_sum"):
        for c in range(chunks):
            summed = own_part[c].astype(F32)
            for d in range(1, tp_count):
                part_copy(d, c).wait_recv()
                summed = summed + part_in[d - 1, c].astype(F32)
            out[:, c * step : (c + 1) * step] = summed.astype(BF16)

    with scope("z_waits"):
        for d in range(1, tp_count):
            for k in range(pieces):
                token_copy(d, k).wait_send()
            for c in range(chunks):
                part_copy(d, c).wait_send()
            across(0, d).wait_send()

        @pl.when(has_next)
        def _():
            rim_copy().wait_send()
            along(0).wait_send()
            along(1).wait_send()

        for e in range(1, sp_count):

            @pl.when(sp + e < sp_count)
            def _(e=e):
                carry_copy(e).wait_send()
                if e > 2:
                    direct(e).wait_send()

            @pl.when(sp >= e)
            def _(e=e):
                for d in range(1, tp_count):
                    across(e, d).wait_send()

        if sp_count > 2:

            @pl.when((sp >= 1) & has_next)
            def _():
                forward(0).wait_send()
                forward(1).wait_send()


def body(
    tokens, norm_gain, recurrent_input, recurrent_gate, attention_gate, query_proj, latent_down,
    rope_key_down, conv_kernel, recurrence_gate_blocks, input_gate_blocks, decay_rate, decay_shift,
    initial_state, latent_gain, latent_up, query_gain, recurrent_output, attention_output,
):
    tp_count = lax.axis_size("tp")
    sp_count = lax.axis_size("sp")
    share, model = tokens.shape
    rows = share * tp_count
    width = recurrent_input.shape[1]
    taken = attention_gate.shape[1]
    head_dim = query_gain.shape[0]
    heads = query_proj.shape[1] // head_dim
    value = taken // heads
    lat = latent_down.shape[1]
    rope = rope_key_down.shape[1]
    cosine, sine = rotary_tables(sp_count * rows, rope)
    key_table = np.concatenate([cosine, cosine, -sine, sine], 1).reshape(-1, share, 2 * rope)
    query_table = np.concatenate([cosine, sine], 1).reshape(sp_count, rows, rope).transpose(0, 2, 1)
    hbm = [
        tokens, latent_down, norm_gain[None], rope_key_down.T, jnp.asarray(key_table),
        recurrent_input, query_proj, query_gain[None], jnp.asarray(query_table), conv_kernel,
        recurrence_gate_blocks, input_gate_blocks, decay_rate[None], decay_shift[None],
        recurrent_gate, attention_gate, latent_gain[None], latent_up, initial_state[None],
        recurrent_output, attention_output,
    ]
    held = [a.shape for a in hbm]
    held[4] = key_table.shape[1:]
    held[8] = query_table.shape[1:]
    vmem = pltpu.VMEM
    dma = pltpu.SemaphoreType.DMA
    others = max(tp_count - 1, 1)
    hops = max(sp_count - 1, 1)
    carries = -(-2 * width // LANES // 8) * 8
    rims = -(-4 * width // LANES // 16) * 16
    pieces = 4 if share % 64 == 0 else 1
    chunks = 4 if model % (4 * LANES) == 0 else 1
    return pl.pallas_call(
        functools.partial(layer_kernel, sp_count, tp_count),
        out_shape=pltpu.VMEM((share, model), BF16),
        in_specs=[pl.BlockSpec(memory_space=pl.ANY)] * len(hbm),
        out_specs=pl.BlockSpec(memory_space=pltpu.VMEM),
        scratch_shapes=[vmem(s, a.dtype) for s, a in zip(held, hbm)]
        + [
            vmem((others, share, model), BF16),
            vmem((rows, model), BF16),
            vmem((sp_count, tp_count, rows + share * rope // lat, lat), BF16),
            vmem((rows, width), BF16),
            vmem((rows, width), BF16),
            vmem((rows, taken), BF16),
            vmem((query_proj.shape[1], rows), BF16),
            vmem((heads, head_dim, rows), BF16),
            vmem((rims, LANES), BF16),
            vmem((rims, LANES), BF16),
            vmem((rows + 24, width), F32),
            vmem((LANES, LANES), BF16),
            vmem((LANES, LANES), BF16),
            vmem((rows, rows), BF16),
            vmem((rows, rows), BF16),
            vmem((rows, LANES), F32),
            vmem((rows, width), F32),
            vmem((rows, width), BF16),
            vmem((width // LANES, rows, LANES), F32),
            vmem((width // LANES, rows, LANES), F32),
            vmem((16, width), F32),
            vmem((carries, LANES), F32),
            vmem((hops, carries, LANES), F32),
            vmem((rows, width), BF16),
            vmem((rows, model), F32),
            vmem((rows, lat * tp_count), BF16),
            vmem((rows, rope), BF16),
            vmem((rows, latent_up.shape[1]), BF16),
            vmem((heads, rows, rows), F32),
            vmem((heads, 8, rows), F32),
            vmem((heads, 8, rows), F32),
            vmem((heads, value, rows), F32),
            vmem((rows, taken), BF16),
            vmem((others, chunks, share, model // chunks), BF16),
            vmem((chunks, share, model // chunks), BF16),
            vmem((others, chunks, share, model // chunks), BF16),
            dma((len(hbm),)),
            dma((pieces,)),
            dma((others, pieces)), dma((others, pieces)),
            dma((2,)), dma((2,)),
            dma((2,)), dma((2,)),
            dma((hops,)), dma((hops,)),
            dma((sp_count, others)), dma((sp_count, others)),
            dma, dma,
            dma((hops,)), dma((hops,)),
            dma((others, chunks)), dma((others, chunks)),
            pltpu.SemaphoreType.REGULAR((hops,)),
        ],
        compiler_params=pltpu.CompilerParams(
            collective_id=0, has_side_effects=True, vmem_limit_bytes=61400 * 1024
        ),
    )(*hbm)


def solution(mesh):
    return jax.shard_map(
        body,
        mesh=mesh,
        in_specs=(
            P(("fs", "sp", "tp"), None),
            P(),
            P(None, "tp"),
            P(None, "tp"),
            P(None, "tp"),
            P(None, "tp"),
            P(None, "tp"),
            P(),
            P(None, "tp"),
            P("tp", None, None),
            P("tp", None, None),
            P("tp"),
            P(("fs", "sp")),
            P(("fs", "tp")),
            P(),
            P(None, "tp"),
            P(),
            P("tp", None),
            P("tp", None),
        ),
        out_specs=P(("fs", "sp", "tp"), None),
        check_vma=False,
    )
```

```python
import functools

import jax
import jax.numpy as jnp
import numpy as np
from jax import lax
from jax.experimental import pallas as pl
from jax.experimental.pallas import tpu as pltpu
from jax.sharding import PartitionSpec as P

EPS = 1e-06
RECURRENT_SCALE = 8.0
THETA = 10000.0
F32 = jnp.float32
BF16 = jnp.bfloat16
LANES = 128


def expm1_neg(y, root):
    small = y * (1.0 + y * (0.5 + y * (1.0 / 6 + y * (1.0 / 24 + y / 120))))
    return jnp.where(y > -0.1, small, root * root - 1.0)


def block_diagonal(scratch, blocks_ref, first):
    size = blocks_ref.shape[1]
    scratch[...] = jnp.zeros_like(scratch)
    for k in range(scratch.shape[0] // size):
        scratch[k * size : (k + 1) * size, k * size : (k + 1) * size] = blocks_ref[first + k]
    return scratch[...]


def scan_rows(decay, state):
    rows = decay.shape[0]
    row = lax.broadcasted_iota(jnp.int32, decay.shape, 0)
    step = 1
    while step < rows:
        inside = row >= step
        before_decay = jnp.where(inside, pltpu.roll(decay, step, 0), 1.0)
        before_state = jnp.where(inside, pltpu.roll(state, step, 0), 0.0)
        state = state + decay * before_state
        decay = decay * before_decay
        step *= 2
    return decay, state


def rms_scaled(values, gain_vec):
    return values * lax.rsqrt(jnp.mean(values * values, axis=-1, keepdims=True) + EPS) * gain_vec


LOG2E = 1.4426950408889634


def rotary_tables(positions, width):
    inv_freq = (1.0 / THETA ** (np.arange(0, width, 2, dtype=np.float32) / width)).astype(np.float32)
    angles = np.arange(positions, dtype=np.float32)[:, None] * inv_freq[None, :]
    cosine = np.cos(angles.astype(np.float64)).astype(np.float32)
    sine = np.sin(angles.astype(np.float64)).astype(np.float32)
    return cosine, sine


def column_step(width):
    return 256 if width % 256 == 0 else width


def remote(src, dst, send, recv, **where):
    return pltpu.make_async_remote_copy(
        src_ref=src, dst_ref=dst, send_sem=send, recv_sem=recv,
        device_id=where, device_id_type=pl.DeviceIdType.MESH,
    )


def scope(name):
    return jax.named_scope(name)


def layer_kernel(
    sp_count, tp_count,
    h_tokens, h_lat, h_norm, h_rope, h_ktab, h_in, h_query, h_qgain, h_qtab, h_conv, h_rec, h_inp,
    h_rate, h_shift, h_gate, h_att, h_lgain, h_up, h_init, h_rout, h_aout,
    out,
    tokens, w_lat, norm_gain, w_rope, key_table, w_in, w_query, query_gain, query_table,
    conv_kernel, rec_blocks, inp_blocks, decay_rate, decay_shift, w_gate, w_att, latent_gain,
    w_up, initial_state, w_rout, w_aout,
    tok_all, normed, lat_all, sig, gate, attp, turned_q, queries, rim_out, rim_in, ext, diag_a, diag_b,
    mixer, unmixer, shift, silu_gate, mixed_rout,
    prod, state, segments, car_out, car_in, rout, racc, xlat, rope_keys, turned_v, kv, held, row_max, row_sum,
    acc, aout, part, own_part, part_in,
    w_sem, tok_sem, tok_s, tok_r, z_s, z_r, y_s, y_r, fwd_s, fwd_r, l_s, l_r, x_s, x_r, rim_s, rim_r, c_s, c_r,
    p_s, p_r, ready,
):
    sp = lax.axis_index("sp")
    tp = lax.axis_index("tp")
    share, model = tokens.shape
    rows = normed.shape[0]
    taps, width = conv_kernel.shape
    head_dim = query_gain.shape[1]
    rope = w_rope.shape[0]
    half = rope // 2
    nope = head_dim - rope
    heads = w_query.shape[1] // head_dim
    lat = w_lat.shape[1]
    value = w_att.shape[1] // heads
    packed = lat // rope
    tall = share // packed
    pieces = tok_s.shape[1]
    piece = share // pieces
    long = rows // 8

    h_refs = (
        h_tokens, h_lat, h_norm, h_rope, h_ktab.at[sp * tp_count + tp], h_in, h_query, h_qgain,
        h_qtab.at[sp], h_conv, h_rec, h_inp, h_rate, h_shift, h_gate, h_att, h_lgain, h_up,
        h_init, h_rout, h_aout,
    )
    w_refs = (
        tokens, w_lat, norm_gain, w_rope, key_table, w_in, w_query, query_gain, query_table,
        conv_kernel, rec_blocks, inp_blocks, decay_rate, decay_shift, w_gate, w_att, latent_gain,
        w_up, initial_state, w_rout, w_aout,
    )
    loads = [
        pltpu.make_async_copy(a, b, w_sem.at[k]) for k, (a, b) in enumerate(zip(h_refs, w_refs)) if k
    ]
    token_loads = [
        pltpu.make_async_copy(
            h_tokens.at[pl.ds(k * piece, piece)], tokens.at[pl.ds(k * piece, piece)], tok_sem.at[k]
        )
        for k in range(pieces)
    ]

    def peer(d):
        return lax.rem(tp + d, tp_count)

    def source(d):
        return lax.rem(tp - d + tp_count, tp_count)

    def greet(sem, **where):
        pl.semaphore_signal(sem, inc=1, device_id=where, device_id_type=pl.DeviceIdType.MESH)

    barrier = pltpu.get_barrier_semaphore()
    with scope("a_loads"):
        for d in range(1, tp_count):
            greet(barrier, tp=peer(d))
        for e in range(1, sp_count):
            pl.when(sp + e < sp_count)(lambda e=e: greet(barrier, sp=sp + e))
        for load in [loads[1], *token_loads, loads[0]]:
            load.start()
    (
        l_lat, l_norm, l_rope, l_ktab, l_in, l_query, l_qgain, l_qtab, l_conv, l_rec, l_inp,
        l_rate, l_shift, l_gate, l_att, l_lgain, l_up, l_init, l_rout, l_aout,
    ) = loads

    def token_copy(d, k):
        part_rows = pl.ds(k * piece, piece)
        return remote(
            h_tokens.at[part_rows], tok_all.at[d - 1, part_rows],
            tok_s.at[d - 1, k], tok_r.at[d - 1, k], tp=peer(d),
        )

    with scope("b_barrier"):
        pl.semaphore_wait(barrier, tp_count - 1 + sp)
        for k in range(pieces):
            for d in range(1, tp_count):
                token_copy(d, k).start()
        for e in range(1, sp_count):
            pl.when(sp >= e)(lambda e=e: greet(ready.at[e - 1], sp=sp - e))
        for load in (loads[2], loads[3], loads[4], loads[5]):
            load.start()

    def share_rows(place):
        return pl.ds(pl.multiple_of(place * share, share), share)

    def put_normed(block, place):
        normed[share_rows(place)] = rms_scaled(block.astype(F32), norm_gain[...]).astype(BF16)

    def put_latent(first, place):
        own[first : first + share] = jnp.dot(
            normed[share_rows(place)], w_lat[...], preferred_element_type=F32
        ).astype(BF16)

    def project(weight, into, here=slice(None)):
        step = column_step(weight.shape[1])
        for c in range(weight.shape[1] // step):
            cols = slice(c * step, (c + 1) * step)
            into[here, cols] = jnp.dot(
                normed[here], weight[:, cols], preferred_element_type=F32
            ).astype(BF16)

    own = lat_all.at[sp, tp]
    with scope("c_norm_own"):
        l_norm.wait()
        for k in range(pieces):
            token_loads[k].wait()
        put_normed(tokens[...], tp)
    with scope("d_lat_a"):
        l_lat.wait()
        put_latent(0, tp)

    def along(k):
        block = lat_all.at[sp, tp, (pl.ds(0, share), pl.ds(share, rows + tall - share))[k]]
        return remote(block, block, z_s.at[k], z_r.at[k], sp=sp + 1)

    def landed(k):
        block = lat_all.at[sp - 1, tp, (pl.ds(0, share), pl.ds(share, rows + tall - share))[k]]
        return remote(block, block, z_s.at[k], z_r.at[k], sp=sp - 1)

    def direct(e):
        block = lat_all.at[sp, tp]
        return remote(block, block, fwd_s.at[e - 2], fwd_r.at[e - 2], sp=sp + e)

    def forward(k):
        block = lat_all.at[sp - 1, tp, (pl.ds(0, share), pl.ds(share, rows + tall - share))[k]]
        return remote(block, block, y_s.at[k], y_r.at[k], sp=sp + 1)

    def forwarded(k):
        block = lat_all.at[sp - 2, tp, (pl.ds(0, share), pl.ds(share, rows + tall - share))[k]]
        return remote(block, block, y_s.at[k], y_r.at[k], sp=sp - 1)

    def arrived(e):
        block = lat_all.at[sp - e, tp]
        return remote(block, block, fwd_s.at[e - 2], fwd_r.at[e - 2], sp=sp - 1)

    def across(e, d):
        block = lat_all.at[sp - e, tp]
        return remote(block, block, l_s.at[e, d - 1], l_r.at[e, d - 1], tp=peer(d))

    def crossed(e, d):
        block = lat_all.at[sp - e, source(d)]
        return remote(block, block, l_s.at[e, d - 1], l_r.at[e, d - 1], tp=source(d))

    def halves(k):
        return (pl.ds(0, share), pl.ds(share, rows + tall - share))[k]

    def across_piece(k, d):
        block = lat_all.at[sp - 2, tp, halves(k)]
        return remote(block, block, x_s.at[k, d - 1], x_r.at[k, d - 1], tp=peer(d))

    def crossed_piece(k, d):
        block = lat_all.at[sp - 2, source(d), halves(k)]
        return remote(block, block, x_s.at[k, d - 1], x_r.at[k, d - 1], tp=source(d))

    def cross(e):
        for d in range(1, tp_count):
            across(e, d).start()

    def wait_crossed(e):
        for d in range(1, tp_count):
            crossed(e, d).wait_recv()

    has_next = sp + 1 < sp_count
    with scope("f_send_a"):

        @pl.when(has_next)
        def _():
            pl.semaphore_wait(ready.at[0], 1)
            along(0).start()

    with scope("e_mixers"):
        row = lax.broadcasted_iota(jnp.int32, (rows, rows), 0)
        column = lax.broadcasted_iota(jnp.int32, (rows, rows), 1)
        mixer[...] = jnp.where(column == (row & 7) * long + (row >> 3), 1.0, 0.0).astype(BF16)
        unmixer[...] = jnp.where(row == (column & 7) * long + (column >> 3), 1.0, 0.0).astype(BF16)
    with scope("e_rope"):
        l_rope.wait()
        l_ktab.wait()
        raw = lax.dot_general(
            normed[share_rows(tp)], w_rope[...], (((1,), (1,)), ((), ())),
            preferred_element_type=F32,
        ).astype(BF16).astype(F32)
        swapped = jnp.concatenate([raw[:, half:], raw[:, :half]], axis=1)
        keyed = (raw * key_table[:, :rope] + swapped * key_table[:, rope:]).astype(BF16)
        for k in range(packed):
            own[share : share + tall, k * rope : (k + 1) * rope] = keyed[k * tall : (k + 1) * tall]
    with scope("g_norm_peer"):
        for k in range(pieces):
            for d in range(1, tp_count):
                token_copy(d, k).wait_recv()
        for d in range(1, tp_count):
            put_normed(tok_all[d - 1], source(d))
    def rim_copy():
        return remote(rim_out, rim_in, rim_s, rim_r, sp=sp + 1)

    def rim_landed():
        return remote(rim_out, rim_in, rim_s, rim_r, sp=sp - 1)

    with scope("i_lat_b"):
        for d in range(1, tp_count):
            put_latent(d * share + tall, source(d))
        pl.when(has_next)(lambda: along(1).start())
        cross(0)
    with scope("h_in_peer"):
        for load in loads[6:]:
            load.start()
        l_in.wait()
        project(w_in, sig)
        tail = sig[rows - 16 :].astype(F32)[12:]
        tail = [tail[:, c * LANES : (c + 1) * LANES] for c in range(width // LANES)]
        if len(tail) * 4 < rim_out.shape[0]:
            tail.append(jnp.zeros((rim_out.shape[0] - len(tail) * 4, LANES), F32))
        rim_out[...] = jnp.concatenate(tail, axis=0).astype(BF16)
        pl.when(has_next)(lambda: rim_copy().start())
    with scope("j_query"):
        l_query.wait()
        step = column_step(w_query.shape[1])
        for c in range(w_query.shape[1] // step):
            cols = slice(c * step, (c + 1) * step)
            raw = jnp.dot(normed[...], w_query[:, cols], preferred_element_type=F32).astype(BF16)
            turned_q[cols] = raw.T
    with scope("k_rotate"):
        l_qgain.wait()
        l_qtab.wait()
        spare = -head_dim % LANES
        gain = query_gain[...]
        if spare:
            gain = jnp.concatenate([gain, jnp.zeros((1, spare), F32)], axis=1)
        gain = jnp.broadcast_to(gain, (LANES, head_dim + spare)).T[:head_dim]
        gain = jnp.concatenate([gain] * (rows // LANES), axis=1)
        cosine = query_table[:half]
        sine = query_table[half:]
        for h in range(heads):
            head = turned_q[h * head_dim : (h + 1) * head_dim].astype(F32)
            square = jnp.sum(head * head, axis=0, keepdims=True)
            head = head * lax.rsqrt(square / head_dim + EPS) * gain
            first, second = head[nope : nope + half], head[nope + half :]
            queries[h, :nope] = head[:nope].astype(BF16)
            queries[h, nope : nope + half] = (first * cosine - second * sine).astype(BF16)
            queries[h, nope + half :] = (first * sine + second * cosine).astype(BF16)

    def relay1(k):
        if sp_count > 1:

            @pl.when(sp >= 1)
            def _():
                landed(k).wait_recv()
                if sp_count > 2:
                    pl.when(has_next)(lambda: forward(k).start())
                if k:
                    cross(1)

    with scope("p_relay1a"):
        relay1(0)

    with scope("q_gates"):
        l_gate.wait()
        project(w_gate, gate)
        silu_gate[...] = jax.nn.silu(
            jnp.dot(mixer[...], gate[...], preferred_element_type=F32)
        )

    with scope("l_direct"):
        for e in range(2, sp_count):

            @pl.when(sp + e < sp_count)
            def _(e=e):
                pl.semaphore_wait(ready.at[e - 1], 1)
                if e > 2:
                    direct(e).start()

    with scope("q_gate_att"):
        l_att.wait()
        project(w_att, attp)

    with scope("p_relay1b"):
        relay1(1)
    with scope("m_rim"):

        @pl.when(sp == 0)
        def _():
            rim_in[...] = jnp.zeros_like(rim_in)

        pl.when(sp > 0)(lambda: rim_landed().wait_recv())
    with scope("n_scan"):
        for load in (l_conv, l_rec, l_inp, l_rate, l_shift):
            load.wait()
        size = rec_blocks.shape[1]
        car_out[...] = jnp.zeros_like(car_out)
        lead = 8 * (taps - 1)
        ext[lead : lead + rows] = jnp.dot(mixer[...], sig[...], preferred_element_type=F32)
        top_row = lax.broadcasted_iota(jnp.int32, (8, width), 0) == 0
        rim = rim_in[...].astype(F32)
        rim = jnp.concatenate(
            [rim[4 * c : 4 * c + 4] for c in range(width // LANES)], axis=1
        )
        for k in range(1, taps):
            last = ext[lead + rows - 8 * k : lead + rows - 8 * k + 8]
            ext[lead - 8 * k : lead - 8 * k + 8] = jnp.where(
                top_row, rim[4 - k : 5 - k], pltpu.roll(last, 1, 0)
            )
        table = jnp.concatenate(
            [decay_shift[:, k * long : (k + 1) * long] for k in range(8)], axis=0
        )
        for i in range(long):
            shift[8 * i : 8 * i + 8] = jnp.broadcast_to(table[:, i : i + 1], (8, LANES))
        groups = width // LANES
        for c in range(groups):
            cols = slice(c * LANES, (c + 1) * LANES)
            conv = conv_kernel[0:1, cols] * ext[0:rows, cols]
            for j in range(1, taps):
                conv = conv + conv_kernel[j : j + 1, cols] * ext[8 * j : 8 * j + rows, cols]
            conv = conv.astype(BF16)
            per = LANES // size
            rec = jax.nn.sigmoid(
                jnp.dot(conv, block_diagonal(diag_a, rec_blocks, c * per), preferred_element_type=F32)
            )
            inp = jax.nn.sigmoid(
                jnp.dot(conv, block_diagonal(diag_b, inp_blocks, c * per), preferred_element_type=F32)
            )
            log_decay = -RECURRENT_SCALE * rec * decay_rate[0:1, cols] + shift[...]
            decay = jnp.exp(log_decay)
            prod[c] = decay
            state[c] = jnp.sqrt(-expm1_neg(2.0 * log_decay, decay)) * inp * conv.astype(F32)
        ones = [prod[c, 0:8] for c in range(groups)]
        twos = [state[c, 0:8] for c in range(groups)]
        for i in range(1, long):
            here = slice(8 * i, 8 * i + 8)
            for c in range(groups):
                decay = prod[c, here]
                twos[c] = decay * twos[c] + state[c, here]
                ones[c] = decay * ones[c]
                prod[c, here] = ones[c]
                state[c, here] = twos[c]
        first_row = lax.broadcasted_iota(jnp.int32, (8, LANES), 0) == 0
        for c in range(groups):
            cols = slice(c * LANES, (c + 1) * LANES)
            one, two = scan_rows(ones[c], twos[c])
            segments[0:8, cols] = jnp.where(first_row, 1.0, pltpu.roll(one, 1, 0))
            segments[8:16, cols] = jnp.where(first_row, 0.0, pltpu.roll(two, 1, 0))
            car_out[2 * c : 2 * c + 1] = one[7:8]
            car_out[2 * c + 1 : 2 * c + 2] = two[7:8]

    def carry_copy(e):
        return remote(car_out, car_in.at[e - 1], c_s.at[e - 1], c_r.at[e - 1], sp=sp + e)

    def carry_landed(e):
        return remote(car_out, car_in.at[e - 1], c_s.at[e - 1], c_r.at[e - 1], sp=sp - e)

    with scope("o_carry"):
        for e in range(1, sp_count):
            pl.when(sp + e < sp_count)(lambda e=e: carry_copy(e).start())
    factor = head_dim ** (-0.5) * LOG2E

    def prepare(e):
        place = sp - e
        blocks = []
        for n in range(tp_count):
            order = [(n - r) % tp_count for r in range(tp_count)]
            first = [0 if j == 0 else tall + j * share for j in order]
            blocks.append(
                jnp.concatenate([lat_all[place, n, f : f + share] for f in first], axis=0).astype(F32)
            )
        square = sum(jnp.sum(x * x, axis=-1, keepdims=True) for x in blocks)
        inverse = lax.rsqrt(square / (lat * tp_count) + EPS)
        for n, x in enumerate(blocks):
            cols = slice(n * lat, (n + 1) * lat)
            xlat[:, cols] = (x * inverse * latent_gain[0:1, cols]).astype(BF16)
        rope_keys[...] = jnp.concatenate(
            [
                lat_all[place, n, share : share + tall, k * rope : (k + 1) * rope]
                for n in range(tp_count)
                for k in range(packed)
            ],
            axis=0,
        )
        step = column_step(w_up.shape[1])
        for c in range(w_up.shape[1] // step):
            cols = slice(c * step, (c + 1) * step)
            kv[:, cols] = jnp.dot(xlat[...], w_up[:, cols], preferred_element_type=F32).astype(BF16)
        for h in range(heads):
            base = h * (nope + value) + nope
            turned_v[h] = kv[:, base : base + value].T

    def score(h, diagonal, lanes, count):
        base = h * (nope + value)
        keys = jnp.concatenate([kv[:, base : base + nope], rope_keys[...]], axis=1)
        scores = jnp.dot(keys, queries[h, :, lanes], preferred_element_type=F32) * factor
        if diagonal:
            seen = lax.broadcasted_iota(jnp.int32, scores.shape, 0)
            scores = jnp.where(
                seen <= lax.broadcasted_iota(jnp.int32, scores.shape, 1), scores, -jnp.inf
            )
        held[h, :, :count] = scores
        return jnp.max(scores, axis=0, keepdims=True)

    def mix(h, top, diagonal, lanes, count):
        if not diagonal:
            before = row_max[h, 0:1, lanes]
            top = jnp.maximum(top, before)
            fade = jnp.exp2(before - top)
        weights = jnp.exp2(held[h, :, :count] - top)
        mass = jnp.sum(weights, axis=0, keepdims=True)
        term = jnp.dot(turned_v[h], weights.astype(BF16), preferred_element_type=F32)
        if not diagonal:
            mass = mass + row_sum[h, 0:1, lanes] * fade
            term = term + acc[h, :, lanes] * fade
        row_max[h, 0:1, lanes] = top
        row_sum[h, 0:1, lanes] = mass
        acc[h, :, lanes] = term

    def heads_over(diagonal, lanes=slice(None), count=rows):
        tops = [score(h, diagonal, lanes, count) for h in range(heads)]
        for h in range(heads):
            mix(h, tops[h], diagonal, lanes, count)

    def attend(e, diagonal):
        prepare(e)
        heads_over(diagonal)

    with scope("r_att0"):
        l_lgain.wait()
        l_up.wait()
        wait_crossed(0)
        prepare(0)
    with scope("r_att0_heads"):
        heads_over(True)
    with scope("t_relay3"):
        if sp_count > 3:

            @pl.when(sp >= 3)
            def _():
                arrived(3).wait_recv()
                cross(3)

    with scope("s_att1"):
        if sp_count > 1:

            @pl.when(sp >= 1)
            def _():
                wait_crossed(1)
                attend(1, False)

    with scope("w_att3"):
        if sp_count > 3:

            @pl.when(sp >= 3)
            def _():
                wait_crossed(3)
                attend(3, False)

        if sp_count > 4:

            def later(e, carry):
                block = lat_all.at[sp - e, tp]
                remote(block, block, fwd_s.at[e - 2], fwd_r.at[e - 2], sp=sp - 1).wait_recv()
                cross(e)
                wait_crossed(e)
                attend(e, False)
                return carry

            lax.fori_loop(4, sp + 1, later, 0)
    with scope("x_relay2"):
        if sp_count > 2:

            @pl.when(sp >= 2)
            def _():
                for k in range(2):
                    forwarded(k).wait_recv()
                    for d in range(1, tp_count):
                        across_piece(k, d).start()

    with scope("u_carrywait"):
        for e in range(1, sp_count):

            @pl.when(sp >= e)
            def _(e=e):
                carry_landed(e).wait_recv()

            @pl.when(sp < e)
            def _(e=e):
                row = lax.broadcasted_iota(jnp.int32, car_out.shape, 0)
                car_in[e - 1] = jnp.where((row & 1) == 0, 1.0, 0.0)

    with scope("v_rout"):
        l_init.wait()
        for c in range(width // LANES):
            cols = slice(c * LANES, (c + 1) * LANES)
            incoming = initial_state[:, cols]
            for e in range(sp_count - 1, 0, -1):
                incoming = (
                    car_in[e - 1, 2 * c : 2 * c + 1] * incoming
                    + car_in[e - 1, 2 * c + 1 : 2 * c + 2]
                )
            enter = segments[0:8, cols] * incoming + segments[8:16, cols]
            full = state[c] + prod[c] * jnp.concatenate([enter] * long, axis=0)
            mixed_rout[:, cols] = (full * silu_gate[:, cols]).astype(BF16)
        rout[...] = jnp.dot(
            unmixer[...], mixed_rout[...], preferred_element_type=F32
        ).astype(BF16)
        l_rout.wait()
        step = column_step(model)
        for c in range(model // step):
            cols = slice(c * step, (c + 1) * step)
            racc[:, cols] = jnp.dot(rout[...], w_rout[:, cols], preferred_element_type=F32)
    chunks, step = part_in.shape[1], part_in.shape[3]
    split = share % LANES == 0

    def part_copy(d, c):
        return remote(
            part.at[d - 1, c], part_in.at[d - 1, c], p_s.at[d - 1, c], p_r.at[d - 1, c], tp=peer(d)
        )

    def partial(place, c):
        cols = slice(c * step, (c + 1) * step)
        here = share_rows(place)
        both = racc[here, cols] + jnp.dot(aout[here], w_aout[:, cols], preferred_element_type=F32)
        return both.astype(BF16)

    def finish(here):
        for h in range(heads):
            cols = slice(h * value, (h + 1) * value)
            attended = (acc[h, :, here] * (1.0 / row_sum[h, 0:1, here])).T
            aout[here, cols] = (attended * jax.nn.silu(attp[here, cols].astype(F32))).astype(BF16)

    def send(d, c):
        part[d - 1, c] = partial(peer(d), c)
        part_copy(d, c).start()

    def last_block():
        for k in range(2):
            for d in range(1, tp_count):
                crossed_piece(k, d).wait_recv()
        prepare(2)
        if not split:
            heads_over(False)
            finish(slice(None))
            for c in range(chunks):
                for d in range(1, tp_count):
                    send(d, c)
            for c in range(chunks):
                own_part[c] = partial(tp, c)
            return
        for d in range(1, tp_count):
            heads_over(False, share_rows(peer(d)), share)
            finish(share_rows(peer(d)))
        mine = share_rows(tp)
        sends = [(d, c) for d in range(1, tp_count) for c in range(chunks)]
        each = -(-2 * len(sends) // heads)
        tops = [score(h, False, mine, share) for h in range(heads)]
        for h in range(heads):
            for d, c in sends[h * each : (h + 1) * each]:
                send(d, c)
            mix(h, tops[h], False, mine, share)
        finish(mine)
        for c in range(chunks):
            own_part[c] = partial(tp, c)

    def no_block():
        finish(slice(None))
        for c in range(chunks):
            for d in range(1, tp_count):
                send(d, c)
        for c in range(chunks):
            own_part[c] = partial(tp, c)

    with scope("y_last"):
        l_aout.wait()
        if sp_count > 2:
            pl.when(sp >= 2)(last_block)
            pl.when(sp < 2)(no_block)
        else:
            no_block()
    with scope("z_sum"):
        for c in range(chunks):
            summed = own_part[c].astype(F32)
            for d in range(1, tp_count):
                part_copy(d, c).wait_recv()
                summed = summed + part_in[d - 1, c].astype(F32)
            out[:, c * step : (c + 1) * step] = summed.astype(BF16)

    with scope("z_waits"):
        for d in range(1, tp_count):
            for k in range(pieces):
                token_copy(d, k).wait_send()
            for c in range(chunks):
                part_copy(d, c).wait_send()
            across(0, d).wait_send()

        @pl.when(has_next)
        def _():
            rim_copy().wait_send()
            along(0).wait_send()
            along(1).wait_send()

        for e in range(1, sp_count):

            @pl.when(sp + e < sp_count)
            def _(e=e):
                carry_copy(e).wait_send()
                if e > 2:
                    direct(e).wait_send()

            @pl.when(sp >= e)
            def _(e=e):
                for d in range(1, tp_count):
                    if e == 2:
                        across_piece(0, d).wait_send()
                        across_piece(1, d).wait_send()
                    else:
                        across(e, d).wait_send()

        if sp_count > 2:

            @pl.when((sp >= 1) & has_next)
            def _():
                forward(0).wait_send()
                forward(1).wait_send()


def body(
    tokens, norm_gain, recurrent_input, recurrent_gate, attention_gate, query_proj, latent_down,
    rope_key_down, conv_kernel, recurrence_gate_blocks, input_gate_blocks, decay_rate, decay_shift,
    initial_state, latent_gain, latent_up, query_gain, recurrent_output, attention_output,
):
    tp_count = lax.axis_size("tp")
    sp_count = lax.axis_size("sp")
    share, model = tokens.shape
    rows = share * tp_count
    width = recurrent_input.shape[1]
    taken = attention_gate.shape[1]
    head_dim = query_gain.shape[0]
    heads = query_proj.shape[1] // head_dim
    value = taken // heads
    lat = latent_down.shape[1]
    rope = rope_key_down.shape[1]
    cosine, sine = rotary_tables(sp_count * rows, rope)
    key_table = np.concatenate([cosine, cosine, -sine, sine], 1).reshape(-1, share, 2 * rope)
    query_table = np.concatenate([cosine, sine], 1).reshape(sp_count, rows, rope).transpose(0, 2, 1)
    hbm = [
        tokens, latent_down, norm_gain[None], rope_key_down.T, jnp.asarray(key_table),
        recurrent_input, query_proj, query_gain[None], jnp.asarray(query_table), conv_kernel,
        recurrence_gate_blocks, input_gate_blocks, decay_rate[None], decay_shift[None],
        recurrent_gate, attention_gate, latent_gain[None], latent_up, initial_state[None],
        recurrent_output, attention_output,
    ]
    held = [a.shape for a in hbm]
    held[4] = key_table.shape[1:]
    held[8] = query_table.shape[1:]
    vmem = pltpu.VMEM
    dma = pltpu.SemaphoreType.DMA
    others = max(tp_count - 1, 1)
    hops = max(sp_count - 1, 1)
    carries = -(-2 * width // LANES // 8) * 8
    rims = -(-4 * width // LANES // 16) * 16
    pieces = 4 if share % 64 == 0 else 1
    chunks = 4 if model % (4 * LANES) == 0 else 1
    return pl.pallas_call(
        functools.partial(layer_kernel, sp_count, tp_count),
        out_shape=pltpu.VMEM((share, model), BF16),
        in_specs=[pl.BlockSpec(memory_space=pl.ANY)] * len(hbm),
        out_specs=pl.BlockSpec(memory_space=pltpu.VMEM),
        scratch_shapes=[vmem(s, a.dtype) for s, a in zip(held, hbm)]
        + [
            vmem((others, share, model), BF16),
            vmem((rows, model), BF16),
            vmem((sp_count, tp_count, rows + share * rope // lat, lat), BF16),
            vmem((rows, width), BF16),
            vmem((rows, width), BF16),
            vmem((rows, taken), BF16),
            vmem((query_proj.shape[1], rows), BF16),
            vmem((heads, head_dim, rows), BF16),
            vmem((rims, LANES), BF16),
            vmem((rims, LANES), BF16),
            vmem((rows + 24, width), F32),
            vmem((LANES, LANES), BF16),
            vmem((LANES, LANES), BF16),
            vmem((rows, rows), BF16),
            vmem((rows, rows), BF16),
            vmem((rows, LANES), F32),
            vmem((rows, width), F32),
            vmem((rows, width), BF16),
            vmem((width // LANES, rows, LANES), F32),
            vmem((width // LANES, rows, LANES), F32),
            vmem((16, width), F32),
            vmem((carries, LANES), F32),
            vmem((hops, carries, LANES), F32),
            vmem((rows, width), BF16),
            vmem((rows, model), F32),
            vmem((rows, lat * tp_count), BF16),
            vmem((rows, rope), BF16),
            vmem((heads, value, rows), BF16),
            vmem((rows, latent_up.shape[1]), BF16),
            vmem((heads, rows, rows), F32),
            vmem((heads, 8, rows), F32),
            vmem((heads, 8, rows), F32),
            vmem((heads, value, rows), F32),
            vmem((rows, taken), BF16),
            vmem((others, chunks, share, model // chunks), BF16),
            vmem((chunks, share, model // chunks), BF16),
            vmem((others, chunks, share, model // chunks), BF16),
            dma((len(hbm),)),
            dma((pieces,)),
            dma((others, pieces)), dma((others, pieces)),
            dma((2,)), dma((2,)),
            dma((2,)), dma((2,)),
            dma((hops,)), dma((hops,)),
            dma((sp_count, others)), dma((sp_count, others)),
            dma((2, others)), dma((2, others)),
            dma, dma,
            dma((hops,)), dma((hops,)),
            dma((others, chunks)), dma((others, chunks)),
            pltpu.SemaphoreType.REGULAR((hops,)),
        ],
        compiler_params=pltpu.CompilerParams(
            collective_id=0, has_side_effects=True, vmem_limit_bytes=61400 * 1024
        ),
    )(*hbm)


def solution(mesh):
    return jax.shard_map(
        body,
        mesh=mesh,
        in_specs=(
            P(("fs", "sp", "tp"), None),
            P(),
            P(None, "tp"),
            P(None, "tp"),
            P(None, "tp"),
            P(None, "tp"),
            P(None, "tp"),
            P(),
            P(None, "tp"),
            P("tp", None, None),
            P("tp", None, None),
            P("tp"),
            P(("fs", "sp")),
            P(("fs", "tp")),
            P(),
            P(None, "tp"),
            P(),
            P("tp", None),
            P("tp", None),
        ),
        out_specs=P(("fs", "sp", "tp"), None),
        check_vma=False,
    )
```

```python
import functools

import jax
import jax.numpy as jnp
import numpy as np
from jax import lax
from jax.experimental import pallas as pl
from jax.experimental.pallas import tpu as pltpu
from jax.sharding import PartitionSpec as P

EPS = 1e-06
RECURRENT_SCALE = 8.0
THETA = 10000.0
F32 = jnp.float32
BF16 = jnp.bfloat16
LANES = 128


def expm1_neg(y, root):
    small = y * (1.0 + y * (0.5 + y * (1.0 / 6 + y * (1.0 / 24 + y / 120))))
    return jnp.where(y > -0.1, small, root * root - 1.0)


def block_diagonal(scratch, blocks_ref, first):
    size = blocks_ref.shape[1]
    scratch[...] = jnp.zeros_like(scratch)
    for k in range(scratch.shape[0] // size):
        scratch[k * size : (k + 1) * size, k * size : (k + 1) * size] = blocks_ref[first + k]
    return scratch[...]


def scan_rows(decay, state):
    rows = decay.shape[0]
    row = lax.broadcasted_iota(jnp.int32, decay.shape, 0)
    step = 1
    while step < rows:
        inside = row >= step
        before_decay = jnp.where(inside, pltpu.roll(decay, step, 0), 1.0)
        before_state = jnp.where(inside, pltpu.roll(state, step, 0), 0.0)
        state = state + decay * before_state
        decay = decay * before_decay
        step *= 2
    return decay, state


def rms_scaled(values, gain_vec):
    return values * lax.rsqrt(jnp.mean(values * values, axis=-1, keepdims=True) + EPS) * gain_vec


LOG2E = 1.4426950408889634


def rotary_tables(positions, width):
    inv_freq = (1.0 / THETA ** (np.arange(0, width, 2, dtype=np.float32) / width)).astype(np.float32)
    angles = np.arange(positions, dtype=np.float32)[:, None] * inv_freq[None, :]
    cosine = np.cos(angles.astype(np.float64)).astype(np.float32)
    sine = np.sin(angles.astype(np.float64)).astype(np.float32)
    return cosine, sine


def column_step(width):
    return 256 if width % 256 == 0 else width


def remote(src, dst, send, recv, **where):
    return pltpu.make_async_remote_copy(
        src_ref=src, dst_ref=dst, send_sem=send, recv_sem=recv,
        device_id=where, device_id_type=pl.DeviceIdType.MESH,
    )


def scope(name):
    return jax.named_scope(name)


def layer_kernel(
    sp_count, tp_count,
    h_tokens, h_lat, h_norm, h_rope, h_ktab, h_in, h_query, h_qgain, h_qtab, h_conv, h_rec, h_inp,
    h_rate, h_shift, h_gate, h_att, h_lgain, h_up, h_init, h_rout, h_aout,
    out,
    tokens, w_lat, norm_gain, w_rope, key_table, w_in, w_query, query_gain, query_table,
    conv_kernel, rec_blocks, inp_blocks, decay_rate, decay_shift, w_gate, w_att, latent_gain,
    w_up, initial_state, w_rout, w_aout,
    tok_all, normed, lat_all, sig, gate, attp, turned_q, queries, rim_out, rim_in, ext, diag_a, diag_b,
    mixer, unmixer, shift, silu_gate, mixed_rout,
    prod, state, segments, car_out, car_in, rout, racc, xlat, rope_keys, turned_v, kv, held, row_max, row_sum,
    acc, aout, part, own_part, part_in,
    w_sem, tok_s, tok_r, z_s, z_r, y_s, y_r, fwd_s, fwd_r, l_s, l_r, x_r, rim_s, rim_r, c_s, c_r,
    p_s, p_r, ready,
):
    sp = lax.axis_index("sp")
    tp = lax.axis_index("tp")
    share, model = tokens.shape
    rows = normed.shape[0]
    taps, width = conv_kernel.shape
    head_dim = query_gain.shape[1]
    rope = w_rope.shape[0]
    half = rope // 2
    nope = head_dim - rope
    heads = w_query.shape[1] // head_dim
    lat = w_lat.shape[1]
    value = w_att.shape[1] // heads
    packed = lat // rope
    tall = share // packed
    pieces = 4 if share % 64 == 0 else 1
    piece = share // pieces
    long = rows // 8

    h_refs = (
        h_tokens, h_lat, h_norm, h_rope, h_ktab.at[sp * tp_count + tp], h_in, h_query, h_qgain,
        h_qtab.at[sp], h_conv, h_rec, h_inp, h_rate, h_shift, h_gate, h_att, h_lgain, h_up,
        h_init, h_rout, h_aout,
    )
    w_refs = (
        tokens, w_lat, norm_gain, w_rope, key_table, w_in, w_query, query_gain, query_table,
        conv_kernel, rec_blocks, inp_blocks, decay_rate, decay_shift, w_gate, w_att, latent_gain,
        w_up, initial_state, w_rout, w_aout,
    )
    slots = (1, 2, 0, 3, 4, 5, 6, 0, 1, 4, 5, 0, 1, 6, 2, 3, 9, 7, 2, 3, 8)
    loads = [
        pltpu.make_async_copy(a, b, w_sem.at[k]) for a, b, k in zip(h_refs, w_refs, slots)
    ]
    token_loads = [
        pltpu.make_async_copy(
            h_tokens.at[pl.ds(k * piece, piece)], tokens.at[pl.ds(k * piece, piece)], w_sem.at[1]
        )
        for k in range(pieces)
    ]

    def peer(d):
        return lax.rem(tp + d, tp_count)

    def source(d):
        return lax.rem(tp - d + tp_count, tp_count)

    def greet(sem, **where):
        pl.semaphore_signal(sem, inc=1, device_id=where, device_id_type=pl.DeviceIdType.MESH)

    (
        l_tok, l_lat, l_norm, l_rope, l_ktab, l_in, l_query, l_qgain, l_qtab, l_conv, l_rec, l_inp,
        l_rate, l_shift, l_gate, l_att, l_lgain, l_up, l_init, l_rout, l_aout,
    ) = loads
    barrier = pltpu.get_barrier_semaphore()
    with scope("a_loads"):
        for d in range(1, tp_count):
            greet(barrier, tp=peer(d))
        for e in range(1, sp_count):
            pl.when(sp + e < sp_count)(lambda e=e: greet(barrier, sp=sp + e))
        l_norm.start()
        for load in token_loads:
            load.start()
        l_lat.start()

    def token_copy(d, k):
        part_rows = pl.ds(k * piece, piece)
        return remote(
            h_tokens.at[part_rows], tok_all.at[d - 1, part_rows],
            tok_s.at[d - 1], tok_r.at[d - 1], tp=peer(d),
        )

    def token_whole(d):
        return remote(h_tokens, tok_all.at[d - 1], tok_s.at[d - 1], tok_r.at[d - 1], tp=peer(d))

    with scope("b_barrier"):
        pl.semaphore_wait(barrier, tp_count - 1 + sp)
        for k in range(pieces):
            for d in range(1, tp_count):
                token_copy(d, k).start()
        for e in range(1, sp_count):
            pl.when(sp >= e)(lambda e=e: greet(ready.at[e - 1], sp=sp - e))
        for load in (l_rope, l_ktab, l_in, l_query):
            load.start()

    def share_rows(place):
        return pl.ds(pl.multiple_of(place * share, share), share)

    def put_normed(block, place):
        normed[share_rows(place)] = rms_scaled(block.astype(F32), norm_gain[...]).astype(BF16)

    def put_latent(first, place):
        own[first : first + share] = jnp.dot(
            normed[share_rows(place)], w_lat[...], preferred_element_type=F32
        ).astype(BF16)

    def project(weight, into, here=slice(None)):
        step = column_step(weight.shape[1])
        for c in range(weight.shape[1] // step):
            cols = slice(c * step, (c + 1) * step)
            into[here, cols] = jnp.dot(
                normed[here], weight[:, cols], preferred_element_type=F32
            ).astype(BF16)

    own = lat_all.at[sp, tp]
    with scope("c_norm_own"):
        l_norm.wait()
        l_tok.wait()
        put_normed(tokens[...], tp)
    with scope("d_lat_a"):
        l_lat.wait()
        put_latent(0, tp)

    def along(k):
        block = lat_all.at[sp, tp, (pl.ds(0, share), pl.ds(share, rows + tall - share))[k]]
        return remote(block, block, z_s, z_r.at[k], sp=sp + 1)

    def landed(k):
        block = lat_all.at[sp - 1, tp, (pl.ds(0, share), pl.ds(share, rows + tall - share))[k]]
        return remote(block, block, z_s, z_r.at[k], sp=sp - 1)

    def direct(e):
        block = lat_all.at[sp, tp]
        return remote(block, block, fwd_s.at[e - 3], fwd_r.at[e - 3], sp=sp + e)

    def forward(k):
        block = lat_all.at[sp - 1, tp, (pl.ds(0, share), pl.ds(share, rows + tall - share))[k]]
        return remote(block, block, y_s, y_r.at[k], sp=sp + 1)

    def forwarded(k):
        block = lat_all.at[sp - 2, tp, (pl.ds(0, share), pl.ds(share, rows + tall - share))[k]]
        return remote(block, block, y_s, y_r.at[k], sp=sp - 1)

    def arrived(e):
        block = lat_all.at[sp - e, tp]
        return remote(block, block, fwd_s.at[e - 3], fwd_r.at[e - 3], sp=sp - 1)

    def late(e):
        return e if isinstance(e, int) and e < 2 else e - 1

    def across(e, d):
        block = lat_all.at[sp - e, tp]
        return remote(block, block, l_s.at[d - 1], l_r.at[late(e), d - 1], tp=peer(d))

    def crossed(e, d):
        block = lat_all.at[sp - e, source(d)]
        return remote(block, block, l_s.at[d - 1], l_r.at[late(e), d - 1], tp=source(d))

    def halves(k):
        return (pl.ds(0, share), pl.ds(share, rows + tall - share))[k]

    def across_piece(k, d):
        block = lat_all.at[sp - 2, tp, halves(k)]
        return remote(block, block, l_s.at[d - 1], x_r.at[d - 1], tp=peer(d))

    def cross(e):
        for d in range(1, tp_count):
            across(e, d).start()

    def wait_crossed(e):
        for d in range(1, tp_count):
            crossed(e, d).wait_recv()

    has_next = sp + 1 < sp_count
    with scope("f_send_a"):

        @pl.when(has_next)
        def _():
            pl.semaphore_wait(ready.at[0], 1)
            along(0).start()

    with scope("e_mixers"):
        row = lax.broadcasted_iota(jnp.int32, (rows, rows), 0)
        column = lax.broadcasted_iota(jnp.int32, (rows, rows), 1)
        mixer[...] = jnp.where(column == (row & 7) * long + (row >> 3), 1.0, 0.0).astype(BF16)
        unmixer[...] = jnp.where(row == (column & 7) * long + (column >> 3), 1.0, 0.0).astype(BF16)
    with scope("e_rope"):
        l_rope.wait()
        l_ktab.wait()
        raw = lax.dot_general(
            normed[share_rows(tp)], w_rope[...], (((1,), (1,)), ((), ())),
            preferred_element_type=F32,
        ).astype(BF16).astype(F32)
        swapped = jnp.concatenate([raw[:, half:], raw[:, :half]], axis=1)
        keyed = (raw * key_table[:, :rope] + swapped * key_table[:, rope:]).astype(BF16)
        for k in range(packed):
            own[share : share + tall, k * rope : (k + 1) * rope] = keyed[k * tall : (k + 1) * tall]
    with scope("g_norm_peer"):
        for d in range(1, tp_count):
            token_whole(d).wait_recv()
            put_normed(tok_all[d - 1], source(d))
    def rim_copy():
        return remote(rim_out, rim_in, rim_s, rim_r, sp=sp + 1)

    def rim_landed():
        return remote(rim_out, rim_in, rim_s, rim_r, sp=sp - 1)

    with scope("i_lat_b"):
        for d in range(1, tp_count):
            put_latent(d * share + tall, source(d))
        pl.when(has_next)(lambda: along(1).start())
        cross(0)
    with scope("h_in_peer"):
        l_in.wait()
        for load in (l_qgain, l_qtab, l_gate, l_att, l_conv, l_rec, l_up, l_lgain, l_aout):
            load.start()
        project(w_in, sig)
        tail = sig[rows - 16 :].astype(F32)[12:]
        tail = [tail[:, c * LANES : (c + 1) * LANES] for c in range(width // LANES)]
        if len(tail) * 4 < rim_out.shape[0]:
            tail.append(jnp.zeros((rim_out.shape[0] - len(tail) * 4, LANES), F32))
        rim_out[...] = jnp.concatenate(tail, axis=0).astype(BF16)
        pl.when(has_next)(lambda: rim_copy().start())
    with scope("j_query"):
        l_query.wait()
        step = column_step(w_query.shape[1])
        for c in range(w_query.shape[1] // step):
            cols = slice(c * step, (c + 1) * step)
            raw = jnp.dot(normed[...], w_query[:, cols], preferred_element_type=F32).astype(BF16)
            turned_q[cols] = raw.T
    with scope("k_rotate"):
        l_qgain.wait()
        l_qtab.wait()
        spare = -head_dim % LANES
        gain = query_gain[...]
        if spare:
            gain = jnp.concatenate([gain, jnp.zeros((1, spare), F32)], axis=1)
        gain = jnp.broadcast_to(gain, (LANES, head_dim + spare)).T[:head_dim]
        gain = jnp.concatenate([gain] * (rows // LANES), axis=1)
        cosine = query_table[:half]
        sine = query_table[half:]
        for h in range(heads):
            head = turned_q[h * head_dim : (h + 1) * head_dim].astype(F32)
            square = jnp.sum(head * head, axis=0, keepdims=True)
            head = head * lax.rsqrt(square / head_dim + EPS) * gain
            first, second = head[nope : nope + half], head[nope + half :]
            queries[h, :nope] = head[:nope].astype(BF16)
            queries[h, nope : nope + half] = (first * cosine - second * sine).astype(BF16)
            queries[h, nope + half :] = (first * sine + second * cosine).astype(BF16)
        for load in (l_inp, l_rate, l_shift):
            load.start()

    def relay1(k):
        if sp_count > 1:

            @pl.when(sp >= 1)
            def _():
                landed(k).wait_recv()
                if sp_count > 2:
                    pl.when(has_next)(lambda: forward(k).start())
                if k:
                    cross(1)

    with scope("p_relay1a"):
        relay1(0)

    with scope("q_gates"):
        l_gate.wait()
        project(w_gate, gate)
        silu_gate[...] = jax.nn.silu(
            jnp.dot(mixer[...], gate[...], preferred_element_type=F32)
        )

    with scope("l_direct"):
        for e in range(2, sp_count):

            @pl.when(sp + e < sp_count)
            def _(e=e):
                pl.semaphore_wait(ready.at[e - 1], 1)
                if e > 2:
                    direct(e).start()

    with scope("q_gate_att"):
        l_att.wait()
        project(w_att, attp)
        for load in (l_init, l_rout):
            load.start()

    with scope("p_relay1b"):
        relay1(1)
    with scope("m_rim"):

        @pl.when(sp == 0)
        def _():
            rim_in[...] = jnp.zeros_like(rim_in)

        pl.when(sp > 0)(lambda: rim_landed().wait_recv())
    with scope("n_scan"):
        for load in (l_conv, l_rec, l_inp, l_rate, l_shift):
            load.wait()
        size = rec_blocks.shape[1]
        car_out[...] = jnp.zeros_like(car_out)
        lead = 8 * (taps - 1)
        ext[lead : lead + rows] = jnp.dot(mixer[...], sig[...], preferred_element_type=F32)
        top_row = lax.broadcasted_iota(jnp.int32, (8, width), 0) == 0
        rim = rim_in[...].astype(F32)
        rim = jnp.concatenate(
            [rim[4 * c : 4 * c + 4] for c in range(width // LANES)], axis=1
        )
        for k in range(1, taps):
            last = ext[lead + rows - 8 * k : lead + rows - 8 * k + 8]
            ext[lead - 8 * k : lead - 8 * k + 8] = jnp.where(
                top_row, rim[4 - k : 5 - k], pltpu.roll(last, 1, 0)
            )
        table = jnp.concatenate(
            [decay_shift[:, k * long : (k + 1) * long] for k in range(8)], axis=0
        )
        for i in range(long):
            shift[8 * i : 8 * i + 8] = jnp.broadcast_to(table[:, i : i + 1], (8, LANES))
        groups = width // LANES
        for c in range(groups):
            cols = slice(c * LANES, (c + 1) * LANES)
            conv = conv_kernel[0:1, cols] * ext[0:rows, cols]
            for j in range(1, taps):
                conv = conv + conv_kernel[j : j + 1, cols] * ext[8 * j : 8 * j + rows, cols]
            conv = conv.astype(BF16)
            per = LANES // size
            rec = jax.nn.sigmoid(
                jnp.dot(conv, block_diagonal(diag_a, rec_blocks, c * per), preferred_element_type=F32)
            )
            inp = jax.nn.sigmoid(
                jnp.dot(conv, block_diagonal(diag_b, inp_blocks, c * per), preferred_element_type=F32)
            )
            log_decay = -RECURRENT_SCALE * rec * decay_rate[0:1, cols] + shift[...]
            decay = jnp.exp(log_decay)
            prod[c] = decay
            state[c] = jnp.sqrt(-expm1_neg(2.0 * log_decay, decay)) * inp * conv.astype(F32)
        ones = [prod[c, 0:8] for c in range(groups)]
        twos = [state[c, 0:8] for c in range(groups)]
        for i in range(1, long):
            here = slice(8 * i, 8 * i + 8)
            for c in range(groups):
                decay = prod[c, here]
                twos[c] = decay * twos[c] + state[c, here]
                ones[c] = decay * ones[c]
                prod[c, here] = ones[c]
                state[c, here] = twos[c]
        first_row = lax.broadcasted_iota(jnp.int32, (8, LANES), 0) == 0
        for c in range(groups):
            cols = slice(c * LANES, (c + 1) * LANES)
            one, two = scan_rows(ones[c], twos[c])
            segments[0:8, cols] = jnp.where(first_row, 1.0, pltpu.roll(one, 1, 0))
            segments[8:16, cols] = jnp.where(first_row, 0.0, pltpu.roll(two, 1, 0))
            car_out[2 * c : 2 * c + 1] = one[7:8]
            car_out[2 * c + 1 : 2 * c + 2] = two[7:8]

    def carry_copy(e):
        return remote(car_out, car_in.at[e - 1], c_s, c_r, sp=sp + e)

    def carry_landed(e):
        return remote(car_out, car_in.at[e - 1], c_s, c_r, sp=sp - e)

    with scope("o_carry"):
        for e in range(1, sp_count):
            pl.when(sp + e < sp_count)(lambda e=e: carry_copy(e).start())
    factor = head_dim ** (-0.5) * LOG2E

    def prepare(e):
        place = sp - e
        blocks = []
        for n in range(tp_count):
            order = [(n - r) % tp_count for r in range(tp_count)]
            first = [0 if j == 0 else tall + j * share for j in order]
            blocks.append(
                jnp.concatenate([lat_all[place, n, f : f + share] for f in first], axis=0).astype(F32)
            )
        square = sum(jnp.sum(x * x, axis=-1, keepdims=True) for x in blocks)
        inverse = lax.rsqrt(square / (lat * tp_count) + EPS)
        for n, x in enumerate(blocks):
            cols = slice(n * lat, (n + 1) * lat)
            xlat[:, cols] = (x * inverse * latent_gain[0:1, cols]).astype(BF16)
        rope_keys[...] = jnp.concatenate(
            [
                lat_all[place, n, share : share + tall, k * rope : (k + 1) * rope]
                for n in range(tp_count)
                for k in range(packed)
            ],
            axis=0,
        )
        step = column_step(w_up.shape[1])
        for c in range(w_up.shape[1] // step):
            cols = slice(c * step, (c + 1) * step)
            kv[:, cols] = jnp.dot(xlat[...], w_up[:, cols], preferred_element_type=F32).astype(BF16)
        for h in range(heads):
            base = h * (nope + value) + nope
            turned_v[h] = kv[:, base : base + value].T

    def score(h, diagonal, lanes, count):
        base = h * (nope + value)
        keys = jnp.concatenate([kv[:, base : base + nope], rope_keys[...]], axis=1)
        scores = jnp.dot(keys, queries[h, :, lanes], preferred_element_type=F32) * factor
        if diagonal:
            seen = lax.broadcasted_iota(jnp.int32, scores.shape, 0)
            scores = jnp.where(
                seen <= lax.broadcasted_iota(jnp.int32, scores.shape, 1), scores, -jnp.inf
            )
        held[h, :, :count] = scores
        return jnp.max(scores, axis=0, keepdims=True)

    def mix(h, top, diagonal, lanes, count):
        if not diagonal:
            before = row_max[h, 0:1, lanes]
            top = jnp.maximum(top, before)
            fade = jnp.exp2(before - top)
        weights = jnp.exp2(held[h, :, :count] - top)
        mass = jnp.sum(weights, axis=0, keepdims=True)
        term = jnp.dot(turned_v[h], weights.astype(BF16), preferred_element_type=F32)
        if not diagonal:
            mass = mass + row_sum[h, 0:1, lanes] * fade
            term = term + acc[h, :, lanes] * fade
        row_max[h, 0:1, lanes] = top
        row_sum[h, 0:1, lanes] = mass
        acc[h, :, lanes] = term

    def heads_over(diagonal, lanes=slice(None), count=rows):
        tops = [score(h, diagonal, lanes, count) for h in range(heads)]
        for h in range(heads):
            mix(h, tops[h], diagonal, lanes, count)

    def attend(e, diagonal):
        prepare(e)
        heads_over(diagonal)

    with scope("r_att0"):
        l_lgain.wait()
        l_up.wait()
        wait_crossed(0)
        prepare(0)
    with scope("r_att0_heads"):
        heads_over(True)
    with scope("t_relay3"):
        if sp_count > 3:

            @pl.when(sp >= 3)
            def _():
                arrived(3).wait_recv()
                cross(3)

    with scope("s_att1"):
        if sp_count > 1:

            @pl.when(sp >= 1)
            def _():
                wait_crossed(1)
                attend(1, False)

    with scope("w_att3"):
        if sp_count > 3:

            @pl.when(sp >= 3)
            def _():
                wait_crossed(3)
                attend(3, False)

        if sp_count > 4:

            def later(e, carry):
                block = lat_all.at[sp - e, tp]
                remote(block, block, fwd_s.at[e - 3], fwd_r.at[e - 3], sp=sp - 1).wait_recv()
                cross(e)
                wait_crossed(e)
                attend(e, False)
                return carry

            lax.fori_loop(4, sp + 1, later, 0)
    with scope("x_relay2"):
        if sp_count > 2:

            @pl.when(sp >= 2)
            def _():
                for k in range(2):
                    forwarded(k).wait_recv()
                    for d in range(1, tp_count):
                        across_piece(k, d).start()

    with scope("u_carrywait"):
        for v in range(1, sp_count):

            @pl.when(sp == v)
            def _(v=v):
                remote(car_in.at[pl.ds(0, v)], car_in.at[pl.ds(0, v)], c_s, c_r, sp=sp - 1).wait_recv()

        for e in range(1, sp_count):

            @pl.when(sp < e)
            def _(e=e):
                row = lax.broadcasted_iota(jnp.int32, car_out.shape, 0)
                car_in[e - 1] = jnp.where((row & 1) == 0, 1.0, 0.0)

    with scope("v_rout"):
        l_init.wait()
        for c in range(width // LANES):
            cols = slice(c * LANES, (c + 1) * LANES)
            incoming = initial_state[:, cols]
            for e in range(sp_count - 1, 0, -1):
                incoming = (
                    car_in[e - 1, 2 * c : 2 * c + 1] * incoming
                    + car_in[e - 1, 2 * c + 1 : 2 * c + 2]
                )
            enter = segments[0:8, cols] * incoming + segments[8:16, cols]
            full = state[c] + prod[c] * jnp.concatenate([enter] * long, axis=0)
            mixed_rout[:, cols] = (full * silu_gate[:, cols]).astype(BF16)
        rout[...] = jnp.dot(
            unmixer[...], mixed_rout[...], preferred_element_type=F32
        ).astype(BF16)
        l_rout.wait()
        step = column_step(model)
        for c in range(model // step):
            cols = slice(c * step, (c + 1) * step)
            racc[:, cols] = jnp.dot(rout[...], w_rout[:, cols], preferred_element_type=F32)
    chunks, step = part_in.shape[1], part_in.shape[3]
    split = share % LANES == 0

    def part_copy(d, c):
        return remote(
            part.at[d - 1, c], part_in.at[d - 1, c], p_s.at[d - 1], p_r.at[d - 1, c], tp=peer(d)
        )

    def partial(place, c):
        cols = slice(c * step, (c + 1) * step)
        here = share_rows(place)
        both = racc[here, cols] + jnp.dot(aout[here], w_aout[:, cols], preferred_element_type=F32)
        return both.astype(BF16)

    def finish(here):
        for h in range(heads):
            cols = slice(h * value, (h + 1) * value)
            attended = (acc[h, :, here] * (1.0 / row_sum[h, 0:1, here])).T
            aout[here, cols] = (attended * jax.nn.silu(attp[here, cols].astype(F32))).astype(BF16)

    def send(d, c):
        part[d - 1, c] = partial(peer(d), c)
        part_copy(d, c).start()

    def last_block():
        for d in range(1, tp_count):
            block = lat_all.at[sp - 2, source(d)]
            remote(block, block, l_s.at[d - 1], x_r.at[d - 1], tp=source(d)).wait_recv()
        prepare(2)
        if not split:
            heads_over(False)
            finish(slice(None))
            for c in range(chunks):
                for d in range(1, tp_count):
                    send(d, c)
            for c in range(chunks):
                own_part[c] = partial(tp, c)
            return
        for d in range(1, tp_count):
            heads_over(False, share_rows(peer(d)), share)
            finish(share_rows(peer(d)))
        mine = share_rows(tp)
        sends = [(d, c) for d in range(1, tp_count) for c in range(chunks)]
        each = -(-2 * len(sends) // heads)
        tops = [score(h, False, mine, share) for h in range(heads)]
        for h in range(heads):
            for d, c in sends[h * each : (h + 1) * each]:
                send(d, c)
            mix(h, tops[h], False, mine, share)
        finish(mine)
        for c in range(chunks):
            own_part[c] = partial(tp, c)

    def no_block():
        finish(slice(None))
        for c in range(chunks):
            for d in range(1, tp_count):
                send(d, c)
        for c in range(chunks):
            own_part[c] = partial(tp, c)

    with scope("y_last"):
        l_aout.wait()
        if sp_count > 2:
            pl.when(sp >= 2)(last_block)
            pl.when(sp < 2)(no_block)
        else:
            no_block()
    with scope("z_sum"):
        for c in range(chunks):
            summed = own_part[c].astype(F32)
            for d in range(1, tp_count):
                part_copy(d, c).wait_recv()
                summed = summed + part_in[d - 1, c].astype(F32)
            out[:, c * step : (c + 1) * step] = summed.astype(BF16)

    with scope("z_waits"):
        for d in range(1, tp_count):
            token_whole(d).wait_send()
            whole = part.at[d - 1]
            remote(whole, whole, p_s.at[d - 1], p_r.at[d - 1, 0], tp=peer(d)).wait_send()

        def all_sent(send, recv, count):
            blocks = lat_all.at[pl.ds(0, count), 0]
            remote(blocks, blocks, send, recv, tp=peer(1)).wait_send()

        for v in range(sp_count):

            @pl.when(sp == v)
            def _(v=v):
                for d in range(1, tp_count):
                    all_sent(l_s.at[d - 1], l_r.at[0, d - 1], v + 1)
                if v + 1 < sp_count:
                    rim_copy().wait_send()
                    all_sent(z_s, z_r.at[0], 1)
                    if v and sp_count > 2:
                        all_sent(y_s, y_r.at[0], 1)
                    carries = car_in.at[pl.ds(0, sp_count - 1 - v)]
                    remote(carries, carries, c_s, c_r, sp=sp + 1).wait_send()
                for e in range(3, sp_count - v):
                    direct(e).wait_send()


def body(
    tokens, norm_gain, recurrent_input, recurrent_gate, attention_gate, query_proj, latent_down,
    rope_key_down, conv_kernel, recurrence_gate_blocks, input_gate_blocks, decay_rate, decay_shift,
    initial_state, latent_gain, latent_up, query_gain, recurrent_output, attention_output,
):
    tp_count = lax.axis_size("tp")
    sp_count = lax.axis_size("sp")
    share, model = tokens.shape
    rows = share * tp_count
    width = recurrent_input.shape[1]
    taken = attention_gate.shape[1]
    head_dim = query_gain.shape[0]
    heads = query_proj.shape[1] // head_dim
    value = taken // heads
    lat = latent_down.shape[1]
    rope = rope_key_down.shape[1]
    cosine, sine = rotary_tables(sp_count * rows, rope)
    key_table = np.concatenate([cosine, cosine, -sine, sine], 1).reshape(-1, share, 2 * rope)
    query_table = np.concatenate([cosine, sine], 1).reshape(sp_count, rows, rope).transpose(0, 2, 1)
    hbm = [
        tokens, latent_down, norm_gain[None], rope_key_down.T, jnp.asarray(key_table),
        recurrent_input, query_proj, query_gain[None], jnp.asarray(query_table), conv_kernel,
        recurrence_gate_blocks, input_gate_blocks, decay_rate[None], decay_shift[None],
        recurrent_gate, attention_gate, latent_gain[None], latent_up, initial_state[None],
        recurrent_output, attention_output,
    ]
    held = [a.shape for a in hbm]
    held[4] = key_table.shape[1:]
    held[8] = query_table.shape[1:]
    vmem = pltpu.VMEM
    dma = pltpu.SemaphoreType.DMA
    others = max(tp_count - 1, 1)
    hops = max(sp_count - 1, 1)
    carries = -(-2 * width // LANES // 8) * 8
    rims = -(-4 * width // LANES // 16) * 16
    chunks = 4 if model % (4 * LANES) == 0 else 1
    return pl.pallas_call(
        functools.partial(layer_kernel, sp_count, tp_count),
        out_shape=pltpu.VMEM((share, model), BF16),
        in_specs=[pl.BlockSpec(memory_space=pl.ANY)] * len(hbm),
        out_specs=pl.BlockSpec(memory_space=pltpu.VMEM),
        scratch_shapes=[vmem(s, a.dtype) for s, a in zip(held, hbm)]
        + [
            vmem((others, share, model), BF16),
            vmem((rows, model), BF16),
            vmem((sp_count, tp_count, rows + share * rope // lat, lat), BF16),
            vmem((rows, width), BF16),
            vmem((rows, width), BF16),
            vmem((rows, taken), BF16),
            vmem((query_proj.shape[1], rows), BF16),
            vmem((heads, head_dim, rows), BF16),
            vmem((rims, LANES), BF16),
            vmem((rims, LANES), BF16),
            vmem((rows + 24, width), F32),
            vmem((LANES, LANES), BF16),
            vmem((LANES, LANES), BF16),
            vmem((rows, rows), BF16),
            vmem((rows, rows), BF16),
            vmem((rows, LANES), F32),
            vmem((rows, width), F32),
            vmem((rows, width), BF16),
            vmem((width // LANES, rows, LANES), F32),
            vmem((width // LANES, rows, LANES), F32),
            vmem((16, width), F32),
            vmem((carries, LANES), F32),
            vmem((hops, carries, LANES), F32),
            vmem((rows, width), BF16),
            vmem((rows, model), F32),
            vmem((rows, lat * tp_count), BF16),
            vmem((rows, rope), BF16),
            vmem((heads, value, rows), BF16),
            vmem((rows, latent_up.shape[1]), BF16),
            vmem((heads, rows, rows), F32),
            vmem((heads, 8, rows), F32),
            vmem((heads, 8, rows), F32),
            vmem((heads, value, rows), F32),
            vmem((rows, taken), BF16),
            vmem((others, chunks, share, model // chunks), BF16),
            vmem((chunks, share, model // chunks), BF16),
            vmem((others, chunks, share, model // chunks), BF16),
            dma((10,)),
            dma((others,)), dma((others,)),
            dma, dma((2,)),
            dma, dma((2,)),
            dma((max(sp_count - 3, 1),)), dma((max(sp_count - 3, 1),)),
            dma((others,)), dma((max(sp_count - 1, 1), others)),
            dma((others,)),
            dma, dma,
            dma, dma,
            dma((others,)), dma((others, chunks)),
            pltpu.SemaphoreType.REGULAR((hops,)),
        ],
        compiler_params=pltpu.CompilerParams(
            collective_id=0, has_side_effects=True, vmem_limit_bytes=61400 * 1024
        ),
    )(*hbm)


def solution(mesh):
    return jax.shard_map(
        body,
        mesh=mesh,
        in_specs=(
            P(("fs", "sp", "tp"), None),
            P(),
            P(None, "tp"),
            P(None, "tp"),
            P(None, "tp"),
            P(None, "tp"),
            P(None, "tp"),
            P(),
            P(None, "tp"),
            P("tp", None, None),
            P("tp", None, None),
            P("tp"),
            P(("fs", "sp")),
            P(("fs", "tp")),
            P(),
            P(None, "tp"),
            P(),
            P("tp", None),
            P("tp", None),
        ),
        out_specs=P(("fs", "sp", "tp"), None),
        check_vma=False,
    )
```

```python
import functools

import jax
import jax.numpy as jnp
import numpy as np
from jax import lax
from jax.experimental import pallas as pl
from jax.experimental.pallas import tpu as pltpu
from jax.sharding import PartitionSpec as P

EPS = 1e-06
RECURRENT_SCALE = 8.0
THETA = 10000.0
F32 = jnp.float32
BF16 = jnp.bfloat16
LANES = 128


def expm1_neg(y, root):
    small = y * (1.0 + y * (0.5 + y * (1.0 / 6 + y * (1.0 / 24 + y / 120))))
    return jnp.where(y > -0.1, small, root * root - 1.0)


def block_diagonal(scratch, blocks_ref, first):
    size = blocks_ref.shape[1]
    scratch[...] = jnp.zeros_like(scratch)
    for k in range(scratch.shape[0] // size):
        scratch[k * size : (k + 1) * size, k * size : (k + 1) * size] = blocks_ref[first + k]
    return scratch[...]


def scan_rows(decay, state):
    rows = decay.shape[0]
    row = lax.broadcasted_iota(jnp.int32, decay.shape, 0)
    step = 1
    while step < rows:
        inside = row >= step
        before_decay = jnp.where(inside, pltpu.roll(decay, step, 0), 1.0)
        before_state = jnp.where(inside, pltpu.roll(state, step, 0), 0.0)
        state = state + decay * before_state
        decay = decay * before_decay
        step *= 2
    return decay, state


def rms_scaled(values, gain_vec):
    return values * lax.rsqrt(jnp.mean(values * values, axis=-1, keepdims=True) + EPS) * gain_vec


LOG2E = 1.4426950408889634


def rotary_tables(positions, width):
    inv_freq = (1.0 / THETA ** (np.arange(0, width, 2, dtype=np.float32) / width)).astype(np.float32)
    angles = np.arange(positions, dtype=np.float32)[:, None] * inv_freq[None, :]
    cosine = np.cos(angles.astype(np.float64)).astype(np.float32)
    sine = np.sin(angles.astype(np.float64)).astype(np.float32)
    return cosine, sine


def column_step(width):
    return 256 if width % 256 == 0 else width


def remote(src, dst, send, recv, **where):
    return pltpu.make_async_remote_copy(
        src_ref=src, dst_ref=dst, send_sem=send, recv_sem=recv,
        device_id=where, device_id_type=pl.DeviceIdType.MESH,
    )


def scope(name):
    return jax.named_scope(name)


def layer_kernel(
    sp_count, tp_count,
    h_tokens, h_lat, h_norm, h_rope, h_ktab, h_in, h_query, h_qgain, h_qtab, h_conv, h_rec, h_inp,
    h_rate, h_shift, h_gate, h_att, h_lgain, h_up, h_init, h_rout, h_aout,
    out,
    tokens, w_lat, norm_gain, w_rope, key_table, w_in, w_query, query_gain, query_table,
    conv_kernel, rec_blocks, inp_blocks, decay_rate, decay_shift, w_gate, w_att, latent_gain,
    w_up, initial_state, w_rout, w_aout,
    tok_all, normed, lat_all, sig, gate, attp, turned_q, queries, rim_out, rim_in, ext, diag_a, diag_b,
    mixer, unmixer, shift, silu_gate, mixed_rout,
    prod, state, segments, car_out, car_in, rout, racc, xlat, rope_keys, turned_v, kv, held, row_max, row_sum,
    acc, aout, part, own_part, part_in, w_aout_in, w_rout_in, rout_in, aout_in, racc_in,
    w_sem, tok_s, tok_r, z_s, z_r, y_s, y_r, fwd_s, fwd_r, l_s, l_r, x_r, rim_s, rim_r, c_s, c_r,
    p_s, p_r, wf_s, wf_r, ro_s, ro_r, ao_s, ao_r, ready,
):
    sp = lax.axis_index("sp")
    tp = lax.axis_index("tp")
    share, model = tokens.shape
    rows = normed.shape[0]
    taps, width = conv_kernel.shape
    head_dim = query_gain.shape[1]
    rope = w_rope.shape[0]
    half = rope // 2
    nope = head_dim - rope
    heads = w_query.shape[1] // head_dim
    lat = w_lat.shape[1]
    value = w_att.shape[1] // heads
    packed = lat // rope
    tall = share // packed
    pieces = 4 if share % 64 == 0 else 1
    piece = share // pieces
    long = rows // 8

    h_refs = (
        h_tokens, h_lat, h_norm, h_rope, h_ktab.at[sp * tp_count + tp], h_in, h_query, h_qgain,
        h_qtab.at[sp], h_conv, h_rec, h_inp, h_rate, h_shift, h_gate, h_att, h_lgain, h_up,
        h_init, h_rout, h_aout,
    )
    w_refs = (
        tokens, w_lat, norm_gain, w_rope, key_table, w_in, w_query, query_gain, query_table,
        conv_kernel, rec_blocks, inp_blocks, decay_rate, decay_shift, w_gate, w_att, latent_gain,
        w_up, initial_state, w_rout, w_aout,
    )
    slots = (1, 2, 0, 3, 4, 5, 6, 0, 1, 4, 5, 0, 1, 6, 2, 3, 9, 7, 2, 3, 8)
    loads = [
        pltpu.make_async_copy(a, b, w_sem.at[k]) for a, b, k in zip(h_refs, w_refs, slots)
    ]
    token_loads = [
        pltpu.make_async_copy(
            h_tokens.at[pl.ds(k * piece, piece)], tokens.at[pl.ds(k * piece, piece)], w_sem.at[1]
        )
        for k in range(pieces)
    ]

    def peer(d):
        return lax.rem(tp + d, tp_count)

    def source(d):
        return lax.rem(tp - d + tp_count, tp_count)

    def greet(sem, **where):
        pl.semaphore_signal(sem, inc=1, device_id=where, device_id_type=pl.DeviceIdType.MESH)

    (
        l_tok, l_lat, l_norm, l_rope, l_ktab, l_in, l_query, l_qgain, l_qtab, l_conv, l_rec, l_inp,
        l_rate, l_shift, l_gate, l_att, l_lgain, l_up, l_init, l_rout, l_aout,
    ) = loads
    barrier = pltpu.get_barrier_semaphore()
    with scope("a_loads"):
        for d in range(1, tp_count):
            greet(barrier, tp=peer(d))
        for e in range(1, sp_count):
            pl.when(sp + e < sp_count)(lambda e=e: greet(barrier, sp=sp + e))
        l_norm.start()
        for load in token_loads:
            load.start()
        l_lat.start()

    def token_copy(d, k):
        part_rows = pl.ds(k * piece, piece)
        return remote(
            h_tokens.at[part_rows], tok_all.at[d - 1, part_rows],
            tok_s.at[d - 1], tok_r.at[d - 1], tp=peer(d),
        )

    near = model // 2

    def weight_copy(k, d):
        source_ref = (h_aout, h_rout)[k].at[:, pl.ds(0, near)]
        target_ref = (w_aout_in, w_rout_in)[k].at[d - 1]
        return remote(source_ref, target_ref, wf_s.at[k, d - 1], wf_r.at[k, d - 1], tp=peer(d))

    def token_whole(d):
        return remote(h_tokens, tok_all.at[d - 1], tok_s.at[d - 1], tok_r.at[d - 1], tp=peer(d))

    with scope("b_barrier"):
        pl.semaphore_wait(barrier, tp_count - 1 + sp)
        for k in range(pieces):
            for d in range(1, tp_count):
                token_copy(d, k).start()
        for e in range(1, sp_count):
            pl.when(sp >= e)(lambda e=e: greet(ready.at[e - 1], sp=sp - e))
        for load in (l_rope, l_ktab, l_in, l_query):
            load.start()

    def share_rows(place):
        return pl.ds(pl.multiple_of(place * share, share), share)

    def put_normed(block, place):
        normed[share_rows(place)] = rms_scaled(block.astype(F32), norm_gain[...]).astype(BF16)

    def put_latent(first, place):
        own[first : first + share] = jnp.dot(
            normed[share_rows(place)], w_lat[...], preferred_element_type=F32
        ).astype(BF16)

    def project(weight, into, here=slice(None)):
        step = column_step(weight.shape[1])
        for c in range(weight.shape[1] // step):
            cols = slice(c * step, (c + 1) * step)
            into[here, cols] = jnp.dot(
                normed[here], weight[:, cols], preferred_element_type=F32
            ).astype(BF16)

    own = lat_all.at[sp, tp]
    with scope("c_norm_own"):
        l_norm.wait()
        l_tok.wait()
        put_normed(tokens[...], tp)
    with scope("d_lat_a"):
        l_lat.wait()
        put_latent(0, tp)

    def along(k):
        block = lat_all.at[sp, tp, (pl.ds(0, share), pl.ds(share, rows + tall - share))[k]]
        return remote(block, block, z_s, z_r.at[k], sp=sp + 1)

    def landed(k):
        block = lat_all.at[sp - 1, tp, (pl.ds(0, share), pl.ds(share, rows + tall - share))[k]]
        return remote(block, block, z_s, z_r.at[k], sp=sp - 1)

    def direct(e):
        block = lat_all.at[sp, tp]
        return remote(block, block, fwd_s.at[e - 3], fwd_r.at[e - 3], sp=sp + e)

    def forward(k):
        block = lat_all.at[sp - 1, tp, (pl.ds(0, share), pl.ds(share, rows + tall - share))[k]]
        return remote(block, block, y_s, y_r.at[k], sp=sp + 1)

    def forwarded(k):
        block = lat_all.at[sp - 2, tp, (pl.ds(0, share), pl.ds(share, rows + tall - share))[k]]
        return remote(block, block, y_s, y_r.at[k], sp=sp - 1)

    def arrived(e):
        block = lat_all.at[sp - e, tp]
        return remote(block, block, fwd_s.at[e - 3], fwd_r.at[e - 3], sp=sp - 1)

    def late(e):
        return e if isinstance(e, int) and e < 2 else e - 1

    def across(e, d):
        block = lat_all.at[sp - e, tp]
        return remote(block, block, l_s.at[d - 1], l_r.at[late(e), d - 1], tp=peer(d))

    def crossed(e, d):
        block = lat_all.at[sp - e, source(d)]
        return remote(block, block, l_s.at[d - 1], l_r.at[late(e), d - 1], tp=source(d))

    def halves(k):
        return (pl.ds(0, share), pl.ds(share, rows + tall - share))[k]

    def across_piece(k, d):
        block = lat_all.at[sp - 2, tp, halves(k)]
        return remote(block, block, l_s.at[d - 1], x_r.at[d - 1], tp=peer(d))

    def cross(e):
        for d in range(1, tp_count):
            across(e, d).start()

    def wait_crossed(e):
        for d in range(1, tp_count):
            crossed(e, d).wait_recv()

    has_next = sp + 1 < sp_count
    with scope("f_send_a"):

        @pl.when(has_next)
        def _():
            pl.semaphore_wait(ready.at[0], 1)
            along(0).start()

    with scope("e_mixers"):
        row = lax.broadcasted_iota(jnp.int32, (rows, rows), 0)
        column = lax.broadcasted_iota(jnp.int32, (rows, rows), 1)
        mixer[...] = jnp.where(column == (row & 7) * long + (row >> 3), 1.0, 0.0).astype(BF16)
        unmixer[...] = jnp.where(row == (column & 7) * long + (column >> 3), 1.0, 0.0).astype(BF16)
    with scope("e_rope"):
        l_rope.wait()
        l_ktab.wait()
        raw = lax.dot_general(
            normed[share_rows(tp)], w_rope[...], (((1,), (1,)), ((), ())),
            preferred_element_type=F32,
        ).astype(BF16).astype(F32)
        swapped = jnp.concatenate([raw[:, half:], raw[:, :half]], axis=1)
        keyed = (raw * key_table[:, :rope] + swapped * key_table[:, rope:]).astype(BF16)
        for k in range(packed):
            own[share : share + tall, k * rope : (k + 1) * rope] = keyed[k * tall : (k + 1) * tall]
    with scope("g_norm_peer"):
        for d in range(1, tp_count):
            token_whole(d).wait_recv()
            put_normed(tok_all[d - 1], source(d))
    def rim_copy():
        return remote(rim_out, rim_in, rim_s, rim_r, sp=sp + 1)

    def rim_landed():
        return remote(rim_out, rim_in, rim_s, rim_r, sp=sp - 1)

    with scope("i_lat_b"):
        for d in range(1, tp_count):
            put_latent(d * share + tall, source(d))
        pl.when(has_next)(lambda: along(1).start())
        cross(0)
        for d in range(1, tp_count):
            weight_copy(0, d).start()
    with scope("h_in_peer"):
        l_in.wait()
        for load in (l_qgain, l_qtab, l_gate, l_att, l_conv, l_rec, l_up, l_lgain, l_aout):
            load.start()
        project(w_in, sig)
        tail = sig[rows - 16 :].astype(F32)[12:]
        tail = [tail[:, c * LANES : (c + 1) * LANES] for c in range(width // LANES)]
        if len(tail) * 4 < rim_out.shape[0]:
            tail.append(jnp.zeros((rim_out.shape[0] - len(tail) * 4, LANES), F32))
        rim_out[...] = jnp.concatenate(tail, axis=0).astype(BF16)
        pl.when(has_next)(lambda: rim_copy().start())
    with scope("j_query"):
        l_query.wait()
        step = column_step(w_query.shape[1])
        for c in range(w_query.shape[1] // step):
            cols = slice(c * step, (c + 1) * step)
            raw = jnp.dot(normed[...], w_query[:, cols], preferred_element_type=F32).astype(BF16)
            turned_q[cols] = raw.T
    with scope("k_rotate"):
        l_qgain.wait()
        l_qtab.wait()
        spare = -head_dim % LANES
        gain = query_gain[...]
        if spare:
            gain = jnp.concatenate([gain, jnp.zeros((1, spare), F32)], axis=1)
        gain = jnp.broadcast_to(gain, (LANES, head_dim + spare)).T[:head_dim]
        gain = jnp.concatenate([gain] * (rows // LANES), axis=1)
        cosine = query_table[:half]
        sine = query_table[half:]
        for h in range(heads):
            head = turned_q[h * head_dim : (h + 1) * head_dim].astype(F32)
            square = jnp.sum(head * head, axis=0, keepdims=True)
            head = head * lax.rsqrt(square / head_dim + EPS) * gain
            first, second = head[nope : nope + half], head[nope + half :]
            queries[h, :nope] = head[:nope].astype(BF16)
            queries[h, nope : nope + half] = (first * cosine - second * sine).astype(BF16)
            queries[h, nope + half :] = (first * sine + second * cosine).astype(BF16)
        for load in (l_inp, l_rate, l_shift):
            load.start()

    def relay1(k):
        if sp_count > 1:

            @pl.when(sp >= 1)
            def _():
                landed(k).wait_recv()
                if sp_count > 2:
                    pl.when(has_next)(lambda: forward(k).start())
                if k:
                    cross(1)

    with scope("p_relay1a"):
        relay1(0)

    with scope("q_gates"):
        l_gate.wait()
        project(w_gate, gate)
        silu_gate[...] = jax.nn.silu(
            jnp.dot(mixer[...], gate[...], preferred_element_type=F32)
        )

    with scope("l_direct"):
        for e in range(2, sp_count):

            @pl.when(sp + e < sp_count)
            def _(e=e):
                pl.semaphore_wait(ready.at[e - 1], 1)
                if e > 2:
                    direct(e).start()

    with scope("q_gate_att"):
        l_att.wait()
        project(w_att, attp)
        for load in (l_init, l_rout):
            load.start()

    with scope("p_relay1b"):
        relay1(1)
        for d in range(1, tp_count):
            weight_copy(1, d).start()
    with scope("m_rim"):

        @pl.when(sp == 0)
        def _():
            rim_in[...] = jnp.zeros_like(rim_in)

        pl.when(sp > 0)(lambda: rim_landed().wait_recv())
    with scope("n_scan"):
        for load in (l_conv, l_rec, l_inp, l_rate, l_shift):
            load.wait()
        size = rec_blocks.shape[1]
        car_out[...] = jnp.zeros_like(car_out)
        lead = 8 * (taps - 1)
        ext[lead : lead + rows] = jnp.dot(mixer[...], sig[...], preferred_element_type=F32)
        top_row = lax.broadcasted_iota(jnp.int32, (8, width), 0) == 0
        rim = rim_in[...].astype(F32)
        rim = jnp.concatenate(
            [rim[4 * c : 4 * c + 4] for c in range(width // LANES)], axis=1
        )
        for k in range(1, taps):
            last = ext[lead + rows - 8 * k : lead + rows - 8 * k + 8]
            ext[lead - 8 * k : lead - 8 * k + 8] = jnp.where(
                top_row, rim[4 - k : 5 - k], pltpu.roll(last, 1, 0)
            )
        table = jnp.concatenate(
            [decay_shift[:, k * long : (k + 1) * long] for k in range(8)], axis=0
        )
        for i in range(long):
            shift[8 * i : 8 * i + 8] = jnp.broadcast_to(table[:, i : i + 1], (8, LANES))
        groups = width // LANES
        for c in range(groups):
            cols = slice(c * LANES, (c + 1) * LANES)
            conv = conv_kernel[0:1, cols] * ext[0:rows, cols]
            for j in range(1, taps):
                conv = conv + conv_kernel[j : j + 1, cols] * ext[8 * j : 8 * j + rows, cols]
            conv = conv.astype(BF16)
            per = LANES // size
            rec = jax.nn.sigmoid(
                jnp.dot(conv, block_diagonal(diag_a, rec_blocks, c * per), preferred_element_type=F32)
            )
            inp = jax.nn.sigmoid(
                jnp.dot(conv, block_diagonal(diag_b, inp_blocks, c * per), preferred_element_type=F32)
            )
            log_decay = -RECURRENT_SCALE * rec * decay_rate[0:1, cols] + shift[...]
            decay = jnp.exp(log_decay)
            prod[c] = decay
            state[c] = jnp.sqrt(-expm1_neg(2.0 * log_decay, decay)) * inp * conv.astype(F32)
        ones = [prod[c, 0:8] for c in range(groups)]
        twos = [state[c, 0:8] for c in range(groups)]
        for i in range(1, long):
            here = slice(8 * i, 8 * i + 8)
            for c in range(groups):
                decay = prod[c, here]
                twos[c] = decay * twos[c] + state[c, here]
                ones[c] = decay * ones[c]
                prod[c, here] = ones[c]
                state[c, here] = twos[c]
        first_row = lax.broadcasted_iota(jnp.int32, (8, LANES), 0) == 0
        for c in range(groups):
            cols = slice(c * LANES, (c + 1) * LANES)
            one, two = scan_rows(ones[c], twos[c])
            segments[0:8, cols] = jnp.where(first_row, 1.0, pltpu.roll(one, 1, 0))
            segments[8:16, cols] = jnp.where(first_row, 0.0, pltpu.roll(two, 1, 0))
            car_out[2 * c : 2 * c + 1] = one[7:8]
            car_out[2 * c + 1 : 2 * c + 2] = two[7:8]

    def carry_copy(e):
        return remote(car_out, car_in.at[e - 1], c_s, c_r, sp=sp + e)

    def carry_landed(e):
        return remote(car_out, car_in.at[e - 1], c_s, c_r, sp=sp - e)

    with scope("o_carry"):
        for e in range(1, sp_count):
            pl.when(sp + e < sp_count)(lambda e=e: carry_copy(e).start())
    factor = head_dim ** (-0.5) * LOG2E

    def prepare(e):
        place = sp - e
        blocks = []
        for n in range(tp_count):
            order = [(n - r) % tp_count for r in range(tp_count)]
            first = [0 if j == 0 else tall + j * share for j in order]
            blocks.append(
                jnp.concatenate([lat_all[place, n, f : f + share] for f in first], axis=0).astype(F32)
            )
        square = sum(jnp.sum(x * x, axis=-1, keepdims=True) for x in blocks)
        inverse = lax.rsqrt(square / (lat * tp_count) + EPS)
        for n, x in enumerate(blocks):
            cols = slice(n * lat, (n + 1) * lat)
            xlat[:, cols] = (x * inverse * latent_gain[0:1, cols]).astype(BF16)
        rope_keys[...] = jnp.concatenate(
            [
                lat_all[place, n, share : share + tall, k * rope : (k + 1) * rope]
                for n in range(tp_count)
                for k in range(packed)
            ],
            axis=0,
        )
        step = column_step(w_up.shape[1])
        for c in range(w_up.shape[1] // step):
            cols = slice(c * step, (c + 1) * step)
            kv[:, cols] = jnp.dot(xlat[...], w_up[:, cols], preferred_element_type=F32).astype(BF16)
        for h in range(heads):
            base = h * (nope + value) + nope
            turned_v[h] = kv[:, base : base + value].T

    def score(h, diagonal, lanes, count):
        base = h * (nope + value)
        keys = jnp.concatenate([kv[:, base : base + nope], rope_keys[...]], axis=1)
        scores = jnp.dot(keys, queries[h, :, lanes], preferred_element_type=F32) * factor
        if diagonal:
            seen = lax.broadcasted_iota(jnp.int32, scores.shape, 0)
            scores = jnp.where(
                seen <= lax.broadcasted_iota(jnp.int32, scores.shape, 1), scores, -jnp.inf
            )
        held[h, :, :count] = scores
        return jnp.max(scores, axis=0, keepdims=True)

    def mix(h, top, diagonal, lanes, count):
        if not diagonal:
            before = row_max[h, 0:1, lanes]
            top = jnp.maximum(top, before)
            fade = jnp.exp2(before - top)
        weights = jnp.exp2(held[h, :, :count] - top)
        mass = jnp.sum(weights, axis=0, keepdims=True)
        term = jnp.dot(turned_v[h], weights.astype(BF16), preferred_element_type=F32)
        if not diagonal:
            mass = mass + row_sum[h, 0:1, lanes] * fade
            term = term + acc[h, :, lanes] * fade
        row_max[h, 0:1, lanes] = top
        row_sum[h, 0:1, lanes] = mass
        acc[h, :, lanes] = term

    def heads_over(diagonal, lanes=slice(None), count=rows):
        tops = [score(h, diagonal, lanes, count) for h in range(heads)]
        for h in range(heads):
            mix(h, tops[h], diagonal, lanes, count)

    def attend(e, diagonal):
        prepare(e)
        heads_over(diagonal)

    with scope("r_att0"):
        l_lgain.wait()
        l_up.wait()
        wait_crossed(0)
        prepare(0)
    with scope("r_att0_heads"):
        heads_over(True)
    with scope("t_relay3"):
        if sp_count > 3:

            @pl.when(sp >= 3)
            def _():
                arrived(3).wait_recv()
                cross(3)

    with scope("s_att1"):
        if sp_count > 1:

            @pl.when(sp >= 1)
            def _():
                wait_crossed(1)
                attend(1, False)

    with scope("w_att3"):
        if sp_count > 3:

            @pl.when(sp >= 3)
            def _():
                wait_crossed(3)
                attend(3, False)

        if sp_count > 4:

            def later(e, carry):
                block = lat_all.at[sp - e, tp]
                remote(block, block, fwd_s.at[e - 3], fwd_r.at[e - 3], sp=sp - 1).wait_recv()
                cross(e)
                wait_crossed(e)
                attend(e, False)
                return carry

            lax.fori_loop(4, sp + 1, later, 0)
    with scope("x_relay2"):
        if sp_count > 2:

            @pl.when(sp >= 2)
            def _():
                for k in range(2):
                    forwarded(k).wait_recv()
                    for d in range(1, tp_count):
                        across_piece(k, d).start()

    with scope("u_carrywait"):
        for v in range(1, sp_count):

            @pl.when(sp == v)
            def _(v=v):
                remote(car_in.at[pl.ds(0, v)], car_in.at[pl.ds(0, v)], c_s, c_r, sp=sp - 1).wait_recv()

        for e in range(1, sp_count):

            @pl.when(sp < e)
            def _(e=e):
                row = lax.broadcasted_iota(jnp.int32, car_out.shape, 0)
                car_in[e - 1] = jnp.where((row & 1) == 0, 1.0, 0.0)

    def rout_copy(d):
        return remote(
            rout.at[share_rows(peer(d))], rout_in.at[d - 1], ro_s.at[d - 1], ro_r.at[d - 1], tp=peer(d)
        )

    def aout_copy(d):
        return remote(
            aout.at[share_rows(peer(d))], aout_in.at[d - 1], ao_s.at[d - 1], ao_r.at[d - 1], tp=peer(d)
        )

    with scope("v_rout"):
        l_init.wait()
        for c in range(width // LANES):
            cols = slice(c * LANES, (c + 1) * LANES)
            incoming = initial_state[:, cols]
            for e in range(sp_count - 1, 0, -1):
                incoming = (
                    car_in[e - 1, 2 * c : 2 * c + 1] * incoming
                    + car_in[e - 1, 2 * c + 1 : 2 * c + 2]
                )
            enter = segments[0:8, cols] * incoming + segments[8:16, cols]
            full = state[c] + prod[c] * jnp.concatenate([enter] * long, axis=0)
            mixed_rout[:, cols] = (full * silu_gate[:, cols]).astype(BF16)
        rout[...] = jnp.dot(
            unmixer[...], mixed_rout[...], preferred_element_type=F32
        ).astype(BF16)
        l_rout.wait()
        for d in range(1, tp_count):
            rout_copy(d).start()
        step = column_step(near)
        for c in range(near // step):
            cols = slice(near + c * step, near + (c + 1) * step)
            racc[:, cols] = jnp.dot(rout[...], w_rout[:, cols], preferred_element_type=F32)
        for c in range(near // step):
            cols = slice(c * step, (c + 1) * step)
            here = share_rows(tp)
            racc[here, cols] = jnp.dot(rout[here], w_rout[:, cols], preferred_element_type=F32)
    chunks, step = part_in.shape[1], part_in.shape[3]
    split = share % LANES == 0

    def part_copy(d, c):
        return remote(
            part.at[d - 1, c], part_in.at[d - 1, c], p_s.at[d - 1], p_r.at[d - 1, c], tp=peer(d)
        )

    def partial(place, cols):
        here = share_rows(place)
        both = racc[here, cols] + jnp.dot(aout[here], w_aout[:, cols], preferred_element_type=F32)
        return both.astype(BF16)

    def far(c):
        return slice(near + c * step, near + (c + 1) * step)

    def near_recurrent():
        for d in range(1, tp_count):
            rout_copy(d).wait_recv()
            weight_copy(1, d).wait_recv()
            for c in range(near // step):
                cols = slice(c * step, (c + 1) * step)
                racc_in[d - 1, :, cols] = jnp.dot(
                    rout_in[d - 1], w_rout_in[d - 1, :, cols], preferred_element_type=F32
                )

    def own_rows():
        for c in range(model // step):
            cols = slice(c * step, (c + 1) * step)
            own_part[:, cols] = partial(tp, cols)

    def finish(here):
        for h in range(heads):
            cols = slice(h * value, (h + 1) * value)
            attended = (acc[h, :, here] * (1.0 / row_sum[h, 0:1, here])).T
            aout[here, cols] = (attended * jax.nn.silu(attp[here, cols].astype(F32))).astype(BF16)

    def send(d, c):
        part[d - 1, c] = partial(peer(d), far(c))
        part_copy(d, c).start()

    def send_all():
        for d in range(1, tp_count):
            aout_copy(d).start()
        for c in range(chunks):
            for d in range(1, tp_count):
                send(d, c)
        near_recurrent()
        own_rows()

    def last_block():
        for d in range(1, tp_count):
            block = lat_all.at[sp - 2, source(d)]
            remote(block, block, l_s.at[d - 1], x_r.at[d - 1], tp=source(d)).wait_recv()
        prepare(2)
        if not split:
            heads_over(False)
            finish(slice(None))
            send_all()
            return
        for d in range(1, tp_count):
            heads_over(False, share_rows(peer(d)), share)
            finish(share_rows(peer(d)))
            aout_copy(d).start()
        mine = share_rows(tp)
        sends = [(d, c) for d in range(1, tp_count) for c in range(chunks)]
        each = -(-2 * len(sends) // heads)
        tops = [score(h, False, mine, share) for h in range(heads)]
        for h in range(heads):
            for d, c in sends[h * each : (h + 1) * each]:
                send(d, c)
            mix(h, tops[h], False, mine, share)
        near_recurrent()
        finish(mine)
        own_rows()

    def no_block():
        finish(slice(None))
        send_all()

    with scope("y_last"):
        l_aout.wait()
        if sp_count > 2:
            pl.when(sp >= 2)(last_block)
            pl.when(sp < 2)(no_block)
        else:
            no_block()
    with scope("z_sum"):
        for d in range(1, tp_count):
            weight_copy(0, d).wait_recv()
            aout_copy(d).wait_recv()
        for c in range(near // step):
            cols = slice(c * step, (c + 1) * step)
            summed = own_part[:, cols].astype(F32)
            for d in range(1, tp_count):
                both = racc_in[d - 1, :, cols] + jnp.dot(
                    aout_in[d - 1], w_aout_in[d - 1, :, cols], preferred_element_type=F32
                )
                summed = summed + both.astype(BF16).astype(F32)
            out[:, cols] = summed.astype(BF16)
        for c in range(chunks):
            summed = own_part[:, far(c)].astype(F32)
            for d in range(1, tp_count):
                part_copy(d, c).wait_recv()
                summed = summed + part_in[d - 1, c].astype(F32)
            out[:, far(c)] = summed.astype(BF16)

    with scope("z_waits"):
        for d in range(1, tp_count):
            token_whole(d).wait_send()
            weight_copy(0, d).wait_send()
            weight_copy(1, d).wait_send()
            rout_copy(d).wait_send()
            aout_copy(d).wait_send()
            whole = part.at[d - 1]
            remote(whole, whole, p_s.at[d - 1], p_r.at[d - 1, 0], tp=peer(d)).wait_send()

        def all_sent(send, recv, count):
            blocks = lat_all.at[pl.ds(0, count), 0]
            remote(blocks, blocks, send, recv, tp=peer(1)).wait_send()

        for v in range(sp_count):

            @pl.when(sp == v)
            def _(v=v):
                for d in range(1, tp_count):
                    all_sent(l_s.at[d - 1], l_r.at[0, d - 1], v + 1)
                if v + 1 < sp_count:
                    rim_copy().wait_send()
                    all_sent(z_s, z_r.at[0], 1)
                    if v and sp_count > 2:
                        all_sent(y_s, y_r.at[0], 1)
                    carries = car_in.at[pl.ds(0, sp_count - 1 - v)]
                    remote(carries, carries, c_s, c_r, sp=sp + 1).wait_send()
                for e in range(3, sp_count - v):
                    direct(e).wait_send()


def body(
    tokens, norm_gain, recurrent_input, recurrent_gate, attention_gate, query_proj, latent_down,
    rope_key_down, conv_kernel, recurrence_gate_blocks, input_gate_blocks, decay_rate, decay_shift,
    initial_state, latent_gain, latent_up, query_gain, recurrent_output, attention_output,
):
    tp_count = lax.axis_size("tp")
    sp_count = lax.axis_size("sp")
    share, model = tokens.shape
    rows = share * tp_count
    width = recurrent_input.shape[1]
    taken = attention_gate.shape[1]
    head_dim = query_gain.shape[0]
    heads = query_proj.shape[1] // head_dim
    value = taken // heads
    lat = latent_down.shape[1]
    rope = rope_key_down.shape[1]
    cosine, sine = rotary_tables(sp_count * rows, rope)
    key_table = np.concatenate([cosine, cosine, -sine, sine], 1).reshape(-1, share, 2 * rope)
    query_table = np.concatenate([cosine, sine], 1).reshape(sp_count, rows, rope).transpose(0, 2, 1)
    hbm = [
        tokens, latent_down, norm_gain[None], rope_key_down.T, jnp.asarray(key_table),
        recurrent_input, query_proj, query_gain[None], jnp.asarray(query_table), conv_kernel,
        recurrence_gate_blocks, input_gate_blocks, decay_rate[None], decay_shift[None],
        recurrent_gate, attention_gate, latent_gain[None], latent_up, initial_state[None],
        recurrent_output, attention_output,
    ]
    held = [a.shape for a in hbm]
    held[4] = key_table.shape[1:]
    held[8] = query_table.shape[1:]
    vmem = pltpu.VMEM
    dma = pltpu.SemaphoreType.DMA
    others = max(tp_count - 1, 1)
    hops = max(sp_count - 1, 1)
    carries = -(-2 * width // LANES // 8) * 8
    rims = -(-4 * width // LANES // 16) * 16
    chunks = 2 if model % (4 * LANES) == 0 else 1
    return pl.pallas_call(
        functools.partial(layer_kernel, sp_count, tp_count),
        out_shape=pltpu.VMEM((share, model), BF16),
        in_specs=[pl.BlockSpec(memory_space=pl.ANY)] * len(hbm),
        out_specs=pl.BlockSpec(memory_space=pltpu.VMEM),
        scratch_shapes=[vmem(s, a.dtype) for s, a in zip(held, hbm)]
        + [
            vmem((others, share, model), BF16),
            vmem((rows, model), BF16),
            vmem((sp_count, tp_count, rows + share * rope // lat, lat), BF16),
            vmem((rows, width), BF16),
            vmem((rows, width), BF16),
            vmem((rows, taken), BF16),
            vmem((query_proj.shape[1], rows), BF16),
            vmem((heads, head_dim, rows), BF16),
            vmem((rims, LANES), BF16),
            vmem((rims, LANES), BF16),
            vmem((rows + 24, width), F32),
            vmem((LANES, LANES), BF16),
            vmem((LANES, LANES), BF16),
            vmem((rows, rows), BF16),
            vmem((rows, rows), BF16),
            vmem((rows, LANES), F32),
            vmem((rows, width), F32),
            vmem((rows, width), BF16),
            vmem((width // LANES, rows, LANES), F32),
            vmem((width // LANES, rows, LANES), F32),
            vmem((16, width), F32),
            vmem((carries, LANES), F32),
            vmem((hops, carries, LANES), F32),
            vmem((rows, width), BF16),
            vmem((rows, model), F32),
            vmem((rows, lat * tp_count), BF16),
            vmem((rows, rope), BF16),
            vmem((heads, value, rows), BF16),
            vmem((rows, latent_up.shape[1]), BF16),
            vmem((heads, rows, rows), F32),
            vmem((heads, 8, rows), F32),
            vmem((heads, 8, rows), F32),
            vmem((heads, value, rows), F32),
            vmem((rows, taken), BF16),
            vmem((others, chunks, share, model // 2 // chunks), BF16),
            vmem((share, model), BF16),
            vmem((others, chunks, share, model // 2 // chunks), BF16),
            vmem((others, taken, model // 2), BF16),
            vmem((others, width, model // 2), BF16),
            vmem((others, share, width), BF16),
            vmem((others, share, taken), BF16),
            vmem((others, share, model // 2), F32),
            dma((10,)),
            dma((others,)), dma((others,)),
            dma, dma((2,)),
            dma, dma((2,)),
            dma((max(sp_count - 3, 1),)), dma((max(sp_count - 3, 1),)),
            dma((others,)), dma((max(sp_count - 1, 1), others)),
            dma((others,)),
            dma, dma,
            dma, dma,
            dma((others,)), dma((others, chunks)),
            dma((2, others)), dma((2, others)),
            dma((others,)), dma((others,)),
            dma((others,)), dma((others,)),
            pltpu.SemaphoreType.REGULAR((hops,)),
        ],
        compiler_params=pltpu.CompilerParams(
            collective_id=0, has_side_effects=True, vmem_limit_bytes=61400 * 1024
        ),
    )(*hbm)


def solution(mesh):
    return jax.shard_map(
        body,
        mesh=mesh,
        in_specs=(
            P(("fs", "sp", "tp"), None),
            P(),
            P(None, "tp"),
            P(None, "tp"),
            P(None, "tp"),
            P(None, "tp"),
            P(None, "tp"),
            P(),
            P(None, "tp"),
            P("tp", None, None),
            P("tp", None, None),
            P("tp"),
            P(("fs", "sp")),
            P(("fs", "tp")),
            P(),
            P(None, "tp"),
            P(),
            P("tp", None),
            P("tp", None),
        ),
        out_specs=P(("fs", "sp", "tp"), None),
        check_vma=False,
    )
```

```python
import functools

import jax
import jax.numpy as jnp
import numpy as np
from jax import lax
from jax.experimental import pallas as pl
from jax.experimental.pallas import tpu as pltpu
from jax.sharding import PartitionSpec as P

EPS = 1e-06
RECURRENT_SCALE = 8.0
THETA = 10000.0
F32 = jnp.float32
BF16 = jnp.bfloat16
LANES = 128


def expm1_neg(y, root):
    small = y * (1.0 + y * (0.5 + y * (1.0 / 6 + y * (1.0 / 24 + y / 120))))
    return jnp.where(y > -0.1, small, root * root - 1.0)


def block_diagonal(scratch, blocks_ref, first):
    size = blocks_ref.shape[1]
    scratch[...] = jnp.zeros_like(scratch)
    for k in range(scratch.shape[0] // size):
        scratch[k * size : (k + 1) * size, k * size : (k + 1) * size] = blocks_ref[first + k]
    return scratch[...]


def scan_rows(decay, state):
    rows = decay.shape[0]
    row = lax.broadcasted_iota(jnp.int32, decay.shape, 0)
    step = 1
    while step < rows:
        inside = row >= step
        before_decay = jnp.where(inside, pltpu.roll(decay, step, 0), 1.0)
        before_state = jnp.where(inside, pltpu.roll(state, step, 0), 0.0)
        state = state + decay * before_state
        decay = decay * before_decay
        step *= 2
    return decay, state


def rms_scaled(values, gain_vec):
    return values * lax.rsqrt(jnp.mean(values * values, axis=-1, keepdims=True) + EPS) * gain_vec


LOG2E = 1.4426950408889634


def rotary_tables(positions, width):
    inv_freq = (1.0 / THETA ** (np.arange(0, width, 2, dtype=np.float32) / width)).astype(np.float32)
    angles = np.arange(positions, dtype=np.float32)[:, None] * inv_freq[None, :]
    cosine = np.cos(angles.astype(np.float64)).astype(np.float32)
    sine = np.sin(angles.astype(np.float64)).astype(np.float32)
    return cosine, sine


def column_step(width):
    return 256 if width % 256 == 0 else width


def remote(src, dst, send, recv, **where):
    return pltpu.make_async_remote_copy(
        src_ref=src, dst_ref=dst, send_sem=send, recv_sem=recv,
        device_id=where, device_id_type=pl.DeviceIdType.MESH,
    )


def scope(name):
    return jax.named_scope(name)


def layer_kernel(
    sp_count, tp_count,
    h_tokens, h_lat, h_norm, h_rope, h_ktab, h_in, h_query, h_qgain, h_qtab, h_conv, h_rec, h_inp,
    h_rate, h_shift, h_gate, h_att, h_lgain, h_up, h_init, h_rout, h_aout,
    out,
    tokens, w_lat, norm_gain, w_rope, key_table, w_in, w_query, query_gain, query_table,
    conv_kernel, rec_blocks, inp_blocks, decay_rate, decay_shift, w_gate, w_att, latent_gain,
    w_up, initial_state, w_rout, w_aout,
    tok_all, normed, lat_all, sig, gate, attp, turned_q, queries, rim_out, rim_in, ext, diag_a, diag_b,
    mixer, unmixer, shift, silu_gate, mixed_rout,
    prod, state, segments, car_out, car_in, rout, racc, xlat, rope_keys, turned_v, kv, held, row_max, row_sum,
    acc, aout, part, own_part, part_in, w_aout_in, w_rout_in, rout_in, aout_in, racc_in,
    w_sem, tok_s, tok_r, z_s, z_r, y_r, fwd_r, l_s, l_r, x_r, rim_s, rim_r, c_s, c_r,
    p_s, p_r, wf_s, wf_r, ro_s, ro_r, ao_s, ao_r, ready,
):
    sp = lax.axis_index("sp")
    tp = lax.axis_index("tp")
    share, model = tokens.shape
    rows = normed.shape[0]
    taps, width = conv_kernel.shape
    head_dim = query_gain.shape[1]
    rope = w_rope.shape[0]
    half = rope // 2
    nope = head_dim - rope
    heads = w_query.shape[1] // head_dim
    lat = w_lat.shape[1]
    value = w_att.shape[1] // heads
    packed = lat // rope
    tall = share // packed
    pieces = 4 if share % 64 == 0 else 1
    piece = share // pieces
    long = rows // 8

    h_refs = (
        h_tokens, h_lat, h_norm, h_rope, h_ktab.at[sp * tp_count + tp], h_in, h_query, h_qgain,
        h_qtab.at[sp], h_conv, h_rec, h_inp, h_rate, h_shift, h_gate, h_att, h_lgain, h_up,
        h_init, h_rout, h_aout,
    )
    w_refs = (
        tokens, w_lat, norm_gain, w_rope, key_table, w_in, w_query, query_gain, query_table,
        conv_kernel, rec_blocks, inp_blocks, decay_rate, decay_shift, w_gate, w_att, latent_gain,
        w_up, initial_state, w_rout, w_aout,
    )
    slots = (1, 2, 0, 3, 4, 5, 6, 0, 1, 4, 5, 0, 1, 6, 2, 3, 9, 7, 2, 3, 8)
    loads = [
        pltpu.make_async_copy(a, b, w_sem.at[k]) for a, b, k in zip(h_refs, w_refs, slots)
    ]
    token_loads = [
        pltpu.make_async_copy(
            h_tokens.at[pl.ds(k * piece, piece)], tokens.at[pl.ds(k * piece, piece)], w_sem.at[1]
        )
        for k in range(pieces)
    ]

    def peer(d):
        return lax.rem(tp + d, tp_count)

    def source(d):
        return lax.rem(tp - d + tp_count, tp_count)

    def greet(sem, **where):
        pl.semaphore_signal(sem, inc=1, device_id=where, device_id_type=pl.DeviceIdType.MESH)

    (
        l_tok, l_lat, l_norm, l_rope, l_ktab, l_in, l_query, l_qgain, l_qtab, l_conv, l_rec, l_inp,
        l_rate, l_shift, l_gate, l_att, l_lgain, l_up, l_init, l_rout, l_aout,
    ) = loads
    barrier = pltpu.get_barrier_semaphore()
    with scope("a_loads"):
        for d in range(1, tp_count):
            greet(barrier, tp=peer(d))
        for e in range(1, sp_count):
            pl.when(sp + e < sp_count)(lambda e=e: greet(barrier, sp=sp + e))
        l_norm.start()
        for load in token_loads:
            load.start()
        l_lat.start()

    def token_copy(d, k):
        part_rows = pl.ds(k * piece, piece)
        return remote(
            h_tokens.at[part_rows], tok_all.at[d - 1, part_rows],
            tok_s.at[d - 1], tok_r.at[d - 1], tp=peer(d),
        )

    near = model // 2

    def weight_copy(k, d):
        source_ref = (h_aout, h_rout)[k].at[:, pl.ds(0, near)]
        target_ref = (w_aout_in, w_rout_in)[k].at[d - 1]
        return remote(source_ref, target_ref, wf_s.at[k, d - 1], wf_r.at[k, d - 1], tp=peer(d))

    def token_whole(d):
        return remote(h_tokens, tok_all.at[d - 1], tok_s.at[d - 1], tok_r.at[d - 1], tp=peer(d))

    with scope("b_barrier"):
        pl.semaphore_wait(barrier, tp_count - 1 + sp)
        for k in range(pieces):
            for d in range(1, tp_count):
                token_copy(d, k).start()
        for e in range(1, sp_count):
            pl.when(sp >= e)(lambda e=e: greet(ready.at[e - 1], sp=sp - e))
        for load in (l_rope, l_ktab, l_in, l_query):
            load.start()

    def share_rows(place):
        return pl.ds(pl.multiple_of(place * share, share), share)

    def put_normed(block, place):
        normed[share_rows(place)] = rms_scaled(block.astype(F32), norm_gain[...]).astype(BF16)

    def put_latent(first, place):
        own[first : first + share] = jnp.dot(
            normed[share_rows(place)], w_lat[...], preferred_element_type=F32
        ).astype(BF16)

    def project(weight, into, here=slice(None)):
        step = column_step(weight.shape[1])
        for c in range(weight.shape[1] // step):
            cols = slice(c * step, (c + 1) * step)
            into[here, cols] = jnp.dot(
                normed[here], weight[:, cols], preferred_element_type=F32
            ).astype(BF16)

    own = lat_all.at[sp, tp]
    with scope("c_norm_own"):
        l_norm.wait()
        l_tok.wait()
        put_normed(tokens[...], tp)
    with scope("d_lat_a"):
        l_lat.wait()
        put_latent(0, tp)

    def along(k):
        block = lat_all.at[sp, tp, (pl.ds(0, share), pl.ds(share, rows + tall - share))[k]]
        return remote(block, block, z_s, z_r.at[k], sp=sp + 1)

    def landed(k):
        block = lat_all.at[sp - 1, tp, (pl.ds(0, share), pl.ds(share, rows + tall - share))[k]]
        return remote(block, block, z_s, z_r.at[k], sp=sp - 1)

    def direct(e):
        block = lat_all.at[sp, tp]
        return remote(block, block, z_s, fwd_r.at[e - 3], sp=sp + e)

    def forward(k):
        block = lat_all.at[sp - 1, tp, (pl.ds(0, share), pl.ds(share, rows + tall - share))[k]]
        return remote(block, block, z_s, y_r.at[k], sp=sp + 1)

    def forwarded(k):
        block = lat_all.at[sp - 2, tp, (pl.ds(0, share), pl.ds(share, rows + tall - share))[k]]
        return remote(block, block, z_s, y_r.at[k], sp=sp - 1)

    def arrived(e):
        block = lat_all.at[sp - e, tp]
        return remote(block, block, z_s, fwd_r.at[e - 3], sp=sp - 1)

    def late(e):
        return e if isinstance(e, int) and e < 2 else e - 1

    def across(e, d):
        block = lat_all.at[sp - e, tp]
        return remote(block, block, l_s.at[d - 1], l_r.at[late(e), d - 1], tp=peer(d))

    def crossed(e, d):
        block = lat_all.at[sp - e, source(d)]
        return remote(block, block, l_s.at[d - 1], l_r.at[late(e), d - 1], tp=source(d))

    def halves(k):
        return (pl.ds(0, share), pl.ds(share, rows + tall - share))[k]

    def across_piece(k, d):
        block = lat_all.at[sp - 2, tp, halves(k)]
        return remote(block, block, l_s.at[d - 1], x_r.at[d - 1], tp=peer(d))

    def cross(e):
        for d in range(1, tp_count):
            across(e, d).start()

    def wait_crossed(e):
        for d in range(1, tp_count):
            crossed(e, d).wait_recv()

    has_next = sp + 1 < sp_count
    with scope("f_send_a"):

        @pl.when(has_next)
        def _():
            pl.semaphore_wait(ready.at[0], 1)
            along(0).start()

    with scope("e_mixers"):
        row = lax.broadcasted_iota(jnp.int32, (rows, rows), 0)
        column = lax.broadcasted_iota(jnp.int32, (rows, rows), 1)
        mixer[...] = jnp.where(column == (row & 7) * long + (row >> 3), 1.0, 0.0).astype(BF16)
        unmixer[...] = jnp.where(row == (column & 7) * long + (column >> 3), 1.0, 0.0).astype(BF16)
    with scope("e_rope"):
        l_rope.wait()
        l_ktab.wait()
        raw = lax.dot_general(
            normed[share_rows(tp)], w_rope[...], (((1,), (1,)), ((), ())),
            preferred_element_type=F32,
        ).astype(BF16).astype(F32)
        swapped = jnp.concatenate([raw[:, half:], raw[:, :half]], axis=1)
        keyed = (raw * key_table[:, :rope] + swapped * key_table[:, rope:]).astype(BF16)
        for k in range(packed):
            own[share : share + tall, k * rope : (k + 1) * rope] = keyed[k * tall : (k + 1) * tall]
    with scope("g_norm_peer"):
        for d in range(1, tp_count):
            token_whole(d).wait_recv()
            put_normed(tok_all[d - 1], source(d))
    def rim_copy():
        return remote(rim_out, rim_in, rim_s, rim_r, sp=sp + 1)

    def rim_landed():
        return remote(rim_out, rim_in, rim_s, rim_r, sp=sp - 1)

    with scope("i_lat_b"):
        for d in range(1, tp_count):
            put_latent(d * share + tall, source(d))
        pl.when(has_next)(lambda: along(1).start())
        cross(0)
        for d in range(1, tp_count):
            weight_copy(0, d).start()
    with scope("h_in_peer"):
        l_in.wait()
        for load in (l_qgain, l_qtab, l_gate, l_att, l_conv, l_rec, l_up, l_lgain, l_aout):
            load.start()
        project(w_in, sig)
        tail = sig[rows - 16 :].astype(F32)[12:]
        tail = [tail[:, c * LANES : (c + 1) * LANES] for c in range(width // LANES)]
        if len(tail) * 4 < rim_out.shape[0]:
            tail.append(jnp.zeros((rim_out.shape[0] - len(tail) * 4, LANES), F32))
        rim_out[...] = jnp.concatenate(tail, axis=0).astype(BF16)
        pl.when(has_next)(lambda: rim_copy().start())
    with scope("j_query"):
        l_query.wait()
        step = column_step(w_query.shape[1])
        for c in range(w_query.shape[1] // step):
            cols = slice(c * step, (c + 1) * step)
            raw = jnp.dot(normed[...], w_query[:, cols], preferred_element_type=F32).astype(BF16)
            turned_q[cols] = raw.T
    with scope("k_rotate"):
        l_qgain.wait()
        l_qtab.wait()
        spare = -head_dim % LANES
        gain = query_gain[...]
        if spare:
            gain = jnp.concatenate([gain, jnp.zeros((1, spare), F32)], axis=1)
        gain = jnp.broadcast_to(gain, (LANES, head_dim + spare)).T[:head_dim]
        gain = jnp.concatenate([gain] * (rows // LANES), axis=1)
        cosine = query_table[:half]
        sine = query_table[half:]
        for h in range(heads):
            head = turned_q[h * head_dim : (h + 1) * head_dim].astype(F32)
            square = jnp.sum(head * head, axis=0, keepdims=True)
            head = head * lax.rsqrt(square / head_dim + EPS) * gain
            first, second = head[nope : nope + half], head[nope + half :]
            queries[h, :nope] = head[:nope].astype(BF16)
            queries[h, nope : nope + half] = (first * cosine - second * sine).astype(BF16)
            queries[h, nope + half :] = (first * sine + second * cosine).astype(BF16)
        for load in (l_inp, l_rate, l_shift):
            load.start()

    def relay1(k):
        if sp_count > 1:

            @pl.when(sp >= 1)
            def _():
                landed(k).wait_recv()
                if sp_count > 2:
                    pl.when(has_next)(lambda: forward(k).start())
                if k:
                    cross(1)

    with scope("p_relay1a"):
        relay1(0)

    with scope("q_gates"):
        l_gate.wait()
        project(w_gate, gate)
        for e in range(2, sp_count):

            @pl.when(sp + e < sp_count)
            def _(e=e):
                pl.semaphore_wait(ready.at[e - 1], 1)
                if e > 2:
                    direct(e).start()

        silu_gate[...] = jax.nn.silu(
            jnp.dot(mixer[...], gate[...], preferred_element_type=F32)
        )

    with scope("q_gate_att"):
        l_att.wait()
        project(w_att, attp)
        for load in (l_init, l_rout):
            load.start()

    with scope("p_relay1b"):
        relay1(1)
        for d in range(1, tp_count):
            weight_copy(1, d).start()
    with scope("m_rim"):

        @pl.when(sp == 0)
        def _():
            rim_in[...] = jnp.zeros_like(rim_in)

        pl.when(sp > 0)(lambda: rim_landed().wait_recv())
    with scope("n_scan"):
        for load in (l_conv, l_rec, l_inp, l_rate, l_shift):
            load.wait()
        size = rec_blocks.shape[1]
        car_out[...] = jnp.zeros_like(car_out)
        lead = 8 * (taps - 1)
        ext[lead : lead + rows] = jnp.dot(mixer[...], sig[...], preferred_element_type=F32)
        top_row = lax.broadcasted_iota(jnp.int32, (8, width), 0) == 0
        rim = rim_in[...].astype(F32)
        rim = jnp.concatenate(
            [rim[4 * c : 4 * c + 4] for c in range(width // LANES)], axis=1
        )
        for k in range(1, taps):
            last = ext[lead + rows - 8 * k : lead + rows - 8 * k + 8]
            ext[lead - 8 * k : lead - 8 * k + 8] = jnp.where(
                top_row, rim[4 - k : 5 - k], pltpu.roll(last, 1, 0)
            )
        table = jnp.concatenate(
            [decay_shift[:, k * long : (k + 1) * long] for k in range(8)], axis=0
        )
        for i in range(long):
            shift[8 * i : 8 * i + 8] = jnp.broadcast_to(table[:, i : i + 1], (8, LANES))
        groups = width // LANES
        for c in range(groups):
            cols = slice(c * LANES, (c + 1) * LANES)
            conv = conv_kernel[0:1, cols] * ext[0:rows, cols]
            for j in range(1, taps):
                conv = conv + conv_kernel[j : j + 1, cols] * ext[8 * j : 8 * j + rows, cols]
            conv = conv.astype(BF16)
            per = LANES // size
            rec = jax.nn.sigmoid(
                jnp.dot(conv, block_diagonal(diag_a, rec_blocks, c * per), preferred_element_type=F32)
            )
            inp = jax.nn.sigmoid(
                jnp.dot(conv, block_diagonal(diag_b, inp_blocks, c * per), preferred_element_type=F32)
            )
            log_decay = -RECURRENT_SCALE * rec * decay_rate[0:1, cols] + shift[...]
            decay = jnp.exp(log_decay)
            prod[c] = decay
            state[c] = jnp.sqrt(-expm1_neg(2.0 * log_decay, decay)) * inp * conv.astype(F32)
        ones = [prod[c, 0:8] for c in range(groups)]
        twos = [state[c, 0:8] for c in range(groups)]
        for i in range(1, long):
            here = slice(8 * i, 8 * i + 8)
            for c in range(groups):
                decay = prod[c, here]
                twos[c] = decay * twos[c] + state[c, here]
                ones[c] = decay * ones[c]
                prod[c, here] = ones[c]
                state[c, here] = twos[c]
        first_row = lax.broadcasted_iota(jnp.int32, (8, LANES), 0) == 0
        for c in range(groups):
            cols = slice(c * LANES, (c + 1) * LANES)
            one, two = scan_rows(ones[c], twos[c])
            segments[0:8, cols] = jnp.where(first_row, 1.0, pltpu.roll(one, 1, 0))
            segments[8:16, cols] = jnp.where(first_row, 0.0, pltpu.roll(two, 1, 0))
            car_out[2 * c : 2 * c + 1] = one[7:8]
            car_out[2 * c + 1 : 2 * c + 2] = two[7:8]

    def carry_copy(e):
        return remote(car_out, car_in.at[e - 1], c_s, c_r, sp=sp + e)

    def carry_landed(e):
        return remote(car_out, car_in.at[e - 1], c_s, c_r, sp=sp - e)

    with scope("o_carry"):
        for e in range(1, sp_count):
            pl.when(sp + e < sp_count)(lambda e=e: carry_copy(e).start())
    factor = head_dim ** (-0.5) * LOG2E

    def prepare(e):
        place = sp - e
        blocks = []
        for n in range(tp_count):
            order = [(n - r) % tp_count for r in range(tp_count)]
            first = [0 if j == 0 else tall + j * share for j in order]
            blocks.append(
                jnp.concatenate([lat_all[place, n, f : f + share] for f in first], axis=0).astype(F32)
            )
        square = sum(jnp.sum(x * x, axis=-1, keepdims=True) for x in blocks)
        inverse = lax.rsqrt(square / (lat * tp_count) + EPS)
        for n, x in enumerate(blocks):
            cols = slice(n * lat, (n + 1) * lat)
            xlat[:, cols] = (x * inverse * latent_gain[0:1, cols]).astype(BF16)
        rope_keys[...] = jnp.concatenate(
            [
                lat_all[place, n, share : share + tall, k * rope : (k + 1) * rope]
                for n in range(tp_count)
                for k in range(packed)
            ],
            axis=0,
        )
        step = column_step(w_up.shape[1])
        for c in range(w_up.shape[1] // step):
            cols = slice(c * step, (c + 1) * step)
            kv[:, cols] = jnp.dot(xlat[...], w_up[:, cols], preferred_element_type=F32).astype(BF16)
        for h in range(heads):
            base = h * (nope + value) + nope
            turned_v[h] = kv[:, base : base + value].T

    def score(h, diagonal, lanes, count):
        base = h * (nope + value)
        keys = jnp.concatenate([kv[:, base : base + nope], rope_keys[...]], axis=1)
        scores = jnp.dot(keys, queries[h, :, lanes], preferred_element_type=F32) * factor
        if diagonal:
            seen = lax.broadcasted_iota(jnp.int32, scores.shape, 0)
            scores = jnp.where(
                seen <= lax.broadcasted_iota(jnp.int32, scores.shape, 1), scores, -jnp.inf
            )
        held[h, :, :count] = scores
        return jnp.max(scores, axis=0, keepdims=True)

    def mix(h, top, diagonal, lanes, count):
        if not diagonal:
            before = row_max[h, 0:1, lanes]
            top = jnp.maximum(top, before)
            fade = jnp.exp2(before - top)
        weights = jnp.exp2(held[h, :, :count] - top)
        mass = jnp.sum(weights, axis=0, keepdims=True)
        term = jnp.dot(turned_v[h], weights.astype(BF16), preferred_element_type=F32)
        if not diagonal:
            mass = mass + row_sum[h, 0:1, lanes] * fade
            term = term + acc[h, :, lanes] * fade
        row_max[h, 0:1, lanes] = top
        row_sum[h, 0:1, lanes] = mass
        acc[h, :, lanes] = term

    def heads_over(diagonal, lanes=slice(None), count=rows):
        tops = [score(h, diagonal, lanes, count) for h in range(heads)]
        for h in range(heads):
            mix(h, tops[h], diagonal, lanes, count)

    def attend(e, diagonal):
        prepare(e)
        heads_over(diagonal)

    with scope("r_att0"):
        l_lgain.wait()
        l_up.wait()
        wait_crossed(0)
        prepare(0)
    with scope("r_att0_heads"):
        heads_over(True)
    with scope("t_relay3"):
        if sp_count > 3:

            @pl.when(sp >= 3)
            def _():
                arrived(3).wait_recv()
                cross(3)

    with scope("s_att1"):
        if sp_count > 1:

            @pl.when(sp >= 1)
            def _():
                wait_crossed(1)
                attend(1, False)

    with scope("w_att3"):
        if sp_count > 3:

            @pl.when(sp >= 3)
            def _():
                wait_crossed(3)
                attend(3, False)

        if sp_count > 4:

            def later(e, carry):
                block = lat_all.at[sp - e, tp]
                remote(block, block, z_s, fwd_r.at[e - 3], sp=sp - 1).wait_recv()
                cross(e)
                wait_crossed(e)
                attend(e, False)
                return carry

            lax.fori_loop(4, sp + 1, later, 0)
    with scope("x_relay2"):
        if sp_count > 2:

            @pl.when(sp >= 2)
            def _():
                for k in range(2):
                    forwarded(k).wait_recv()
                    for d in range(1, tp_count):
                        across_piece(k, d).start()

    with scope("u_carrywait"):
        for v in range(1, sp_count):

            @pl.when(sp == v)
            def _(v=v):
                remote(car_in.at[pl.ds(0, v)], car_in.at[pl.ds(0, v)], c_s, c_r, sp=sp - 1).wait_recv()

        for e in range(1, sp_count):

            @pl.when(sp < e)
            def _(e=e):
                row = lax.broadcasted_iota(jnp.int32, car_out.shape, 0)
                car_in[e - 1] = jnp.where((row & 1) == 0, 1.0, 0.0)

    def rout_copy(d):
        return remote(
            rout.at[share_rows(peer(d))], rout_in.at[d - 1], ro_s.at[d - 1], ro_r.at[d - 1], tp=peer(d)
        )

    def aout_copy(d):
        return remote(
            aout.at[share_rows(peer(d))], aout_in.at[d - 1], ao_s.at[d - 1], ao_r.at[d - 1], tp=peer(d)
        )

    with scope("v_rout"):
        l_init.wait()
        for c in range(width // LANES):
            cols = slice(c * LANES, (c + 1) * LANES)
            incoming = initial_state[:, cols]
            for e in range(sp_count - 1, 0, -1):
                incoming = (
                    car_in[e - 1, 2 * c : 2 * c + 1] * incoming
                    + car_in[e - 1, 2 * c + 1 : 2 * c + 2]
                )
            enter = segments[0:8, cols] * incoming + segments[8:16, cols]
            full = state[c] + prod[c] * jnp.concatenate([enter] * long, axis=0)
            mixed_rout[:, cols] = (full * silu_gate[:, cols]).astype(BF16)
        rout[...] = jnp.dot(
            unmixer[...], mixed_rout[...], preferred_element_type=F32
        ).astype(BF16)
        l_rout.wait()
        for d in range(1, tp_count):
            rout_copy(d).start()
        step = column_step(near)
        for c in range(near // step):
            cols = slice(near + c * step, near + (c + 1) * step)
            racc[:, cols] = jnp.dot(rout[...], w_rout[:, cols], preferred_element_type=F32)
        for c in range(near // step):
            cols = slice(c * step, (c + 1) * step)
            here = share_rows(tp)
            racc[here, cols] = jnp.dot(rout[here], w_rout[:, cols], preferred_element_type=F32)
    chunks, step = part_in.shape[1], part_in.shape[3]
    split = share % LANES == 0

    def part_copy(d, c):
        return remote(
            part.at[d - 1, c], part_in.at[d - 1, c], p_s.at[d - 1], p_r.at[d - 1, c], tp=peer(d)
        )

    def partial(place, cols):
        here = share_rows(place)
        both = racc[here, cols] + jnp.dot(aout[here], w_aout[:, cols], preferred_element_type=F32)
        return both.astype(BF16)

    def far(c):
        return slice(near + c * step, near + (c + 1) * step)

    def near_recurrent():
        for d in range(1, tp_count):
            rout_copy(d).wait_recv()
            weight_copy(1, d).wait_recv()
            for c in range(near // step):
                cols = slice(c * step, (c + 1) * step)
                racc_in[d - 1, :, cols] = jnp.dot(
                    rout_in[d - 1], w_rout_in[d - 1, :, cols], preferred_element_type=F32
                )

    def own_rows():
        for c in range(model // step):
            cols = slice(c * step, (c + 1) * step)
            own_part[:, cols] = partial(tp, cols)

    def finish(here):
        for h in range(heads):
            cols = slice(h * value, (h + 1) * value)
            attended = (acc[h, :, here] * (1.0 / row_sum[h, 0:1, here])).T
            aout[here, cols] = (attended * jax.nn.silu(attp[here, cols].astype(F32))).astype(BF16)

    def send(d, c):
        part[d - 1, c] = partial(peer(d), far(c))
        part_copy(d, c).start()

    def send_all():
        for d in range(1, tp_count):
            aout_copy(d).start()
        for c in range(chunks):
            for d in range(1, tp_count):
                send(d, c)
        near_recurrent()
        own_rows()

    def last_block():
        for d in range(1, tp_count):
            block = lat_all.at[sp - 2, source(d)]
            remote(block, block, l_s.at[d - 1], x_r.at[d - 1], tp=source(d)).wait_recv()
        prepare(2)
        if not split:
            heads_over(False)
            finish(slice(None))
            send_all()
            return
        for d in range(1, tp_count):
            heads_over(False, share_rows(peer(d)), share)
            finish(share_rows(peer(d)))
            aout_copy(d).start()
        mine = share_rows(tp)
        sends = [(d, c) for d in range(1, tp_count) for c in range(chunks)]
        each = -(-2 * len(sends) // heads)
        tops = [score(h, False, mine, share) for h in range(heads)]
        for h in range(heads):
            for d, c in sends[h * each : (h + 1) * each]:
                send(d, c)
            mix(h, tops[h], False, mine, share)
        near_recurrent()
        finish(mine)
        own_rows()

    def no_block():
        finish(slice(None))
        send_all()

    with scope("y_last"):
        l_aout.wait()
        if sp_count > 2:
            pl.when(sp >= 2)(last_block)
            pl.when(sp < 2)(no_block)
        else:
            no_block()
    with scope("z_sum"):
        for d in range(1, tp_count):
            weight_copy(0, d).wait_recv()
            aout_copy(d).wait_recv()
        for c in range(near // step):
            cols = slice(c * step, (c + 1) * step)
            summed = own_part[:, cols].astype(F32)
            for d in range(1, tp_count):
                both = racc_in[d - 1, :, cols] + jnp.dot(
                    aout_in[d - 1], w_aout_in[d - 1, :, cols], preferred_element_type=F32
                )
                summed = summed + both.astype(BF16).astype(F32)
            out[:, cols] = summed.astype(BF16)
        for c in range(chunks):
            summed = own_part[:, far(c)].astype(F32)
            for d in range(1, tp_count):
                part_copy(d, c).wait_recv()
                summed = summed + part_in[d - 1, c].astype(F32)
            out[:, far(c)] = summed.astype(BF16)

    with scope("z_waits"):
        for d in range(1, tp_count):
            token_whole(d).wait_send()
            weight_copy(0, d).wait_send()
            weight_copy(1, d).wait_send()
            rout_copy(d).wait_send()
            aout_copy(d).wait_send()
            whole = part.at[d - 1]
            remote(whole, whole, p_s.at[d - 1], p_r.at[d - 1, 0], tp=peer(d)).wait_send()

        def all_sent(send, recv, count):
            blocks = lat_all.at[pl.ds(0, count), 0]
            remote(blocks, blocks, send, recv, tp=peer(1)).wait_send()

        for v in range(sp_count):

            @pl.when(sp == v)
            def _(v=v):
                for d in range(1, tp_count):
                    all_sent(l_s.at[d - 1], l_r.at[0, d - 1], v + 1)
                if v + 1 < sp_count:
                    rim_copy().wait_send()
                    onward = int(v > 0 and sp_count > 2)
                    all_sent(z_s, z_r.at[0], 1 + onward + max(sp_count - 3 - v, 0))
                    carries = car_in.at[pl.ds(0, sp_count - 1 - v)]
                    remote(carries, carries, c_s, c_r, sp=sp + 1).wait_send()


def body(
    tokens, norm_gain, recurrent_input, recurrent_gate, attention_gate, query_proj, latent_down,
    rope_key_down, conv_kernel, recurrence_gate_blocks, input_gate_blocks, decay_rate, decay_shift,
    initial_state, latent_gain, latent_up, query_gain, recurrent_output, attention_output,
):
    tp_count = lax.axis_size("tp")
    sp_count = lax.axis_size("sp")
    share, model = tokens.shape
    rows = share * tp_count
    width = recurrent_input.shape[1]
    taken = attention_gate.shape[1]
    head_dim = query_gain.shape[0]
    heads = query_proj.shape[1] // head_dim
    value = taken // heads
    lat = latent_down.shape[1]
    rope = rope_key_down.shape[1]
    cosine, sine = rotary_tables(sp_count * rows, rope)
    key_table = np.concatenate([cosine, cosine, -sine, sine], 1).reshape(-1, share, 2 * rope)
    query_table = np.concatenate([cosine, sine], 1).reshape(sp_count, rows, rope).transpose(0, 2, 1)
    hbm = [
        tokens, latent_down, norm_gain[None], rope_key_down.T, jnp.asarray(key_table),
        recurrent_input, query_proj, query_gain[None], jnp.asarray(query_table), conv_kernel,
        recurrence_gate_blocks, input_gate_blocks, decay_rate[None], decay_shift[None],
        recurrent_gate, attention_gate, latent_gain[None], latent_up, initial_state[None],
        recurrent_output, attention_output,
    ]
    held = [a.shape for a in hbm]
    held[4] = key_table.shape[1:]
    held[8] = query_table.shape[1:]
    vmem = pltpu.VMEM
    dma = pltpu.SemaphoreType.DMA
    others = max(tp_count - 1, 1)
    hops = max(sp_count - 1, 1)
    carries = -(-2 * width // LANES // 8) * 8
    rims = -(-4 * width // LANES // 16) * 16
    chunks = 1
    return pl.pallas_call(
        functools.partial(layer_kernel, sp_count, tp_count),
        out_shape=pltpu.VMEM((share, model), BF16),
        in_specs=[pl.BlockSpec(memory_space=pl.ANY)] * len(hbm),
        out_specs=pl.BlockSpec(memory_space=pltpu.VMEM),
        scratch_shapes=[vmem(s, a.dtype) for s, a in zip(held, hbm)]
        + [
            vmem((others, share, model), BF16),
            vmem((rows, model), BF16),
            vmem((sp_count, tp_count, rows + share * rope // lat, lat), BF16),
            vmem((rows, width), BF16),
            vmem((rows, width), BF16),
            vmem((rows, taken), BF16),
            vmem((query_proj.shape[1], rows), BF16),
            vmem((heads, head_dim, rows), BF16),
            vmem((rims, LANES), BF16),
            vmem((rims, LANES), BF16),
            vmem((rows + 24, width), F32),
            vmem((LANES, LANES), BF16),
            vmem((LANES, LANES), BF16),
            vmem((rows, rows), BF16),
            vmem((rows, rows), BF16),
            vmem((rows, LANES), F32),
            vmem((rows, width), F32),
            vmem((rows, width), BF16),
            vmem((width // LANES, rows, LANES), F32),
            vmem((width // LANES, rows, LANES), F32),
            vmem((16, width), F32),
            vmem((carries, LANES), F32),
            vmem((hops, carries, LANES), F32),
            vmem((rows, width), BF16),
            vmem((rows, model), F32),
            vmem((rows, lat * tp_count), BF16),
            vmem((rows, rope), BF16),
            vmem((heads, value, rows), BF16),
            vmem((rows, latent_up.shape[1]), BF16),
            vmem((heads, rows, rows), F32),
            vmem((heads, 8, rows), F32),
            vmem((heads, 8, rows), F32),
            vmem((heads, value, rows), F32),
            vmem((rows, taken), BF16),
            vmem((others, chunks, share, model // 2 // chunks), BF16),
            vmem((share, model), BF16),
            vmem((others, chunks, share, model // 2 // chunks), BF16),
            vmem((others, taken, model // 2), BF16),
            vmem((others, width, model // 2), BF16),
            vmem((others, share, width), BF16),
            vmem((others, share, taken), BF16),
            vmem((others, share, model // 2), F32),
            dma((10,)),
            dma((others,)), dma((others,)),
            dma, dma((2,)),
            dma((2,)),
            dma((max(sp_count - 3, 1),)),
            dma((others,)), dma((max(sp_count - 1, 1), others)),
            dma((others,)),
            dma, dma,
            dma, dma,
            dma((others,)), dma((others, chunks)),
            dma((2, others)), dma((2, others)),
            dma((others,)), dma((others,)),
            dma((others,)), dma((others,)),
            pltpu.SemaphoreType.REGULAR((hops,)),
        ],
        compiler_params=pltpu.CompilerParams(
            collective_id=0, has_side_effects=True, vmem_limit_bytes=61400 * 1024
        ),
    )(*hbm)


def solution(mesh):
    return jax.shard_map(
        body,
        mesh=mesh,
        in_specs=(
            P(("fs", "sp", "tp"), None),
            P(),
            P(None, "tp"),
            P(None, "tp"),
            P(None, "tp"),
            P(None, "tp"),
            P(None, "tp"),
            P(),
            P(None, "tp"),
            P("tp", None, None),
            P("tp", None, None),
            P("tp"),
            P(("fs", "sp")),
            P(("fs", "tp")),
            P(),
            P(None, "tp"),
            P(),
            P("tp", None),
            P("tp", None),
        ),
        out_specs=P(("fs", "sp", "tp"), None),
        check_vma=False,
    )
```

```python
import functools

import jax
import jax.numpy as jnp
import numpy as np
from jax import lax
from jax.experimental import pallas as pl
from jax.experimental.pallas import tpu as pltpu
from jax.sharding import PartitionSpec as P

EPS = 1e-06
RECURRENT_SCALE = 8.0
THETA = 10000.0
F32 = jnp.float32
BF16 = jnp.bfloat16
LANES = 128


def expm1_neg(y, root):
    small = y * (1.0 + y * (0.5 + y * (1.0 / 6 + y * (1.0 / 24 + y / 120))))
    return jnp.where(y > -0.1, small, root * root - 1.0)


def block_diagonal(scratch, blocks_ref, first):
    size = blocks_ref.shape[1]
    scratch[...] = jnp.zeros_like(scratch)
    for k in range(scratch.shape[0] // size):
        scratch[k * size : (k + 1) * size, k * size : (k + 1) * size] = blocks_ref[first + k]
    return scratch[...]


def scan_rows(decay, state):
    rows = decay.shape[0]
    row = lax.broadcasted_iota(jnp.int32, decay.shape, 0)
    step = 1
    while step < rows:
        inside = row >= step
        before_decay = jnp.where(inside, pltpu.roll(decay, step, 0), 1.0)
        before_state = jnp.where(inside, pltpu.roll(state, step, 0), 0.0)
        state = state + decay * before_state
        decay = decay * before_decay
        step *= 2
    return decay, state


def rms_scaled(values, gain_vec):
    return values * lax.rsqrt(jnp.mean(values * values, axis=-1, keepdims=True) + EPS) * gain_vec


LOG2E = 1.4426950408889634


def rotary_tables(positions, width):
    inv_freq = (1.0 / THETA ** (np.arange(0, width, 2, dtype=np.float32) / width)).astype(np.float32)
    angles = np.arange(positions, dtype=np.float32)[:, None] * inv_freq[None, :]
    cosine = np.cos(angles.astype(np.float64)).astype(np.float32)
    sine = np.sin(angles.astype(np.float64)).astype(np.float32)
    return cosine, sine


def column_step(width):
    return 256 if width % 256 == 0 else width


def remote(src, dst, send, recv, **where):
    return pltpu.make_async_remote_copy(
        src_ref=src, dst_ref=dst, send_sem=send, recv_sem=recv,
        device_id=where, device_id_type=pl.DeviceIdType.MESH,
    )


def scope(name):
    return jax.named_scope(name)


def layer_kernel(
    sp_count, tp_count,
    h_tokens, h_lat, h_norm, h_rope, h_ktab, h_in, h_query, h_qgain, h_qtab, h_conv, h_rec, h_inp,
    h_rate, h_shift, h_gate, h_att, h_lgain, h_up, h_init, h_rout, h_aout,
    out,
    tokens, w_lat, norm_gain, w_rope, key_table, w_in, w_query, query_gain, query_table,
    conv_kernel, rec_blocks, inp_blocks, decay_rate, decay_shift, w_gate, w_att, latent_gain,
    w_up, initial_state, w_rout, w_aout,
    tok_all, normed, lat_all, sig, gate, attp, turned_q, queries, rim_out, rim_in, ext, diag_a, diag_b,
    mixer, unmixer, shift, silu_gate, silu_att, mixed_rout,
    prod, state, segments, car_out, car_in, rout, racc, xlat, rope_keys, turned_v, kv, held, row_max, row_sum,
    acc, aout, part, own_part, part_in, w_aout_in, w_rout_in, rout_in, aout_in, racc_in,
    w_sem, tok_s, tok_r, z_s, z_r, y_r, fwd_r, l_s, l_r, x_r, rim_s, rim_r, c_s, c_r,
    p_s, p_r, wf_s, wf_r, ro_s, ro_r, ao_s, ao_r, ready,
):
    sp = lax.axis_index("sp")
    tp = lax.axis_index("tp")
    share, model = tokens.shape
    rows = normed.shape[0]
    taps, width = conv_kernel.shape
    head_dim = query_gain.shape[1]
    rope = w_rope.shape[0]
    half = rope // 2
    nope = head_dim - rope
    heads = w_query.shape[1] // head_dim
    lat = w_lat.shape[1]
    value = w_att.shape[1] // heads
    packed = lat // rope
    tall = share // packed
    pieces = 4 if share % 64 == 0 else 1
    piece = share // pieces
    long = rows // 8

    h_refs = (
        h_tokens, h_lat, h_norm, h_rope, h_ktab.at[sp * tp_count + tp], h_in, h_query, h_qgain,
        h_qtab.at[sp], h_conv, h_rec, h_inp, h_rate, h_shift, h_gate, h_att, h_lgain, h_up,
        h_init, h_rout, h_aout,
    )
    w_refs = (
        tokens, w_lat, norm_gain, w_rope, key_table, w_in, w_query, query_gain, query_table,
        conv_kernel, rec_blocks, inp_blocks, decay_rate, decay_shift, w_gate, w_att, latent_gain,
        w_up, initial_state, w_rout, w_aout,
    )
    slots = (1, 2, 0, 3, 4, 5, 6, 0, 1, 4, 5, 0, 1, 6, 2, 3, 9, 7, 2, 3, 8)
    loads = [
        pltpu.make_async_copy(a, b, w_sem.at[k]) for a, b, k in zip(h_refs, w_refs, slots)
    ]
    token_loads = [
        pltpu.make_async_copy(
            h_tokens.at[pl.ds(k * piece, piece)], tokens.at[pl.ds(k * piece, piece)], w_sem.at[1]
        )
        for k in range(pieces)
    ]

    def peer(d):
        return lax.rem(tp + d, tp_count)

    def source(d):
        return lax.rem(tp - d + tp_count, tp_count)

    def greet(sem, **where):
        pl.semaphore_signal(sem, inc=1, device_id=where, device_id_type=pl.DeviceIdType.MESH)

    (
        l_tok, l_lat, l_norm, l_rope, l_ktab, l_in, l_query, l_qgain, l_qtab, l_conv, l_rec, l_inp,
        l_rate, l_shift, l_gate, l_att, l_lgain, l_up, l_init, l_rout, l_aout,
    ) = loads
    barrier = pltpu.get_barrier_semaphore()
    with scope("a_loads"):
        for d in range(1, tp_count):
            greet(barrier, tp=peer(d))
        for e in range(1, sp_count):
            pl.when(sp + e < sp_count)(lambda e=e: greet(barrier, sp=sp + e))
        l_norm.start()
        for load in token_loads:
            load.start()
        l_lat.start()

    def token_copy(d, k):
        part_rows = pl.ds(k * piece, piece)
        return remote(
            h_tokens.at[part_rows], tok_all.at[d - 1, part_rows],
            tok_s.at[d - 1], tok_r.at[d - 1], tp=peer(d),
        )

    near = model // 2

    def weight_copy(k, d):
        source_ref = (h_aout, h_rout)[k].at[:, pl.ds(0, near)]
        target_ref = (w_aout_in, w_rout_in)[k].at[d - 1]
        return remote(source_ref, target_ref, wf_s.at[k, d - 1], wf_r.at[k, d - 1], tp=peer(d))

    def token_whole(d):
        return remote(h_tokens, tok_all.at[d - 1], tok_s.at[d - 1], tok_r.at[d - 1], tp=peer(d))

    with scope("b_barrier"):
        pl.semaphore_wait(barrier, tp_count - 1 + sp)
        for k in range(pieces):
            for d in range(1, tp_count):
                token_copy(d, k).start()
        for e in range(1, sp_count):
            pl.when(sp >= e)(lambda e=e: greet(ready.at[e - 1], sp=sp - e))
        for load in (l_rope, l_ktab, l_in, l_query):
            load.start()

    def share_rows(place):
        return pl.ds(pl.multiple_of(place * share, share), share)

    def put_normed(block, place):
        normed[share_rows(place)] = rms_scaled(block.astype(F32), norm_gain[...]).astype(BF16)

    def put_latent(first, place):
        own[first : first + share] = jnp.dot(
            normed[share_rows(place)], w_lat[...], preferred_element_type=F32
        ).astype(BF16)

    def project(weight, into, here=slice(None)):
        step = column_step(weight.shape[1])
        for c in range(weight.shape[1] // step):
            cols = slice(c * step, (c + 1) * step)
            into[here, cols] = jnp.dot(
                normed[here], weight[:, cols], preferred_element_type=F32
            ).astype(BF16)

    own = lat_all.at[sp, tp]
    with scope("c_norm_own"):
        l_norm.wait()
        l_tok.wait()
        put_normed(tokens[...], tp)
    with scope("d_lat_a"):
        l_lat.wait()
        put_latent(0, tp)

    def along(k):
        block = lat_all.at[sp, tp, (pl.ds(0, share), pl.ds(share, rows + tall - share))[k]]
        return remote(block, block, z_s, z_r.at[k], sp=sp + 1)

    def landed(k):
        block = lat_all.at[sp - 1, tp, (pl.ds(0, share), pl.ds(share, rows + tall - share))[k]]
        return remote(block, block, z_s, z_r.at[k], sp=sp - 1)

    def direct(e):
        block = lat_all.at[sp, tp]
        return remote(block, block, z_s, fwd_r.at[e - 3], sp=sp + e)

    def forward(k):
        block = lat_all.at[sp - 1, tp, (pl.ds(0, share), pl.ds(share, rows + tall - share))[k]]
        return remote(block, block, z_s, y_r.at[k], sp=sp + 1)

    def forwarded(k):
        block = lat_all.at[sp - 2, tp, (pl.ds(0, share), pl.ds(share, rows + tall - share))[k]]
        return remote(block, block, z_s, y_r.at[k], sp=sp - 1)

    def arrived(e):
        block = lat_all.at[sp - e, tp]
        return remote(block, block, z_s, fwd_r.at[e - 3], sp=sp - 1)

    def late(e):
        return e if isinstance(e, int) and e < 2 else e - 1

    def across(e, d):
        block = lat_all.at[sp - e, tp]
        return remote(block, block, l_s.at[d - 1], l_r.at[late(e), d - 1], tp=peer(d))

    def crossed(e, d):
        block = lat_all.at[sp - e, source(d)]
        return remote(block, block, l_s.at[d - 1], l_r.at[late(e), d - 1], tp=source(d))

    def halves(k):
        return (pl.ds(0, share), pl.ds(share, rows + tall - share))[k]

    def across_piece(k, d):
        block = lat_all.at[sp - 2, tp, halves(k)]
        return remote(block, block, l_s.at[d - 1], x_r.at[d - 1], tp=peer(d))

    def cross(e):
        for d in range(1, tp_count):
            across(e, d).start()

    def wait_crossed(e):
        for d in range(1, tp_count):
            crossed(e, d).wait_recv()

    has_next = sp + 1 < sp_count
    with scope("f_send_a"):

        @pl.when(has_next)
        def _():
            pl.semaphore_wait(ready.at[0], 1)
            along(0).start()

    with scope("e_mixers"):
        row = lax.broadcasted_iota(jnp.int32, (rows, rows), 0)
        column = lax.broadcasted_iota(jnp.int32, (rows, rows), 1)
        mixer[...] = jnp.where(column == (row & 7) * long + (row >> 3), 1.0, 0.0).astype(BF16)
        unmixer[...] = jnp.where(row == (column & 7) * long + (column >> 3), 1.0, 0.0).astype(BF16)
    with scope("e_rope"):
        l_rope.wait()
        l_ktab.wait()
        raw = lax.dot_general(
            normed[share_rows(tp)], w_rope[...], (((1,), (1,)), ((), ())),
            preferred_element_type=F32,
        ).astype(BF16).astype(F32)
        swapped = jnp.concatenate([raw[:, half:], raw[:, :half]], axis=1)
        keyed = (raw * key_table[:, :rope] + swapped * key_table[:, rope:]).astype(BF16)
        for k in range(packed):
            own[share : share + tall, k * rope : (k + 1) * rope] = keyed[k * tall : (k + 1) * tall]
    with scope("g_norm_peer"):
        for d in range(1, tp_count):
            token_whole(d).wait_recv()
            put_normed(tok_all[d - 1], source(d))
    def rim_copy():
        return remote(rim_out, rim_in, rim_s, rim_r, sp=sp + 1)

    def rim_landed():
        return remote(rim_out, rim_in, rim_s, rim_r, sp=sp - 1)

    with scope("i_lat_b"):
        for d in range(1, tp_count):
            put_latent(d * share + tall, source(d))
        pl.when(has_next)(lambda: along(1).start())
        cross(0)
        for d in range(1, tp_count):
            weight_copy(0, d).start()
    with scope("h_in_peer"):
        l_in.wait()
        for load in (l_qgain, l_qtab, l_gate, l_att, l_conv, l_rec, l_up, l_lgain, l_aout):
            load.start()
        project(w_in, sig)
        tail = sig[rows - 16 :].astype(F32)[12:]
        tail = [tail[:, c * LANES : (c + 1) * LANES] for c in range(width // LANES)]
        if len(tail) * 4 < rim_out.shape[0]:
            tail.append(jnp.zeros((rim_out.shape[0] - len(tail) * 4, LANES), F32))
        rim_out[...] = jnp.concatenate(tail, axis=0).astype(BF16)
        pl.when(has_next)(lambda: rim_copy().start())
    with scope("j_query"):
        l_query.wait()
        step = column_step(w_query.shape[1])
        for c in range(w_query.shape[1] // step):
            cols = slice(c * step, (c + 1) * step)
            raw = jnp.dot(normed[...], w_query[:, cols], preferred_element_type=F32).astype(BF16)
            turned_q[cols] = raw.T
    with scope("k_rotate"):
        l_qgain.wait()
        l_qtab.wait()
        spare = -head_dim % LANES
        gain = query_gain[...]
        if spare:
            gain = jnp.concatenate([gain, jnp.zeros((1, spare), F32)], axis=1)
        gain = jnp.broadcast_to(gain, (LANES, head_dim + spare)).T[:head_dim]
        gain = jnp.concatenate([gain] * (rows // LANES), axis=1)
        cosine = query_table[:half]
        sine = query_table[half:]
        for h in range(heads):
            head = turned_q[h * head_dim : (h + 1) * head_dim].astype(F32)
            square = jnp.sum(head * head, axis=0, keepdims=True)
            head = head * lax.rsqrt(square / head_dim + EPS) * gain
            first, second = head[nope : nope + half], head[nope + half :]
            queries[h, :nope] = head[:nope].astype(BF16)
            queries[h, nope : nope + half] = (first * cosine - second * sine).astype(BF16)
            queries[h, nope + half :] = (first * sine + second * cosine).astype(BF16)
        for load in (l_inp, l_rate, l_shift):
            load.start()

    def relay1(k):
        if sp_count > 1:

            @pl.when(sp >= 1)
            def _():
                landed(k).wait_recv()
                if sp_count > 2:
                    pl.when(has_next)(lambda: forward(k).start())
                if k:
                    cross(1)

    with scope("p_relay1a"):
        relay1(0)

    with scope("q_gates"):
        l_gate.wait()
        project(w_gate, gate)
        for e in range(2, sp_count):

            @pl.when(sp + e < sp_count)
            def _(e=e):
                pl.semaphore_wait(ready.at[e - 1], 1)
                if e > 2:
                    direct(e).start()

        silu_gate[...] = jax.nn.silu(
            jnp.dot(mixer[...], gate[...], preferred_element_type=F32)
        )

    with scope("q_gate_att"):
        l_att.wait()
        project(w_att, attp)
        for load in (l_init, l_rout):
            load.start()

    with scope("p_relay1b"):
        relay1(1)
        for d in range(1, tp_count):
            weight_copy(1, d).start()
    silu_att[...] = jax.nn.silu(attp[...].astype(F32)).T
    with scope("m_rim"):

        @pl.when(sp == 0)
        def _():
            rim_in[...] = jnp.zeros_like(rim_in)

        pl.when(sp > 0)(lambda: rim_landed().wait_recv())
    with scope("n_scan"):
        for load in (l_conv, l_rec, l_inp, l_rate, l_shift):
            load.wait()
        size = rec_blocks.shape[1]
        car_out[...] = jnp.zeros_like(car_out)
        lead = 8 * (taps - 1)
        ext[lead : lead + rows] = jnp.dot(mixer[...], sig[...], preferred_element_type=F32)
        top_row = lax.broadcasted_iota(jnp.int32, (8, width), 0) == 0
        rim = rim_in[...].astype(F32)
        rim = jnp.concatenate(
            [rim[4 * c : 4 * c + 4] for c in range(width // LANES)], axis=1
        )
        for k in range(1, taps):
            last = ext[lead + rows - 8 * k : lead + rows - 8 * k + 8]
            ext[lead - 8 * k : lead - 8 * k + 8] = jnp.where(
                top_row, rim[4 - k : 5 - k], pltpu.roll(last, 1, 0)
            )
        table = jnp.concatenate(
            [decay_shift[:, k * long : (k + 1) * long] for k in range(8)], axis=0
        )
        for i in range(long):
            shift[8 * i : 8 * i + 8] = jnp.broadcast_to(table[:, i : i + 1], (8, LANES))
        groups = width // LANES
        for c in range(groups):
            cols = slice(c * LANES, (c + 1) * LANES)
            conv = conv_kernel[0:1, cols] * ext[0:rows, cols]
            for j in range(1, taps):
                conv = conv + conv_kernel[j : j + 1, cols] * ext[8 * j : 8 * j + rows, cols]
            conv = conv.astype(BF16)
            per = LANES // size
            rec = jax.nn.sigmoid(
                jnp.dot(conv, block_diagonal(diag_a, rec_blocks, c * per), preferred_element_type=F32)
            )
            inp = jax.nn.sigmoid(
                jnp.dot(conv, block_diagonal(diag_b, inp_blocks, c * per), preferred_element_type=F32)
            )
            log_decay = -RECURRENT_SCALE * rec * decay_rate[0:1, cols] + shift[...]
            decay = jnp.exp(log_decay)
            prod[c] = decay
            state[c] = jnp.sqrt(-expm1_neg(2.0 * log_decay, decay)) * inp * conv.astype(F32)
        ones = [prod[c, 0:8] for c in range(groups)]
        twos = [state[c, 0:8] for c in range(groups)]
        for i in range(1, long):
            here = slice(8 * i, 8 * i + 8)
            for c in range(groups):
                decay = prod[c, here]
                twos[c] = decay * twos[c] + state[c, here]
                ones[c] = decay * ones[c]
                prod[c, here] = ones[c]
                state[c, here] = twos[c]
        first_row = lax.broadcasted_iota(jnp.int32, (8, LANES), 0) == 0
        for c in range(groups):
            cols = slice(c * LANES, (c + 1) * LANES)
            one, two = scan_rows(ones[c], twos[c])
            segments[0:8, cols] = jnp.where(first_row, 1.0, pltpu.roll(one, 1, 0))
            segments[8:16, cols] = jnp.where(first_row, 0.0, pltpu.roll(two, 1, 0))
            car_out[2 * c : 2 * c + 1] = one[7:8]
            car_out[2 * c + 1 : 2 * c + 2] = two[7:8]

    def carry_copy(e):
        return remote(car_out, car_in.at[e - 1], c_s, c_r, sp=sp + e)

    def carry_landed(e):
        return remote(car_out, car_in.at[e - 1], c_s, c_r, sp=sp - e)

    with scope("o_carry"):
        for e in range(1, sp_count):
            pl.when(sp + e < sp_count)(lambda e=e: carry_copy(e).start())
    factor = head_dim ** (-0.5) * LOG2E

    def prepare(e):
        place = sp - e
        blocks = []
        for n in range(tp_count):
            order = [(n - r) % tp_count for r in range(tp_count)]
            first = [0 if j == 0 else tall + j * share for j in order]
            blocks.append(
                jnp.concatenate([lat_all[place, n, f : f + share] for f in first], axis=0).astype(F32)
            )
        square = sum(jnp.sum(x * x, axis=-1, keepdims=True) for x in blocks)
        inverse = lax.rsqrt(square / (lat * tp_count) + EPS)
        for n, x in enumerate(blocks):
            cols = slice(n * lat, (n + 1) * lat)
            xlat[:, cols] = (x * inverse * latent_gain[0:1, cols]).astype(BF16)
        rope_keys[...] = jnp.concatenate(
            [
                lat_all[place, n, share : share + tall, k * rope : (k + 1) * rope]
                for n in range(tp_count)
                for k in range(packed)
            ],
            axis=0,
        )
        step = column_step(w_up.shape[1])
        for c in range(w_up.shape[1] // step):
            cols = slice(c * step, (c + 1) * step)
            kv[:, cols] = jnp.dot(xlat[...], w_up[:, cols], preferred_element_type=F32).astype(BF16)
        for h in range(heads):
            base = h * (nope + value) + nope
            turned_v[h] = kv[:, base : base + value].T

    def score(h, diagonal, lanes, count):
        base = h * (nope + value)
        keys = jnp.concatenate([kv[:, base : base + nope], rope_keys[...]], axis=1)
        scores = jnp.dot(keys, queries[h, :, lanes], preferred_element_type=F32) * factor
        if diagonal:
            seen = lax.broadcasted_iota(jnp.int32, scores.shape, 0)
            scores = jnp.where(
                seen <= lax.broadcasted_iota(jnp.int32, scores.shape, 1), scores, -jnp.inf
            )
        held[h, :, :count] = scores
        return jnp.max(scores, axis=0, keepdims=True)

    def mix(h, top, diagonal, lanes, count):
        if not diagonal:
            before = row_max[h, 0:1, lanes]
            top = jnp.maximum(top, before)
            fade = jnp.exp2(before - top)
        weights = jnp.exp2(held[h, :, :count] - top)
        mass = jnp.sum(weights, axis=0, keepdims=True)
        term = jnp.dot(turned_v[h], weights.astype(BF16), preferred_element_type=F32)
        if not diagonal:
            mass = mass + row_sum[h, 0:1, lanes] * fade
            term = term + acc[h, :, lanes] * fade
        row_max[h, 0:1, lanes] = top
        row_sum[h, 0:1, lanes] = mass
        acc[h, :, lanes] = term

    def heads_over(diagonal, lanes=slice(None), count=rows):
        tops = [score(h, diagonal, lanes, count) for h in range(heads)]
        for h in range(heads):
            mix(h, tops[h], diagonal, lanes, count)

    def attend(e, diagonal):
        prepare(e)
        heads_over(diagonal)

    with scope("r_att0"):
        l_lgain.wait()
        l_up.wait()
        wait_crossed(0)
        prepare(0)
    with scope("r_att0_heads"):
        heads_over(True)
    with scope("t_relay3"):
        if sp_count > 3:

            @pl.when(sp >= 3)
            def _():
                arrived(3).wait_recv()
                cross(3)

    with scope("s_att1"):
        if sp_count > 1:

            @pl.when(sp >= 1)
            def _():
                wait_crossed(1)
                attend(1, False)

    with scope("w_att3"):
        if sp_count > 3:

            @pl.when(sp >= 3)
            def _():
                wait_crossed(3)
                attend(3, False)

        if sp_count > 4:

            def later(e, carry):
                block = lat_all.at[sp - e, tp]
                remote(block, block, z_s, fwd_r.at[e - 3], sp=sp - 1).wait_recv()
                cross(e)
                wait_crossed(e)
                attend(e, False)
                return carry

            lax.fori_loop(4, sp + 1, later, 0)
    with scope("x_relay2"):
        if sp_count > 2:

            @pl.when(sp >= 2)
            def _():
                for k in range(2):
                    forwarded(k).wait_recv()
                    for d in range(1, tp_count):
                        across_piece(k, d).start()

    with scope("u_carrywait"):
        for v in range(1, sp_count):

            @pl.when(sp == v)
            def _(v=v):
                remote(car_in.at[pl.ds(0, v)], car_in.at[pl.ds(0, v)], c_s, c_r, sp=sp - 1).wait_recv()

        for e in range(1, sp_count):

            @pl.when(sp < e)
            def _(e=e):
                row = lax.broadcasted_iota(jnp.int32, car_out.shape, 0)
                car_in[e - 1] = jnp.where((row & 1) == 0, 1.0, 0.0)

    def rout_copy(d):
        return remote(
            rout.at[share_rows(peer(d))], rout_in.at[d - 1], ro_s.at[d - 1], ro_r.at[d - 1], tp=peer(d)
        )

    def aout_copy(d):
        return remote(
            aout.at[share_rows(peer(d))], aout_in.at[d - 1], ao_s.at[d - 1], ao_r.at[d - 1], tp=peer(d)
        )

    with scope("v_rout"):
        l_init.wait()
        for c in range(width // LANES):
            cols = slice(c * LANES, (c + 1) * LANES)
            incoming = initial_state[:, cols]
            for e in range(sp_count - 1, 0, -1):
                incoming = (
                    car_in[e - 1, 2 * c : 2 * c + 1] * incoming
                    + car_in[e - 1, 2 * c + 1 : 2 * c + 2]
                )
            enter = segments[0:8, cols] * incoming + segments[8:16, cols]
            full = state[c] + prod[c] * jnp.concatenate([enter] * long, axis=0)
            mixed_rout[:, cols] = (full * silu_gate[:, cols]).astype(BF16)
        rout[...] = jnp.dot(
            unmixer[...], mixed_rout[...], preferred_element_type=F32
        ).astype(BF16)
        l_rout.wait()
        for d in range(1, tp_count):
            rout_copy(d).start()
        step = column_step(near)
        for c in range(near // step):
            cols = slice(near + c * step, near + (c + 1) * step)
            racc[:, cols] = jnp.dot(rout[...], w_rout[:, cols], preferred_element_type=F32)
        for c in range(near // step):
            cols = slice(c * step, (c + 1) * step)
            here = share_rows(tp)
            racc[here, cols] = jnp.dot(rout[here], w_rout[:, cols], preferred_element_type=F32)
    chunks, step = part_in.shape[1], part_in.shape[3]
    split = share % LANES == 0

    def part_copy(d, c):
        return remote(
            part.at[d - 1, c], part_in.at[d - 1, c], p_s.at[d - 1], p_r.at[d - 1, c], tp=peer(d)
        )

    def partial(place, cols):
        here = share_rows(place)
        both = racc[here, cols] + jnp.dot(aout[here], w_aout[:, cols], preferred_element_type=F32)
        return both.astype(BF16)

    def far(c):
        return slice(near + c * step, near + (c + 1) * step)

    def near_recurrent():
        for d in range(1, tp_count):
            rout_copy(d).wait_recv()
            weight_copy(1, d).wait_recv()
            for c in range(near // step):
                cols = slice(c * step, (c + 1) * step)
                racc_in[d - 1, :, cols] = jnp.dot(
                    rout_in[d - 1], w_rout_in[d - 1, :, cols], preferred_element_type=F32
                )

    def own_rows():
        for c in range(model // step):
            cols = slice(c * step, (c + 1) * step)
            own_part[:, cols] = partial(tp, cols)

    def finish(here):
        for h in range(heads):
            cols = slice(h * value, (h + 1) * value)
            attended = acc[h, :, here] * (1.0 / row_sum[h, 0:1, here])
            aout[here, cols] = (attended * silu_att[cols, here]).astype(BF16).T

    def send(d, c):
        part[d - 1, c] = partial(peer(d), far(c))
        part_copy(d, c).start()

    def send_all():
        for d in range(1, tp_count):
            aout_copy(d).start()
        for c in range(chunks):
            for d in range(1, tp_count):
                send(d, c)
        near_recurrent()
        own_rows()

    def last_block():
        for d in range(1, tp_count):
            block = lat_all.at[sp - 2, source(d)]
            remote(block, block, l_s.at[d - 1], x_r.at[d - 1], tp=source(d)).wait_recv()
        prepare(2)
        if not split:
            heads_over(False)
            finish(slice(None))
            send_all()
            return
        for d in range(1, tp_count):
            heads_over(False, share_rows(peer(d)), share)
            finish(share_rows(peer(d)))
            aout_copy(d).start()
        mine = share_rows(tp)
        sends = [(d, c) for d in range(1, tp_count) for c in range(chunks)]
        each = -(-2 * len(sends) // heads)
        tops = [score(h, False, mine, share) for h in range(heads)]
        for h in range(heads):
            for d, c in sends[h * each : (h + 1) * each]:
                send(d, c)
            mix(h, tops[h], False, mine, share)
        near_recurrent()
        finish(mine)
        own_rows()

    def no_block():
        finish(slice(None))
        send_all()

    with scope("y_last"):
        l_aout.wait()
        if sp_count > 2:
            pl.when(sp >= 2)(last_block)
            pl.when(sp < 2)(no_block)
        else:
            no_block()
    with scope("z_sum"):
        for d in range(1, tp_count):
            weight_copy(0, d).wait_recv()
            aout_copy(d).wait_recv()
        for c in range(near // step):
            cols = slice(c * step, (c + 1) * step)
            summed = own_part[:, cols].astype(F32)
            for d in range(1, tp_count):
                both = racc_in[d - 1, :, cols] + jnp.dot(
                    aout_in[d - 1], w_aout_in[d - 1, :, cols], preferred_element_type=F32
                )
                summed = summed + both.astype(BF16).astype(F32)
            out[:, cols] = summed.astype(BF16)
        for c in range(chunks):
            summed = own_part[:, far(c)].astype(F32)
            for d in range(1, tp_count):
                part_copy(d, c).wait_recv()
                summed = summed + part_in[d - 1, c].astype(F32)
            out[:, far(c)] = summed.astype(BF16)

    with scope("z_waits"):
        for d in range(1, tp_count):
            token_whole(d).wait_send()
            weight_copy(0, d).wait_send()
            weight_copy(1, d).wait_send()
            rout_copy(d).wait_send()
            aout_copy(d).wait_send()
            whole = part.at[d - 1]
            remote(whole, whole, p_s.at[d - 1], p_r.at[d - 1, 0], tp=peer(d)).wait_send()

        def all_sent(send, recv, count):
            blocks = lat_all.at[pl.ds(0, count), 0]
            remote(blocks, blocks, send, recv, tp=peer(1)).wait_send()

        for v in range(sp_count):

            @pl.when(sp == v)
            def _(v=v):
                for d in range(1, tp_count):
                    all_sent(l_s.at[d - 1], l_r.at[0, d - 1], v + 1)
                if v + 1 < sp_count:
                    rim_copy().wait_send()
                    onward = int(v > 0 and sp_count > 2)
                    all_sent(z_s, z_r.at[0], 1 + onward + max(sp_count - 3 - v, 0))
                    carries = car_in.at[pl.ds(0, sp_count - 1 - v)]
                    remote(carries, carries, c_s, c_r, sp=sp + 1).wait_send()


def body(
    tokens, norm_gain, recurrent_input, recurrent_gate, attention_gate, query_proj, latent_down,
    rope_key_down, conv_kernel, recurrence_gate_blocks, input_gate_blocks, decay_rate, decay_shift,
    initial_state, latent_gain, latent_up, query_gain, recurrent_output, attention_output,
):
    tp_count = lax.axis_size("tp")
    sp_count = lax.axis_size("sp")
    share, model = tokens.shape
    rows = share * tp_count
    width = recurrent_input.shape[1]
    taken = attention_gate.shape[1]
    head_dim = query_gain.shape[0]
    heads = query_proj.shape[1] // head_dim
    value = taken // heads
    lat = latent_down.shape[1]
    rope = rope_key_down.shape[1]
    cosine, sine = rotary_tables(sp_count * rows, rope)
    key_table = np.concatenate([cosine, cosine, -sine, sine], 1).reshape(-1, share, 2 * rope)
    query_table = np.concatenate([cosine, sine], 1).reshape(sp_count, rows, rope).transpose(0, 2, 1)
    hbm = [
        tokens, latent_down, norm_gain[None], rope_key_down.T, jnp.asarray(key_table),
        recurrent_input, query_proj, query_gain[None], jnp.asarray(query_table), conv_kernel,
        recurrence_gate_blocks, input_gate_blocks, decay_rate[None], decay_shift[None],
        recurrent_gate, attention_gate, latent_gain[None], latent_up, initial_state[None],
        recurrent_output, attention_output,
    ]
    held = [a.shape for a in hbm]
    held[4] = key_table.shape[1:]
    held[8] = query_table.shape[1:]
    vmem = pltpu.VMEM
    dma = pltpu.SemaphoreType.DMA
    others = max(tp_count - 1, 1)
    hops = max(sp_count - 1, 1)
    carries = -(-2 * width // LANES // 8) * 8
    rims = -(-4 * width // LANES // 16) * 16
    chunks = 1
    return pl.pallas_call(
        functools.partial(layer_kernel, sp_count, tp_count),
        out_shape=pltpu.VMEM((share, model), BF16),
        in_specs=[pl.BlockSpec(memory_space=pl.ANY)] * len(hbm),
        out_specs=pl.BlockSpec(memory_space=pltpu.VMEM),
        scratch_shapes=[vmem(s, a.dtype) for s, a in zip(held, hbm)]
        + [
            vmem((others, share, model), BF16),
            vmem((rows, model), BF16),
            vmem((sp_count, tp_count, rows + share * rope // lat, lat), BF16),
            vmem((rows, width), BF16),
            vmem((rows, width), BF16),
            vmem((rows, taken), BF16),
            vmem((query_proj.shape[1], rows), BF16),
            vmem((heads, head_dim, rows), BF16),
            vmem((rims, LANES), BF16),
            vmem((rims, LANES), BF16),
            vmem((rows + 24, width), F32),
            vmem((LANES, LANES), BF16),
            vmem((LANES, LANES), BF16),
            vmem((rows, rows), BF16),
            vmem((rows, rows), BF16),
            vmem((rows, LANES), F32),
            vmem((rows, width), F32),
            vmem((taken, rows), F32),
            vmem((rows, width), BF16),
            vmem((width // LANES, rows, LANES), F32),
            vmem((width // LANES, rows, LANES), F32),
            vmem((16, width), F32),
            vmem((carries, LANES), F32),
            vmem((hops, carries, LANES), F32),
            vmem((rows, width), BF16),
            vmem((rows, model), F32),
            vmem((rows, lat * tp_count), BF16),
            vmem((rows, rope), BF16),
            vmem((heads, value, rows), BF16),
            vmem((rows, latent_up.shape[1]), BF16),
            vmem((heads, rows, rows), F32),
            vmem((heads, 8, rows), F32),
            vmem((heads, 8, rows), F32),
            vmem((heads, value, rows), F32),
            vmem((rows, taken), BF16),
            vmem((others, chunks, share, model // 2 // chunks), BF16),
            vmem((share, model), BF16),
            vmem((others, chunks, share, model // 2 // chunks), BF16),
            vmem((others, taken, model // 2), BF16),
            vmem((others, width, model // 2), BF16),
            vmem((others, share, width), BF16),
            vmem((others, share, taken), BF16),
            vmem((others, share, model // 2), F32),
            dma((10,)),
            dma((others,)), dma((others,)),
            dma, dma((2,)),
            dma((2,)),
            dma((max(sp_count - 3, 1),)),
            dma((others,)), dma((max(sp_count - 1, 1), others)),
            dma((others,)),
            dma, dma,
            dma, dma,
            dma((others,)), dma((others, chunks)),
            dma((2, others)), dma((2, others)),
            dma((others,)), dma((others,)),
            dma((others,)), dma((others,)),
            pltpu.SemaphoreType.REGULAR((hops,)),
        ],
        compiler_params=pltpu.CompilerParams(
            collective_id=0, has_side_effects=True, vmem_limit_bytes=61400 * 1024
        ),
    )(*hbm)


def solution(mesh):
    return jax.shard_map(
        body,
        mesh=mesh,
        in_specs=(
            P(("fs", "sp", "tp"), None),
            P(),
            P(None, "tp"),
            P(None, "tp"),
            P(None, "tp"),
            P(None, "tp"),
            P(None, "tp"),
            P(),
            P(None, "tp"),
            P("tp", None, None),
            P("tp", None, None),
            P("tp"),
            P(("fs", "sp")),
            P(("fs", "tp")),
            P(),
            P(None, "tp"),
            P(),
            P("tp", None),
            P("tp", None),
        ),
        out_specs=P(("fs", "sp", "tp"), None),
        check_vma=False,
    )
```
